256 devices in a mesh: grp: 2 (over y), sp: 32 (over z, core), tp: 4 (over x).
Axes of the slice: x: 4, y: 2, z: 16, core: 2. Of those that a mesh axis runs over, the one named last changes fastest.
The devices are a block of a 4x16x16 slice.
Arguments:
- recept: bfloat16 [32768, 2048], P(('grp', 'sp'), 'tp'), parts along dimension 0, may hold values from -6 to 6
- key_input: bfloat16 [32768, 2048], P(('grp', 'sp'), 'tp'), parts along dimension 0, may hold values from -6 to 6
- value_input: bfloat16 [32768, 2048], P(('grp', 'sp'), 'tp'), parts along dimension 0, may hold values from -6 to 6
- output_gate_input: bfloat16 [32768, 2048], P(('grp', 'sp'), 'tp'), parts along dimension 0, may hold values from -6 to 6
- decay_input_part: bfloat16 [32768, 2048], P(('grp', 'sp'), 'tp'), parts along dimension 0, may hold values from -4.8 to 4.8
- correction_rate_input: bfloat16 [32768, 2048], P(('grp', 'sp'), 'tp'), parts along dimension 0, may hold values from -4 to 4
- head_decay_offset: float32 [32768, 32], P(('grp', 'sp'), 'tp'), parts along dimension 0, may hold values from -2.1 to 0
- decay_fixed_bias: float32 [2048], P('tp'), may hold values from -11.5 to -2.8
- correction_rate_bias: float32 [2048], P('tp'), may hold values from -8.5 to 1
- head_norm_gain: float32 [2048], P('tp'), may hold values from 0.1 to 1.9
- self_term_weight: float32 [2048], P('tp'), may hold values from -2 to 2
- output_weight_matrix: bfloat16 [2048, 2048], P('tp'), may hold values from -0.125 to 0.125
- residual: bfloat16 [32768, 2048], P(('grp', 'sp', 'tp')), parts along dimension 0, may hold values from -6 to 6
- feedforward_norm_gain: float32 [2048], replicated, may hold values from 0.1 to 1.9
- routed_expert_index: int32 [32768, 2], P(('grp', 'sp', 'tp')), parts along dimension 0, may hold values from 0 to 31, all different within a row; in each aligned block of 128 rows (0 to 127, 128 to 255, ...) at most 12 rows name the same one
- routed_expert_weight: float32 [32768, 2], P(('grp', 'sp', 'tp')), parts along dimension 0, may hold values from 0.2 to 1
- gate_weight_experts: bfloat16 [32, 2048, 1024], P('sp', None, 'tp'), may hold values from -0.125 to 0.125
- up_weight_experts: bfloat16 [32, 2048, 1024], P('sp', None, 'tp'), may hold values from -0.125 to 0.125
- down_weight_experts: bfloat16 [32, 1024, 2048], P('sp', 'tp'), may hold values from -0.1875 to 0.1875
Outputs:
- output: bfloat16 [32768, 2048], P(('grp', 'sp', 'tp')), parts along dimension 0
The draws below stay inside these ranges and needn't reach their ends.
There are 2 independent parts, one for each index of `grp`. The reference program is written for one: setup_inputs(seed, part) draws one part's arguments, and reference() takes and returns one part's arrays. A program takes and returns all parts, laid end to end along the dimension named above; an argument that names none is the same for every part. Nothing has to cross between parts.
Inputs may be any that keep to these rules, and one draw needn't show every extreme that they name: `routed_expert_index`: in each aligned block of 128 rows (the rows of one device) no expert is named by more than 12 routes; the two experts of a row differ.
All inputs are finite; a program needn't handle non-finite values.
Results may differ from the reference program's by a relative error of at most 0.0058.
Values may be sent and summed in bfloat16 or wider, within the bound.
A program may use at most 128 MiB of HBM per device.

```python
import math
import jax
import jax.numpy as jnp
import numpy as np
from jax import lax

D = 2048
HEAD_COUNT = 32
HEAD_CHANNELS = 64
MODEL_WIDTH = 2048
FF = 1024
EXPERTS = 32
TOK_SP = 512
SEQUENCE_TOKENS = 16384
CAP = 12
N_SP = 32
N_TP = 4


def head_kinds(key):
    share = 5
    fast_heads = jax.random.randint(jax.random.fold_in(key, 11), (HEAD_COUNT,), 0, 10) < share
    return jnp.repeat(fast_heads, HEAD_CHANNELS)


def draw_decay_fixed_bias(key, part):
    fast_chan = head_kinds(key)
    uniform_draw = jax.random.uniform(jax.random.fold_in(key, 12), (MODEL_WIDTH,), jnp.float32)
    return jnp.where(fast_chan, -3.8 + uniform_draw, -11.5 + uniform_draw).astype(jnp.float32)


def draw_correction_rate_bias(key, part):
    fast_chan = head_kinds(key)
    uniform_draw = jax.random.uniform(jax.random.fold_in(key, 13), (MODEL_WIDTH,), jnp.float32)
    return jnp.where(fast_chan, -1.0 + 2.0 * uniform_draw, -8.5 + uniform_draw).astype(jnp.float32)


def draw_decay_input_part(key, part):
    noise = jnp.clip(jax.random.normal(jax.random.fold_in(key, 21), (SEQUENCE_TOKENS, MODEL_WIDTH), jnp.float32), -4.0, 4.0)
    shifts = jax.random.uniform(jax.random.fold_in(key, 22), (SEQUENCE_TOKENS // TOK_SP, 1, 1), jnp.float32, -0.8, 0.8)
    shaped = noise.reshape(SEQUENCE_TOKENS // TOK_SP, TOK_SP, MODEL_WIDTH) + shifts
    return shaped.reshape(SEQUENCE_TOKENS, MODEL_WIDTH).astype(jnp.bfloat16)


def draw_correction_rate_input(key, part):
    noise = jnp.clip(jax.random.normal(jax.random.fold_in(key, 31), (SEQUENCE_TOKENS, MODEL_WIDTH), jnp.float32), -4.0, 4.0)
    return noise.astype(jnp.bfloat16)


def draw_head_decay_offset(key, part):
    spots = jax.random.randint(jax.random.fold_in(key, 41), (3, HEAD_COUNT), 0, SEQUENCE_TOKENS)
    losses = jnp.log(jax.random.uniform(jax.random.fold_in(key, 42), (3, HEAD_COUNT), jnp.float32, 0.5, 0.8))
    places = jnp.arange(SEQUENCE_TOKENS, dtype=jnp.int32)[None, :, None]
    hits = places == spots[:, None, :]
    return jnp.sum(jnp.where(hits, losses[:, None, :], 0.0), axis=0).astype(jnp.float32)


def level_of(rng, dims, split, least, top_value):
    gain, own = 1.0, jax.random.fold_in(rng, 6)
    for dim, blocks in split:
        draws = jnp.exp(jax.random.uniform(jax.random.fold_in(own, dim), (blocks,), jnp.float32, least / len(split), top_value / len(split)))
        gain = gain * jnp.repeat(draws, dims[dim] // blocks).reshape([-1 if axis == dim else 1 for axis in range(len(dims))])
    return gain


def routed_block(rng, own, number, rows, amount, top, most, lean):
    sequence = jax.random.permutation(rng, amount)
    crowded, common = load_shares(amount, rows * top, most, lean, True), load_shares(amount, rows * top, most, lean, False)
    places = jnp.arange(amount)

    def named(sizes, turn):
        used = int((sizes > 0).sum())
        fixed = max(1, used // 4)
        moved = fixed + (places - fixed + turn * (used - fixed)) % max(1, amount - fixed)
        return jnp.zeros((amount,), jnp.int32).at[sequence[jnp.where(places < fixed, places, moved)]].set(jnp.asarray(sizes, jnp.int32))

    sizes = jnp.where(number % 4 == 0, named(crowded, number // 4), named(common, number - number // 4 - 1))
    mixed = jax.random.permutation(jax.random.fold_in(own, 3), amount)
    donor, receiver = mixed[0:amount // 2 * 2:2], mixed[1:amount // 2 * 2:2]
    slack = jnp.minimum(sizes[donor] - 1, most - sizes[receiver]) // 2
    slack = jnp.where((donor == sequence[0]) | (receiver == sequence[0]) | (sizes[receiver] == 0), 0, jnp.maximum(slack, 0))
    moved = jax.random.randint(jax.random.fold_in(own, 4), (amount // 2,), 0, 1 << 20) % (slack + 1)
    sizes = sizes.at[donor].add(-moved).at[receiver].add(moved)
    labels = jnp.searchsorted(jnp.cumsum(sizes), jnp.arange(rows * top), side="right").astype(jnp.int32)
    table = labels.reshape(top, rows).T
    table = table[jax.random.permutation(jax.random.fold_in(own, 1), rows)]
    turn = jax.random.randint(jax.random.fold_in(own, 2), (rows, 1), 0, top)
    return jnp.take_along_axis(table, (jnp.arange(top)[None, :] + turn) % top, axis=1)


def load_shares(count, total, limit, slope, full):
    portions = [(1 << 20) // math.isqrt(rank ** slope) + 1 for rank in range(1, count + 1)]
    largest = limit if full else min(limit, max(-(-total // count), total * portions[0] // sum(portions)))
    least = 1 if total - largest >= count - 1 else 0
    given, surplus = [largest] + [least] * (count - 1), total - largest - least * (count - 1)
    while surplus > 0:
        candidates = [i for i in range(1, count) if given[i] < largest] or [i for i in range(1, count) if given[i] < limit]
        whole, remaining = sum([portions[i] for i in candidates]), surplus
        for i in candidates:
            extra = min(limit - given[i], max(1, remaining * portions[i] // whole), surplus)
            given[i] = given[i] + extra
            surplus = surplus - extra
    return np.array(given)


def bell_draw(stream_key, dims, width, reach, shards=(), held_as=jnp.bfloat16):
    values = jax.random.normal(stream_key, dims, jnp.float32) * width
    if len(shards) > 0:
        values = level_of(stream_key, dims, shards, -0.22, 0.18) * values
    return jnp.clip(values, min=-reach, max=reach).astype(held_as)


def setup_inputs(seed: int = 0, part: int = 0) -> dict:
    streams_of = jax.random.split(jax.random.key(seed), 20)
    own_keys = jax.random.split(jax.random.fold_in(streams_of[19], part), 20)
    recept = bell_draw(own_keys[0], (SEQUENCE_TOKENS, MODEL_WIDTH), 1.0, 6.0, ((0, 32), (1, 4)))
    key_input = bell_draw(own_keys[1], (SEQUENCE_TOKENS, MODEL_WIDTH), 1.0, 6.0, ((0, 32), (1, 4)))
    value_input = bell_draw(own_keys[2], (SEQUENCE_TOKENS, MODEL_WIDTH), 1.0, 6.0, ((0, 32), (1, 4)))
    output_gate_input = bell_draw(own_keys[3], (SEQUENCE_TOKENS, MODEL_WIDTH), 1.0, 6.0, ((0, 32), (1, 4)))
    decay_input_part = draw_decay_input_part(jax.random.fold_in(jax.random.fold_in(streams_of[19], part), 71), part)
    correction_rate_input = draw_correction_rate_input(jax.random.fold_in(jax.random.fold_in(streams_of[19], part), 71), part)
    head_decay_offset = draw_head_decay_offset(jax.random.fold_in(jax.random.fold_in(streams_of[19], part), 71), part)
    decay_fixed_bias = draw_decay_fixed_bias(jax.random.fold_in(streams_of[19], 71), part)
    correction_rate_bias = draw_correction_rate_bias(jax.random.fold_in(streams_of[19], 71), part)
    head_norm_gain = jnp.clip(1.0 + 0.18 * jax.random.normal(streams_of[9], (MODEL_WIDTH,), jnp.float32), 0.1, 1.9)
    self_term_weight = bell_draw(streams_of[10], (MODEL_WIDTH,), 0.15, 2.0, ((0, 4),), jnp.float32)
    output_weight_matrix = bell_draw(streams_of[11], (MODEL_WIDTH, D), MODEL_WIDTH ** -0.5, 0.125, ((0, 4),))
    residual = bell_draw(own_keys[12], (SEQUENCE_TOKENS, D), 1.0, 6.0, ((0, 128),))
    feedforward_norm_gain = jnp.clip(1.0 + 0.18 * jax.random.normal(streams_of[13], (D,), jnp.float32), 0.1, 1.9)
    routed_expert_index_keys = jax.random.split(jax.random.fold_in(own_keys[14], 1), SEQUENCE_TOKENS // (TOK_SP // N_TP))
    routed_expert_index_turns = jax.random.permutation(jax.random.fold_in(own_keys[14], 3), SEQUENCE_TOKENS // (TOK_SP // N_TP))
    routed_expert_index = jax.vmap(lambda own, number: routed_block(jax.random.fold_in(own_keys[14], 2), own, number, TOK_SP // N_TP, EXPERTS, 2, CAP, 1))(routed_expert_index_keys, routed_expert_index_turns).reshape((SEQUENCE_TOKENS, 2))
    routed_expert_weight = jnp.clip(0.2 + 0.8 * jax.random.uniform(own_keys[15], (SEQUENCE_TOKENS, 2), jnp.float32) ** level_of(own_keys[15], (SEQUENCE_TOKENS, 2), ((0, 128),), -0.2, 0.2), 0.2, 1.0)
    gate_weight_experts = bell_draw(streams_of[16], (EXPERTS, D, FF), D ** -0.5, 0.125, ((0, 32), (2, 4)))
    up_weight_experts = bell_draw(streams_of[17], (EXPERTS, D, FF), D ** -0.5, 0.125, ((0, 32), (2, 4)))
    down_weight_experts = bell_draw(streams_of[18], (EXPERTS, FF, D), FF ** -0.5, 0.1875, ((0, 32), (1, 4)))
    return {"recept": recept, "key_input": key_input, "value_input": value_input, "output_gate_input": output_gate_input, "decay_input_part": decay_input_part, "correction_rate_input": correction_rate_input, "head_decay_offset": head_decay_offset, "decay_fixed_bias": decay_fixed_bias, "correction_rate_bias": correction_rate_bias, "head_norm_gain": head_norm_gain, "self_term_weight": self_term_weight, "output_weight_matrix": output_weight_matrix, "residual": residual, "feedforward_norm_gain": feedforward_norm_gain, "routed_expert_index": routed_expert_index, "routed_expert_weight": routed_expert_weight, "gate_weight_experts": gate_weight_experts, "up_weight_experts": up_weight_experts, "down_weight_experts": down_weight_experts}


PRECISE = lax.Precision.HIGHEST
GROUP_EPS = 0.00064
NORM_EPS = 1e-06

def recurrence(receptance_per_head, decay_per_head, key_per_head, value_per_head, remove_h, write_h):

    def advance(states, inputs):
        recept_t, decay_t, key_t, value_t, remove_t, write_t = inputs
        removed = jnp.einsum('hvk,hk->hv', states, remove_t, precision=PRECISE)
        states = states * decay_t[:, None, :] + removed[:, :, None] * write_t[:, None, :] + value_t[:, :, None] * key_t[:, None, :]
        return (states, jnp.einsum('hvk,hk->hv', states, recept_t, precision=PRECISE))
    initial = jnp.zeros((HEAD_COUNT, HEAD_CHANNELS, HEAD_CHANNELS), jnp.float32)
    _, readout = lax.scan(advance, initial, (receptance_per_head, decay_per_head, key_per_head, value_per_head, remove_h, write_h))
    return readout

def expert_rows(features, gate_mat, up_mat, down_mat):
    gated = jnp.dot(features, gate_mat, preferred_element_type=jnp.float32)
    upward = jnp.dot(features, up_mat, preferred_element_type=jnp.float32)
    hidden = (jax.nn.silu(gated) * upward).astype(jnp.bfloat16)
    blocks = jnp.einsum('rjf,jfd->rjd', hidden.reshape(features.shape[0], N_TP, FF // N_TP).astype(jnp.float32), down_mat.reshape(N_TP, FF // N_TP, D).astype(jnp.float32), precision=PRECISE)
    rounded = lax.optimization_barrier(blocks.astype(jnp.bfloat16)).astype(jnp.float32)
    return lax.optimization_barrier(jnp.sum(rounded, axis=1)).astype(jnp.bfloat16)

def reference(recept, key_input, value_input, output_gate_input, decay_input_part, correction_rate_input, head_decay_offset, decay_fixed_bias, correction_rate_bias, head_norm_gain, self_term_weight, output_weight_matrix, residual, feedforward_norm_gain, routed_expert_index, routed_expert_weight, gate_weight_experts, up_weight_experts, down_weight_experts):

    def split_into_heads(tensor):
        return tensor.astype(jnp.float32).reshape(SEQUENCE_TOKENS, HEAD_COUNT, HEAD_CHANNELS)
    receptance_per_head, key_per_head, value_per_head = (split_into_heads(recept), split_into_heads(key_input), split_into_heads(value_input))
    weight_logarithm = -jax.nn.softplus(-(decay_fixed_bias + decay_input_part.astype(jnp.float32))) - 0.5
    decay_per_head = jnp.exp(-jnp.exp(split_into_heads(weight_logarithm)) + head_decay_offset[:, :, None])
    rate_h = split_into_heads(jax.nn.sigmoid(correction_rate_bias + correction_rate_input.astype(jnp.float32)))
    unit_key = key_per_head * lax.rsqrt(lax.optimization_barrier(jnp.sum(key_per_head * key_per_head, axis=-1, keepdims=True)) + NORM_EPS)
    readout = recurrence(receptance_per_head, decay_per_head, key_per_head, value_per_head, -unit_key, unit_key * rate_h)
    center = lax.optimization_barrier(jnp.mean(readout, axis=-1, keepdims=True))
    spread = lax.optimization_barrier(jnp.mean(jnp.square(readout - center), axis=-1, keepdims=True))
    normalized_state = (readout - center) * lax.rsqrt(spread + GROUP_EPS) * head_norm_gain.reshape(HEAD_COUNT, HEAD_CHANNELS)
    self_term = lax.optimization_barrier(jnp.sum(receptance_per_head * key_per_head * self_term_weight.reshape(HEAD_COUNT, HEAD_CHANNELS), axis=-1, keepdims=True)) * value_per_head
    attention_result = ((normalized_state + self_term).reshape(SEQUENCE_TOKENS, MODEL_WIDTH) * output_gate_input.astype(jnp.float32)).astype(jnp.bfloat16)
    proj = jnp.dot(attention_result, output_weight_matrix, preferred_element_type=jnp.float32).astype(jnp.bfloat16)
    stream = residual.astype(jnp.float32) + lax.optimization_barrier(proj).astype(jnp.float32)
    ffn_in = (stream * lax.rsqrt(lax.optimization_barrier(jnp.mean(stream * stream, axis=-1, keepdims=True)) + NORM_EPS) * feedforward_norm_gain).astype(jnp.bfloat16)
    flat_ids = routed_expert_index.reshape(-1).astype(jnp.int32)
    flat_weights = routed_expert_weight.reshape(-1)
    top_count = routed_expert_index.shape[1]
    order = jnp.argsort(flat_ids, stable=True).astype(jnp.int32)
    counts = lax.optimization_barrier(jnp.sum((flat_ids[:, None] == jnp.arange(EXPERTS, dtype=jnp.int32)[None, :]).astype(jnp.int32), axis=0))
    starts = (jnp.cumsum(counts) - counts).astype(jnp.int32)
    room = N_SP * N_TP * CAP
    padded = jnp.concatenate([order, jnp.zeros((room,), jnp.int32)])

    def one_expert(accum, expert):
        entries = lax.dynamic_slice_in_dim(padded, starts[expert], room)
        live = jnp.arange(room, dtype=jnp.int32) < counts[expert]
        positions = (entries // top_count).astype(jnp.int32)
        result = expert_rows(ffn_in[positions], gate_weight_experts[expert], up_weight_experts[expert], down_weight_experts[expert])
        scales = jnp.where(live, flat_weights[entries], 0.0)
        return (accum.at[positions].add(result.astype(jnp.float32) * scales[:, None]), None)
    accum, _ = lax.scan(one_expert, jnp.zeros((SEQUENCE_TOKENS, D), jnp.float32), jnp.arange(EXPERTS, dtype=jnp.int32))
    return (stream + accum).astype(jnp.bfloat16)
```

```python
import functools

import jax
import jax.numpy as jnp
from jax import lax
from jax.experimental import pallas as pl
from jax.experimental.pallas import tpu as pltpu
from jax.sharding import PartitionSpec as P

f32, bf16 = jnp.float32, jnp.bfloat16
MESH = pl.DeviceIdType.MESH
NN = (((1,), (0,)), ((), ()))
NT = (((1,), (1,)), ((), ()))
GROUP_EPS = 0.00064
NORM_EPS = 1e-06
SPAN = 64
LANES = 128
HEAD = 64
DECAY_SCALE = 0.6065306597126334
QUARTERS = 4
BLOCK = 4
VMEM_SPEC = pl.BlockSpec(memory_space=pltpu.VMEM)


def dot(a, b, dims=NN):
    return lax.dot_general(a.astype(bf16), b.astype(bf16), dims, preferred_element_type=f32)


def halves(x):
    high = x.astype(bf16)
    return high, (x - high.astype(f32)).astype(bf16)


def dot_split_left(a, b):
    high, low = halves(a)
    return dot(high, b) + dot(low, b)


def dot_split_right(a, b):
    high, low = halves(b)
    return dot(a, high) + dot(a, low)


def iota(shape, dim):
    return lax.broadcasted_iota(jnp.int32, shape, dim)


def sigmoid(x):
    return 1.0 / (1.0 + jnp.exp(-x))


def head_ones():
    shape = (LANES, LANES)
    return jnp.where((iota(shape, 0) >> 6) == (iota(shape, 1) >> 6), 1.0, 0.0).astype(bf16)


def stacked(x):
    first = iota(x.shape, 1) < HEAD
    zero = jnp.zeros_like(x)
    return jnp.concatenate([jnp.where(first, x, zero), jnp.where(first, zero, x)], axis=0)


def chunk_maps(recept, key, value, decay_pre, rate_pre, offset, decay_bias, rate_bias):
    row = iota((SPAN, LANES), 0)
    col = iota((SPAN, LANES), 1) & (HEAD - 1)
    decay_log = offset - DECAY_SCALE * sigmoid(decay_bias + decay_pre)
    rate = sigmoid(rate_bias + rate_pre)
    norm = dot_split_left(key * key, head_ones())
    unit = key * lax.rsqrt(norm + NORM_EPS)
    square = (SPAN, SPAN)
    lower = jnp.where(iota(square, 0) >= iota(square, 1), 1.0, 0.0).astype(bf16)
    cumul = dot_split_right(lower, decay_log)
    middle = cumul[SPAN // 2 - 1 : SPAN // 2, :]
    rel = cumul - middle
    rise, fall = jnp.exp(rel), jnp.exp(-rel)
    to_middle = jnp.exp(middle)
    to_end = jnp.exp(cumul[SPAN - 1 : SPAN, :] - middle)
    remove = -unit * jnp.exp(rel - decay_log)
    read = recept * rise
    write = unit * rate * fall
    keys = key * fall
    scores = dot(
        jnp.concatenate([remove.astype(bf16), read.astype(bf16)], axis=0),
        jnp.concatenate([stacked(write.astype(bf16)), stacked(keys.astype(bf16))], axis=0),
        NT,
    )
    strict, within = row > col, row >= col
    lower_part = jnp.where(strict, scores[:SPAN, :LANES], 0.0)
    remove_key = jnp.where(strict, scores[:SPAN, LANES:], 0.0)
    read_write = jnp.where(within, scores[SPAN:, :LANES], 0.0)
    read_key = jnp.where(within, scores[SPAN:, LANES:], 0.0)

    def merging(level):
        size = 1 << level
        same = (row >> (level + 1)) == (col >> (level + 1))
        return same & ((row & size) != 0) & ((col & size) == 0)

    inverse = jnp.where(row == col, 1.0, jnp.where(merging(0), lower_part, 0.0))
    for level in range(1, SPAN.bit_length() - 1):
        block = jnp.where(merging(level), lower_part, 0.0)
        inner = dot(block, stacked(inverse.astype(bf16)))
        inverse = inverse + dot(inverse, stacked(inner.astype(bf16)))
    removed_value = dot(remove_key, stacked(value.astype(bf16)))
    solved = dot(
        inverse,
        jnp.concatenate(
            [stacked((remove * to_middle).astype(bf16)), stacked(removed_value.astype(bf16))], axis=1
        ),
    )
    left = jnp.concatenate([solved[:, :LANES], read * to_middle], axis=0).astype(bf16)
    write_end = jnp.concatenate([write * to_end, keys * to_end], axis=0).T.astype(bf16)
    ending = jnp.broadcast_to(to_end * to_middle, (LANES, LANES)).T
    within_maps = jnp.concatenate([read_write, read_key], axis=1).astype(bf16)
    return left, solved[:, LANES:], within_maps, write_end, ending


def mixer_kernel(
    pairs, chunks,
    recept_ref, key_ref, value_ref, decay_ref, rate_ref, offset_ref, decay_bias_ref, rate_bias_ref,
    summary_ref, map_ref, own_ref,
    left_ref, solved_ref, within_ref, write_ref, ending_ref, state_ref, removed_ref, partial_ref,
):
    first_head = iota((SPAN, LANES), 1) < HEAD

    def rows_of(c):
        return pl.ds(pl.multiple_of(c * SPAN, SPAN), SPAN)

    def prepare(c):
        rows = rows_of(c)
        for p in range(pairs):
            cols = slice(p * LANES, (p + 1) * LANES)
            offset = jnp.where(
                first_head, offset_ref[rows, 2 * p : 2 * p + 1], offset_ref[rows, 2 * p + 1 : 2 * p + 2]
            )
            left, solved, within, write, ending = chunk_maps(
                recept_ref[rows, cols].astype(f32),
                key_ref[rows, cols].astype(f32),
                value_ref[rows, cols].astype(f32),
                decay_ref[rows, cols].astype(f32),
                rate_ref[rows, cols].astype(f32),
                offset,
                decay_bias_ref[:, cols],
                rate_bias_ref[:, cols],
            )
            left_ref[c, p] = left
            solved_ref[c, p] = solved
            within_ref[c, p] = within
            write_ref[c, p] = write
            ending_ref[c, p] = ending

    unroll = 2 if chunks % 2 == 0 else 1

    def prepare_some(i, _):
        for k in range(unroll):
            prepare(i * unroll + k)
        return 0

    lax.fori_loop(0, chunks // unroll, prepare_some, 0)

    square = (LANES, LANES)
    eye = jnp.where(iota(square, 0) == iota(square, 1), 1.0, 0.0)
    for p in range(pairs):
        state_ref[p, :, :LANES] = eye
        state_ref[p, :, LANES:] = jnp.zeros(square, f32)
    own_block = (iota((LANES, 2 * LANES), 0) >> 6) == ((iota((LANES, 2 * LANES), 1) >> 6) & 1)

    def advance(c, _):
        rows = rows_of(c)
        for p in range(pairs):
            value = value_ref[rows, p * LANES : (p + 1) * LANES]
            state = state_ref[p]
            crossed = dot(left_ref[c, p], state)
            removed = jnp.concatenate(
                [crossed[:SPAN, :LANES], crossed[:SPAN, LANES:] + solved_ref[c, p]], axis=1
            ).astype(bf16)
            removed_ref[c, p] = removed
            partial_ref[c, p] = crossed[SPAN:]
            right = jnp.concatenate(
                [removed, jnp.concatenate([jnp.zeros_like(value), value], axis=1)], axis=0
            )
            update = dot(write_ref[c, p], right)
            ending = ending_ref[c, p]
            state_ref[p] = state * jnp.concatenate([ending, ending], axis=1) + jnp.where(
                own_block, update, 0.0
            )
        return 0

    lax.fori_loop(0, chunks, advance, 0)

    for p in range(pairs):
        transit = state_ref[p, :, :LANES] - eye
        added = state_ref[p, :, LANES:]
        summary_ref[p, 0] = (transit[:HEAD] + transit[HEAD:]).astype(bf16)
        summary_ref[p, 1] = (added[:HEAD] + added[HEAD:]).astype(bf16)

    def emit(c, _):
        rows = rows_of(c)
        for p in range(pairs):
            cols = slice(p * LANES, (p + 1) * LANES)
            removed = removed_ref[c, p]
            value = stacked(value_ref[rows, cols])
            right = jnp.concatenate(
                [
                    jnp.concatenate([stacked(removed[:, :LANES]), stacked(removed[:, LANES:])], axis=1),
                    jnp.concatenate([jnp.zeros_like(value), value], axis=1),
                ],
                axis=0,
            )
            both = partial_ref[c, p] + dot(within_ref[c, p], right)
            map_ref[rows, cols] = both[:, :LANES].astype(bf16)
            own_ref[rows, cols] = both[:, LANES:]
        return 0

    lax.fori_loop(0, chunks, emit, 0)


def mixer_local(recept, key, value, decay, rate, offset, decay_bias, rate_bias):
    length, width = recept.shape
    pairs, chunks = width // LANES, length // SPAN
    per = (chunks, pairs)
    return pl.pallas_call(
        functools.partial(mixer_kernel, pairs, chunks),
        name="mixer_local",
        out_shape=(
            jax.ShapeDtypeStruct((pairs, 2, HEAD, LANES), bf16),
            jax.ShapeDtypeStruct((length, width), bf16),
            jax.ShapeDtypeStruct((length, width), f32),
        ),
        in_specs=[VMEM_SPEC] * 8,
        out_specs=(VMEM_SPEC,) * 3,
        scratch_shapes=[
            pltpu.VMEM(per + (2 * SPAN, LANES), bf16),
            pltpu.VMEM(per + (SPAN, LANES), f32),
            pltpu.VMEM(per + (SPAN, 2 * LANES), bf16),
            pltpu.VMEM(per + (LANES, 2 * SPAN), bf16),
            pltpu.VMEM(per + (LANES, LANES), f32),
            pltpu.VMEM((pairs, LANES, 2 * LANES), f32),
            pltpu.VMEM(per + (SPAN, 2 * LANES), bf16),
            pltpu.VMEM(per + (SPAN, 2 * LANES), f32),
        ],
        compiler_params=pltpu.CompilerParams(vmem_limit_bytes=40 << 20),
        cost_estimate=pl.CostEstimate(
            flops=80 * 2 * LANES * length * width, bytes_accessed=12 * length * width, transcendentals=0
        ),
    )(recept, key, value, decay, rate, offset, decay_bias, rate_bias)


def prefix_kernel(n, pairs, summary_ref, enter_ref, got, states, entry, sent1, came1, sent2, came2):
    me = lax.axis_index("sp")
    stride = n // pairs
    works = lax.rem(me, stride) == 0
    mine = lax.div(me, stride)
    barrier = pltpu.get_barrier_semaphore()

    def greet(device):
        pl.semaphore_signal(barrier, inc=1, device_id={"sp": device}, device_id_type=MESH)

    @pl.when(works)
    def _():
        def body(j, _):
            greet(lax.rem(me + j, n))
            return 0

        lax.fori_loop(1, n, body, 0)
        pl.semaphore_wait(barrier, n - 1)

    @pl.when(jnp.logical_not(works))
    def _():
        for p in range(pairs):
            greet(p * stride)
        pl.semaphore_wait(barrier, pairs)

    def outward(p):
        return pltpu.make_async_remote_copy(
            src_ref=summary_ref.at[p], dst_ref=got.at[me], send_sem=sent1.at[p], recv_sem=came1.at[me],
            device_id={"sp": p * stride}, device_id_type=MESH,
        )

    def inward(i):
        return pltpu.make_async_remote_copy(
            src_ref=summary_ref.at[0], dst_ref=got.at[i], send_sem=sent1.at[0], recv_sem=came1.at[i],
            device_id={"sp": i}, device_id_type=MESH,
        )

    def back(i, p):
        return pltpu.make_async_remote_copy(
            src_ref=states.at[i], dst_ref=entry.at[p], send_sem=sent2.at[i], recv_sem=came2.at[p],
            device_id={"sp": i}, device_id_type=MESH,
        )

    for p in range(pairs):
        @pl.when(me != p * stride)
        def _():
            outward(p).start()

        @pl.when(me == p * stride)
        def _():
            got[me] = summary_ref[p]

    @pl.when(works)
    def _():
        def step(i, state):
            states[i] = state.astype(bf16)

            @pl.when(i != me)
            def _():
                back(i, mine).start()
                inward(i).wait_recv()

            @pl.when(i == me)
            def _():
                entry[mine] = states[i]

            high, low = halves(state)
            transit, added = got[i, 0], got[i, 1].astype(f32)
            moved = dot(transit, stacked(high)) + dot(transit, stacked(low))
            return state + (moved + added)

        lax.fori_loop(0, n, step, jnp.zeros((HEAD, LANES), f32))

    for p in range(pairs):
        @pl.when(me != p * stride)
        def _():
            back(0, p).wait_recv()

        enter_ref[p] = entry[p]

    for p in range(pairs):
        @pl.when(me != p * stride)
        def _():
            outward(p).wait_send()

    @pl.when(works)
    def _():
        def body(i, _):
            @pl.when(i != me)
            def _():
                back(i, mine).wait_send()

            return 0

        lax.fori_loop(0, n, body, 0)


def prefix_states(summary, n):
    pairs = summary.shape[0]
    return pl.pallas_call(
        functools.partial(prefix_kernel, n, pairs),
        name="prefix_states",
        out_shape=jax.ShapeDtypeStruct((pairs, HEAD, LANES), bf16),
        in_specs=[VMEM_SPEC],
        out_specs=VMEM_SPEC,
        scratch_shapes=[
            pltpu.VMEM((n, 2, HEAD, LANES), bf16),
            pltpu.VMEM((n, HEAD, LANES), bf16),
            pltpu.VMEM((pairs, HEAD, LANES), bf16),
            pltpu.SemaphoreType.DMA((pairs,)),
            pltpu.SemaphoreType.DMA((n,)),
            pltpu.SemaphoreType.DMA((n,)),
            pltpu.SemaphoreType.DMA((pairs,)),
        ],
        compiler_params=pltpu.CompilerParams(collective_id=0, has_side_effects=True),
        cost_estimate=pl.CostEstimate(flops=10**9, bytes_accessed=60 << 20, transcendentals=0),
    )(summary)


def readout_kernel(
    pairs, length, recept_ref, key_ref, value_ref, gate_ref, gain_ref, self_ref, map_ref, own_ref,
    enter_ref, out_ref,
):
    ones = head_ones()
    for p in range(pairs):
        cols = slice(p * LANES, (p + 1) * LANES)
        state = stacked(enter_ref[p])
        for start in range(0, length, 128):
            rows = slice(start, start + 128)
            value = value_ref[rows, cols].astype(f32)
            own = recept_ref[rows, cols].astype(f32) * key_ref[rows, cols].astype(f32) * self_ref[:, cols]
            own = dot_split_left(own, ones) * value
            read = dot(map_ref[rows, cols], state) + own_ref[rows, cols]
            center = read - dot_split_left(read, ones) * (1.0 / HEAD)
            spread = dot_split_left(center * center, ones) * (1.0 / HEAD)
            normed = center * lax.rsqrt(spread + GROUP_EPS) * gain_ref[:, cols]
            out_ref[rows, cols] = ((normed + own) * gate_ref[rows, cols].astype(f32)).astype(bf16)


def readout(recept, key, value, gate, gain, self_weight, maps, own, enter):
    length, width = recept.shape
    return pl.pallas_call(
        functools.partial(readout_kernel, width // LANES, length),
        name="readout",
        out_shape=jax.ShapeDtypeStruct((length, width), bf16),
        in_specs=[VMEM_SPEC] * 9,
        out_specs=VMEM_SPEC,
        cost_estimate=pl.CostEstimate(flops=10**9, bytes_accessed=16 << 20, transcendentals=0),
    )(recept, key, value, gate, gain, self_weight, maps, own, enter)


def route_columns(index_ref, experts, capacity):
    rows = index_ref.shape[0]
    lane = iota((rows, LANES), 1)
    first = lane == index_ref[:, 0:1]
    second = lane == index_ref[:, 1:2]
    square = (rows, rows)
    before = jnp.where(iota(square, 0) > iota(square, 1), 1.0, 0.0)
    both = jnp.where(first, 1.0, 0.0) + jnp.where(second, 1.0, 0.0)
    counts = dot(before, both) + (lane * capacity).astype(f32)
    return [jnp.sum(jnp.where(hit, counts, 0.0), axis=1, keepdims=True) for hit in (first, second)]


def build_kernel(experts, capacity, residual_ref, proj_ref, gain_ref, index_ref, out_ref, stack_ref):
    rows, width = residual_ref.shape
    part = width // QUARTERS
    stream = residual_ref[...].astype(f32) + proj_ref[...].astype(f32)
    scale = lax.rsqrt(jnp.mean(stream * stream, axis=1, keepdims=True) + NORM_EPS)
    ffn_in = (stream * scale * gain_ref[...]).astype(bf16)
    for q in range(QUARTERS):
        stack_ref[q * rows : (q + 1) * rows] = ffn_in[:, q * part : (q + 1) * part]
    targets = [
        jnp.broadcast_to(t, (rows, rows)).T[:1] for t in route_columns(index_ref, experts, capacity)
    ]
    block = QUARTERS * capacity
    many = BLOCK * block
    line = iota((many, 1), 0)
    device = lax.div(line, block)
    quarter = lax.div(lax.rem(line, block), capacity)
    slot = (device * capacity + lax.rem(line, capacity)).astype(f32)
    for g in range(experts // BLOCK):
        wanted = slot + float(g * BLOCK * capacity)
        hit = jnp.where((wanted == targets[0]) | (wanted == targets[1]), 1.0, 0.0)
        place = jnp.concatenate(
            [jnp.where(quarter == q, hit, 0.0) for q in range(QUARTERS)], axis=1
        ).astype(bf16)
        lines = dot(place, stack_ref[...]).astype(bf16)
        for k in range(BLOCK):
            out_ref[g * BLOCK + k] = lines[k * block : (k + 1) * block]


def build(residual, proj, gain, index, experts, capacity):
    rows, width = residual.shape
    return pl.pallas_call(
        functools.partial(build_kernel, experts, capacity),
        name="build",
        out_shape=jax.ShapeDtypeStruct((experts, QUARTERS * capacity, width // QUARTERS), bf16),
        in_specs=[VMEM_SPEC] * 4,
        out_specs=VMEM_SPEC,
        scratch_shapes=[pltpu.VMEM((QUARTERS * rows, width // QUARTERS), bf16)],
        cost_estimate=pl.CostEstimate(flops=10**9, bytes_accessed=8 << 20, transcendentals=0),
    )(residual, proj, gain, index)


def exchange_kernel(n, src_ref, out_ref, own_sem, sent, came):
    me = lax.axis_index("sp")
    barrier = pltpu.get_barrier_semaphore()

    def greet(k, _):
        pl.semaphore_signal(
            barrier, inc=1, device_id={"sp": lax.rem(me + k, n)}, device_id_type=MESH
        )
        return 0

    lax.fori_loop(1, n, greet, 0)
    own = pltpu.make_async_copy(src_ref.at[me], out_ref.at[me], own_sem)
    own.start()
    pl.semaphore_wait(barrier, n - 1)

    def copy(k):
        to = lax.rem(me + k, n)
        return pltpu.make_async_remote_copy(
            src_ref=src_ref.at[to], dst_ref=out_ref.at[me], send_sem=sent.at[k], recv_sem=came.at[k],
            device_id={"sp": to}, device_id_type=MESH,
        )

    def start(k, _):
        away = n // 2 - lax.div(k, 2)
        copy(jnp.where(lax.rem(k, 2) == 0, away, n - away)).start()
        return 0

    def arrived(k):
        frm = lax.rem(me + n - k, n)
        return pltpu.make_async_remote_copy(
            src_ref=src_ref.at[frm], dst_ref=out_ref.at[frm], send_sem=sent.at[k], recv_sem=came.at[k],
            device_id={"sp": frm}, device_id_type=MESH,
        )

    copy(n // 2).start()
    lax.fori_loop(2, n, start, 0)
    own.wait()

    def finish(k, _):
        arrived(k).wait_recv()
        copy(k).wait_send()
        return 0

    lax.fori_loop(1, n, finish, 0)


def exchange(blocks, n, number):
    return pl.pallas_call(
        functools.partial(exchange_kernel, n),
        name=f"exchange_{number}",
        out_shape=jax.ShapeDtypeStruct(blocks.shape, blocks.dtype),
        in_specs=[VMEM_SPEC],
        out_specs=VMEM_SPEC,
        scratch_shapes=[
            pltpu.SemaphoreType.DMA,
            pltpu.SemaphoreType.DMA((n,)),
            pltpu.SemaphoreType.DMA((n,)),
        ],
        compiler_params=pltpu.CompilerParams(collective_id=number, has_side_effects=True),
        cost_estimate=pl.CostEstimate(flops=10**6, bytes_accessed=200 << 20, transcendentals=0),
    )(blocks)


def reorder(capacity, to_rows):
    many = BLOCK * QUARTERS * capacity
    square = (many, many)
    out, line = (iota(square, 0), iota(square, 1)) if to_rows else (iota(square, 1), iota(square, 0))
    device, quarter = lax.div(line, QUARTERS * capacity), lax.rem(lax.div(line, capacity), QUARTERS)
    place = (quarter * BLOCK + device) * capacity + lax.rem(line, capacity)
    return jnp.where(out == place, 1.0, 0.0).astype(bf16)


def expert_kernel(n, capacity, came_ref, gate_ref, up_ref, down_ref, out_ref, rows_ref, total_ref):
    j = pl.program_id(0)
    block = QUARTERS * capacity
    height = BLOCK * capacity
    part = rows_ref.shape[1] // QUARTERS

    @pl.when(j == 0)
    def _():
        order = reorder(capacity, True)
        for g in range(n // BLOCK):
            lines = jnp.concatenate([came_ref[g * BLOCK + k] for k in range(BLOCK)], axis=0)
            moved = dot(order, lines).astype(bf16)
            for q in range(QUARTERS):
                rows_ref[g * height : (g + 1) * height, q * part : (q + 1) * part] = moved[
                    q * height : (q + 1) * height
                ]
        total_ref[...] = jnp.zeros_like(total_ref)

    gated = dot(rows_ref[...], gate_ref[0])
    upward = dot(rows_ref[...], up_ref[0])
    hidden = (gated * sigmoid(gated) * upward).astype(bf16)
    total_ref[...] += dot(hidden, down_ref[0])

    @pl.when(j == pl.num_programs(0) - 1)
    def _():
        order = reorder(capacity, False)
        for g in range(n // BLOCK):
            rows = slice(g * height, (g + 1) * height)
            lines = jnp.concatenate(
                [total_ref[rows, q * part : (q + 1) * part] for q in range(QUARTERS)], axis=0
            )
            moved = dot(order, lines).astype(bf16)
            for k in range(BLOCK):
                out_ref[g * BLOCK + k] = moved[k * block : (k + 1) * block]


def expert_rows(came, gate, up, down, capacity):
    n, block, part = came.shape
    pieces, width, units = gate.shape
    whole = pl.BlockSpec((n, block, part), lambda j: (0, 0, 0))
    return pl.pallas_call(
        functools.partial(expert_kernel, n, capacity),
        name="expert_rows",
        grid=(pieces,),
        out_shape=jax.ShapeDtypeStruct(came.shape, bf16),
        in_specs=[
            whole,
            pl.BlockSpec((1, width, units), lambda j: (j, 0, 0)),
            pl.BlockSpec((1, width, units), lambda j: (j, 0, 0)),
            pl.BlockSpec((1, units, width), lambda j: (j, 0, 0)),
        ],
        out_specs=whole,
        scratch_shapes=[
            pltpu.VMEM((n * capacity, width), bf16),
            pltpu.VMEM((n * capacity, width), f32),
        ],
        compiler_params=pltpu.CompilerParams(
            dimension_semantics=("arbitrary",), vmem_limit_bytes=40 << 20
        ),
        cost_estimate=pl.CostEstimate(flops=5 * 10**9, bytes_accessed=16 << 20, transcendentals=0),
    )(came, gate, up, down)


def combine_kernel(n, capacity, residual_ref, proj_ref, index_ref, weight_ref, back_ref, out_ref, rows_ref):
    rows, width = residual_ref.shape
    part = width // QUARTERS
    height = BLOCK * capacity
    order = reorder(capacity, True)
    for g in range(n // BLOCK):
        lines = jnp.concatenate([back_ref[g * BLOCK + k] for k in range(BLOCK)], axis=0)
        moved = dot(order, lines).astype(bf16)
        for q in range(QUARTERS):
            rows_ref[g * height : (g + 1) * height, q * part : (q + 1) * part] = moved[
                q * height : (q + 1) * height
            ]
    targets = route_columns(index_ref, n, capacity)
    slot = iota((rows, n * capacity), 1).astype(f32)
    mix = jnp.where(slot == targets[0], weight_ref[:, 0:1], 0.0) + jnp.where(
        slot == targets[1], weight_ref[:, 1:2], 0.0
    )
    high, low = halves(mix)
    for q in range(QUARTERS):
        cols = slice(q * part, (q + 1) * part)
        routed = dot(high, rows_ref[:, cols]) + dot(low, rows_ref[:, cols])
        stream = residual_ref[:, cols].astype(f32) + proj_ref[:, cols].astype(f32)
        out_ref[:, cols] = (stream + routed).astype(bf16)


def combine(residual, proj, index, weight, back, capacity):
    n = back.shape[0]
    return pl.pallas_call(
        functools.partial(combine_kernel, n, capacity),
        name="combine",
        out_shape=jax.ShapeDtypeStruct(residual.shape, bf16),
        in_specs=[VMEM_SPEC] * 5,
        out_specs=VMEM_SPEC,
        scratch_shapes=[pltpu.VMEM((n * capacity, residual.shape[1]), bf16)],
        cost_estimate=pl.CostEstimate(flops=10**9, bytes_accessed=8 << 20, transcendentals=0),
    )(residual, proj, index, weight, back)


def local(
    recept, key_input, value_input, output_gate_input, decay_input_part, correction_rate_input,
    head_decay_offset, decay_fixed_bias, correction_rate_bias, head_norm_gain, self_term_weight,
    output_weight_matrix, residual, feedforward_norm_gain, routed_expert_index, routed_expert_weight,
    gate_weight_experts, up_weight_experts, down_weight_experts,
):
    n = lax.axis_size("sp")
    out_weight = lax.all_gather(output_weight_matrix, "tp")
    gate = lax.all_gather(gate_weight_experts[0], "tp")
    up = lax.all_gather(up_weight_experts[0], "tp")
    down = lax.all_gather(down_weight_experts[0], "tp")

    summary, maps, own = mixer_local(
        recept, key_input, value_input, decay_input_part, correction_rate_input, head_decay_offset,
        decay_fixed_bias[None], correction_rate_bias[None],
    )
    enter = prefix_states(summary, n)
    mixed = readout(
        recept, key_input, value_input, output_gate_input, head_norm_gain[None], self_term_weight[None],
        maps, own, enter,
    )
    shares = mixed.reshape(lax.axis_size("tp"), -1, mixed.shape[1])
    shares = lax.all_to_all(shares, "tp", split_axis=0, concat_axis=0, tiled=True)
    proj = jnp.einsum("jrc,jcd->rd", shares, out_weight, preferred_element_type=f32).astype(bf16)

    rows = residual.shape[0]
    experts = gate_weight_experts.shape[0] * n
    capacity = 3 * rows // experts
    outgoing = build(residual, proj, feedforward_norm_gain[None], routed_expert_index, experts, capacity)
    came = exchange(outgoing, n, 1)
    results = expert_rows(came, gate, up, down, capacity)
    back = exchange(results, n, 2)
    return combine(residual, proj, routed_expert_index, routed_expert_weight, back, capacity)


def solution(mesh):
    shared = P(("grp", "sp", "tp"), None)
    split = P(("grp", "sp"), "tp")
    return jax.shard_map(
        local,
        mesh=mesh,
        in_specs=(split,) * 7 + (P("tp"),) * 4 + (P("tp", None), shared, P(), shared, shared)
        + (P("sp", None, "tp"), P("sp", None, "tp"), P("sp", "tp", None)),
        out_specs=shared,
        check_vma=False,
    )
```

```python
import functools

import jax
import jax.numpy as jnp
from jax import lax
from jax.experimental import pallas as pl
from jax.experimental.pallas import tpu as pltpu
from jax.sharding import PartitionSpec as P

f32, bf16 = jnp.float32, jnp.bfloat16
MESH = pl.DeviceIdType.MESH
NN = (((1,), (0,)), ((), ()))
NT = (((1,), (1,)), ((), ()))
GROUP_EPS = 0.00064
NORM_EPS = 1e-06
SPAN = 64
LANES = 128
HEAD = 64
DECAY_SCALE = 0.6065306597126334
QUARTERS = 4
BLOCK = 4
VMEM_SPEC = pl.BlockSpec(memory_space=pltpu.VMEM)


def dot(a, b, dims=NN):
    return lax.dot_general(a.astype(bf16), b.astype(bf16), dims, preferred_element_type=f32)


def halves(x):
    high = x.astype(bf16)
    return high, (x - high.astype(f32)).astype(bf16)


def dot_split_left(a, b):
    high, low = halves(a)
    return dot(high, b) + dot(low, b)


def dot_split_right(a, b):
    high, low = halves(b)
    return dot(a, high) + dot(a, low)


def iota(shape, dim):
    return lax.broadcasted_iota(jnp.int32, shape, dim)


def sigmoid(x):
    return 1.0 / (1.0 + jnp.exp(-x))


def head_ones():
    shape = (LANES, LANES)
    return jnp.where((iota(shape, 0) >> 6) == (iota(shape, 1) >> 6), 1.0, 0.0).astype(bf16)


def stacked(x):
    first = iota(x.shape, 1) < HEAD
    zero = jnp.zeros_like(x)
    return jnp.concatenate([jnp.where(first, x, zero), jnp.where(first, zero, x)], axis=0)


def chunk_maps(units):
    row = iota((SPAN, LANES), 0)
    col = iota((SPAN, LANES), 1) & (HEAD - 1)
    square = (SPAN, SPAN)
    lower = jnp.where(iota(square, 0) >= iota(square, 1), 1.0, 0.0).astype(bf16)
    ones = head_ones()

    def each(work, *lists):
        return [work(*parts) for parts in zip(*lists)]

    def elementwise(recept, key, value, decay_pre, rate_pre, offset, decay_bias, rate_bias):
        decay_log = offset - DECAY_SCALE * sigmoid(decay_bias + decay_pre.astype(f32))
        key = key.astype(f32)
        return decay_log, dot_split_right(lower, decay_log), dot_split_left(key * key, ones)

    def scaled(unit, first):
        recept, key, value, decay_pre, rate_pre, offset, decay_bias, rate_bias = unit
        decay_log, cumul, norm = first
        key = key.astype(f32)
        rate = sigmoid(rate_bias + rate_pre.astype(f32))
        unit_key = key * lax.rsqrt(norm + NORM_EPS)
        middle = cumul[SPAN // 2 - 1 : SPAN // 2, :]
        rel = cumul - middle
        rise, fall = jnp.exp(rel), jnp.exp(-rel)
        to_middle = jnp.exp(middle)
        to_end = jnp.exp(cumul[SPAN - 1 : SPAN, :] - middle)
        remove = -unit_key * jnp.exp(rel - decay_log)
        read = recept.astype(f32) * rise
        write = unit_key * rate * fall
        keys = key * fall
        left = jnp.concatenate([remove.astype(bf16), read.astype(bf16)], axis=0)
        right = jnp.concatenate([stacked(write.astype(bf16)), stacked(keys.astype(bf16))], axis=0)
        from_start = [(remove * to_middle).astype(bf16), (read * to_middle).astype(bf16)]
        write_end = jnp.concatenate([write * to_end, keys * to_end], axis=0).T.astype(bf16)
        ending = jnp.broadcast_to(to_end * to_middle, (LANES, LANES)).T
        return dot(left, right, NT), from_start, write_end, ending

    first = [elementwise(*unit) for unit in units]
    second = each(scaled, units, first)
    scores = [item[0] for item in second]
    strict, within = row > col, row >= col

    def merging(level):
        size = 1 << level
        same = (row >> (level + 1)) == (col >> (level + 1))
        return same & ((row & size) != 0) & ((col & size) == 0)

    lower_part = [jnp.where(strict, s[:SPAN, :LANES], 0.0).astype(bf16) for s in scores]
    remove_key = [jnp.where(strict, s[:SPAN, LANES:], 0.0).astype(bf16) for s in scores]
    within_maps = [
        jnp.where(
            jnp.concatenate([within, within], axis=1), s[SPAN:], 0.0
        ).astype(bf16)
        for s in scores
    ]
    removed_value = [dot(m, stacked(unit[2])).astype(bf16) for m, unit in zip(remove_key, units)]
    inverse = [jnp.where(row == col, 1.0, jnp.where(merging(0), m.astype(f32), 0.0)) for m in lower_part]
    for level in range(1, SPAN.bit_length() - 1):
        chosen = merging(level)
        inner = [
            dot(jnp.where(chosen, m, jnp.zeros_like(m)), stacked(x.astype(bf16)))
            for m, x in zip(lower_part, inverse)
        ]
        inverse = [x + dot(x, stacked(y.astype(bf16))) for x, y in zip(inverse, inner)]
    solved = [
        dot(x, jnp.concatenate([stacked(item[1][0]), stacked(v)], axis=1))
        for x, item, v in zip(inverse, second, removed_value)
    ]
    return [
        (jnp.concatenate([q[:, :LANES].astype(bf16), item[1][1]], axis=0), q[:, LANES:], maps) + item[2:]
        for q, item, maps in zip(solved, second, within_maps)
    ]


def mixer_kernel(
    pairs, chunks,
    recept_ref, key_ref, value_ref, decay_ref, rate_ref, offset_ref, decay_bias_ref, rate_bias_ref,
    summary_ref, map_ref, own_ref,
    left_ref, solved_ref, within_ref, write_ref, ending_ref, state_ref, removed_ref, partial_ref,
):
    first_head = iota((SPAN, LANES), 1) < HEAD

    def rows_of(c):
        return pl.ds(pl.multiple_of(c * SPAN, SPAN), SPAN)

    unroll = 2 if chunks % 2 == 0 else 1

    def prepare(i, _):
        places = [(i * unroll + k, p) for k in range(unroll) for p in range(pairs)]
        units = []
        for c, p in places:
            rows, cols = rows_of(c), slice(p * LANES, (p + 1) * LANES)
            offset = jnp.where(
                first_head, offset_ref[rows, 2 * p : 2 * p + 1], offset_ref[rows, 2 * p + 1 : 2 * p + 2]
            )
            units.append(
                (
                    recept_ref[rows, cols], key_ref[rows, cols], value_ref[rows, cols],
                    decay_ref[rows, cols], rate_ref[rows, cols], offset,
                    decay_bias_ref[:, cols], rate_bias_ref[:, cols],
                )
            )
        for (c, p), (left, solved, within, write, ending) in zip(places, chunk_maps(units)):
            left_ref[c, p] = left
            solved_ref[c, p] = solved
            within_ref[c, p] = within
            write_ref[c, p] = write
            ending_ref[c, p] = ending
        return 0

    lax.fori_loop(0, chunks // unroll, prepare, 0)

    square = (LANES, LANES)
    eye = jnp.where(iota(square, 0) == iota(square, 1), 1.0, 0.0)
    for p in range(pairs):
        state_ref[p, :, :LANES] = eye
        state_ref[p, :, LANES:] = jnp.zeros(square, f32)
    own_block = (iota((LANES, 2 * LANES), 0) >> 6) == ((iota((LANES, 2 * LANES), 1) >> 6) & 1)

    def advance(c, _):
        rows = rows_of(c)
        states = [state_ref[p] for p in range(pairs)]
        crossed = [dot(left_ref[c, p], states[p]) for p in range(pairs)]
        removed = [
            jnp.concatenate(
                [x[:SPAN, :LANES], x[:SPAN, LANES:] + solved_ref[c, p]], axis=1
            ).astype(bf16)
            for p, x in enumerate(crossed)
        ]
        updates = []
        for p in range(pairs):
            value = value_ref[rows, p * LANES : (p + 1) * LANES]
            right = jnp.concatenate(
                [removed[p], jnp.concatenate([jnp.zeros_like(value), value], axis=1)], axis=0
            )
            updates.append(dot(write_ref[c, p], right))
        for p in range(pairs):
            removed_ref[c, p] = removed[p]
            partial_ref[c, p] = crossed[p][SPAN:]
            ending = ending_ref[c, p]
            state_ref[p] = states[p] * jnp.concatenate([ending, ending], axis=1) + jnp.where(
                own_block, updates[p], 0.0
            )
        return 0

    lax.fori_loop(0, chunks, advance, 0)

    for p in range(pairs):
        transit = state_ref[p, :, :LANES] - eye
        added = state_ref[p, :, LANES:]
        summary_ref[p, 0] = (transit[:HEAD] + transit[HEAD:]).astype(bf16)
        summary_ref[p, 1] = (added[:HEAD] + added[HEAD:]).astype(bf16)

    def emit(c, _):
        rows = rows_of(c)
        for p in range(pairs):
            cols = slice(p * LANES, (p + 1) * LANES)
            removed = removed_ref[c, p]
            value = stacked(value_ref[rows, cols])
            right = jnp.concatenate(
                [
                    jnp.concatenate([stacked(removed[:, :LANES]), stacked(removed[:, LANES:])], axis=1),
                    jnp.concatenate([jnp.zeros_like(value), value], axis=1),
                ],
                axis=0,
            )
            both = partial_ref[c, p] + dot(within_ref[c, p], right)
            map_ref[rows, cols] = both[:, :LANES].astype(bf16)
            own_ref[rows, cols] = both[:, LANES:]
        return 0

    lax.fori_loop(0, chunks, emit, 0)


def mixer_local(recept, key, value, decay, rate, offset, decay_bias, rate_bias):
    length, width = recept.shape
    pairs, chunks = width // LANES, length // SPAN
    per = (chunks, pairs)
    return pl.pallas_call(
        functools.partial(mixer_kernel, pairs, chunks),
        name="mixer_local",
        out_shape=(
            jax.ShapeDtypeStruct((pairs, 2, HEAD, LANES), bf16),
            jax.ShapeDtypeStruct((length, width), bf16),
            jax.ShapeDtypeStruct((length, width), f32),
        ),
        in_specs=[VMEM_SPEC] * 8,
        out_specs=(VMEM_SPEC,) * 3,
        scratch_shapes=[
            pltpu.VMEM(per + (2 * SPAN, LANES), bf16),
            pltpu.VMEM(per + (SPAN, LANES), f32),
            pltpu.VMEM(per + (SPAN, 2 * LANES), bf16),
            pltpu.VMEM(per + (LANES, 2 * SPAN), bf16),
            pltpu.VMEM(per + (LANES, LANES), f32),
            pltpu.VMEM((pairs, LANES, 2 * LANES), f32),
            pltpu.VMEM(per + (SPAN, 2 * LANES), bf16),
            pltpu.VMEM(per + (SPAN, 2 * LANES), f32),
        ],
        cost_estimate=pl.CostEstimate(
            flops=80 * 2 * LANES * length * width, bytes_accessed=12 * length * width, transcendentals=0
        ),
    )(recept, key, value, decay, rate, offset, decay_bias, rate_bias)


def prefix_kernel(n, pairs, summary_ref, enter_ref, got, states, entry, sent1, came1, sent2, came2):
    me = lax.axis_index("sp")
    stride = n // pairs
    works = lax.rem(me, stride) == 0
    mine = lax.div(me, stride)
    barrier = pltpu.get_barrier_semaphore()

    def greet(device):
        pl.semaphore_signal(barrier, inc=1, device_id={"sp": device}, device_id_type=MESH)

    @pl.when(works)
    def _():
        def body(j, _):
            greet(lax.rem(me + j, n))
            return 0

        lax.fori_loop(1, n, body, 0)
        pl.semaphore_wait(barrier, n - 1)

    @pl.when(jnp.logical_not(works))
    def _():
        for p in range(pairs):
            greet(p * stride)
        pl.semaphore_wait(barrier, pairs)

    def outward(p):
        return pltpu.make_async_remote_copy(
            src_ref=summary_ref.at[p], dst_ref=got.at[me], send_sem=sent1.at[p], recv_sem=came1.at[me],
            device_id={"sp": p * stride}, device_id_type=MESH,
        )

    def inward(i):
        return pltpu.make_async_remote_copy(
            src_ref=summary_ref.at[0], dst_ref=got.at[i], send_sem=sent1.at[0], recv_sem=came1.at[i],
            device_id={"sp": i}, device_id_type=MESH,
        )

    def back(i, p):
        return pltpu.make_async_remote_copy(
            src_ref=states.at[i], dst_ref=entry.at[p], send_sem=sent2.at[i], recv_sem=came2.at[p],
            device_id={"sp": i}, device_id_type=MESH,
        )

    for p in range(pairs):
        @pl.when(me != p * stride)
        def _():
            outward(p).start()

        @pl.when(me == p * stride)
        def _():
            got[me] = summary_ref[p]

    @pl.when(works)
    def _():
        def step(i, state):
            states[i] = state.astype(bf16)

            @pl.when(i != me)
            def _():
                back(i, mine).start()
                inward(i).wait_recv()

            @pl.when(i == me)
            def _():
                entry[mine] = states[i]

            high, low = halves(state)
            transit, added = got[i, 0], got[i, 1].astype(f32)
            moved = dot(transit, stacked(high)) + dot(transit, stacked(low))
            return state + (moved + added)

        lax.fori_loop(0, n, step, jnp.zeros((HEAD, LANES), f32))

    for p in range(pairs):
        @pl.when(me != p * stride)
        def _():
            back(0, p).wait_recv()

        enter_ref[p] = entry[p]

    for p in range(pairs):
        @pl.when(me != p * stride)
        def _():
            outward(p).wait_send()

    @pl.when(works)
    def _():
        def body(i, _):
            @pl.when(i != me)
            def _():
                back(i, mine).wait_send()

            return 0

        lax.fori_loop(0, n, body, 0)


def prefix_states(summary, n):
    pairs = summary.shape[0]
    return pl.pallas_call(
        functools.partial(prefix_kernel, n, pairs),
        name="prefix_states",
        out_shape=jax.ShapeDtypeStruct((pairs, HEAD, LANES), bf16),
        in_specs=[VMEM_SPEC],
        out_specs=VMEM_SPEC,
        scratch_shapes=[
            pltpu.VMEM((n, 2, HEAD, LANES), bf16),
            pltpu.VMEM((n, HEAD, LANES), bf16),
            pltpu.VMEM((pairs, HEAD, LANES), bf16),
            pltpu.SemaphoreType.DMA((pairs,)),
            pltpu.SemaphoreType.DMA((n,)),
            pltpu.SemaphoreType.DMA((n,)),
            pltpu.SemaphoreType.DMA((pairs,)),
        ],
        compiler_params=pltpu.CompilerParams(collective_id=0, has_side_effects=True),
        cost_estimate=pl.CostEstimate(flops=10**9, bytes_accessed=60 << 20, transcendentals=0),
    )(summary)


def readout_kernel(
    pairs, length, recept_ref, key_ref, value_ref, gate_ref, gain_ref, self_ref, map_ref, own_ref,
    enter_ref, out_ref,
):
    ones = head_ones()
    for p in range(pairs):
        cols = slice(p * LANES, (p + 1) * LANES)
        state = stacked(enter_ref[p])
        for start in range(0, length, 128):
            rows = slice(start, start + 128)
            value = value_ref[rows, cols].astype(f32)
            own = recept_ref[rows, cols].astype(f32) * key_ref[rows, cols].astype(f32) * self_ref[:, cols]
            own = dot_split_left(own, ones) * value
            read = dot(map_ref[rows, cols], state) + own_ref[rows, cols]
            center = read - dot_split_left(read, ones) * (1.0 / HEAD)
            spread = dot_split_left(center * center, ones) * (1.0 / HEAD)
            normed = center * lax.rsqrt(spread + GROUP_EPS) * gain_ref[:, cols]
            out_ref[rows, cols] = ((normed + own) * gate_ref[rows, cols].astype(f32)).astype(bf16)


def readout(recept, key, value, gate, gain, self_weight, maps, own, enter):
    length, width = recept.shape
    return pl.pallas_call(
        functools.partial(readout_kernel, width // LANES, length),
        name="readout",
        out_shape=jax.ShapeDtypeStruct((length, width), bf16),
        in_specs=[VMEM_SPEC] * 9,
        out_specs=VMEM_SPEC,
        cost_estimate=pl.CostEstimate(flops=10**9, bytes_accessed=16 << 20, transcendentals=0),
    )(recept, key, value, gate, gain, self_weight, maps, own, enter)


def route_columns(index_ref, experts, capacity):
    rows = index_ref.shape[0]
    lane = iota((rows, LANES), 1)
    first = lane == index_ref[:, 0:1]
    second = lane == index_ref[:, 1:2]
    square = (rows, rows)
    before = jnp.where(iota(square, 0) > iota(square, 1), 1.0, 0.0)
    both = jnp.where(first, 1.0, 0.0) + jnp.where(second, 1.0, 0.0)
    counts = dot(before, both) + (lane * capacity).astype(f32)
    return [jnp.sum(jnp.where(hit, counts, 0.0), axis=1, keepdims=True) for hit in (first, second)]


def build_kernel(experts, capacity, residual_ref, proj_ref, gain_ref, index_ref, out_ref, stack_ref):
    rows, width = residual_ref.shape
    part = width // QUARTERS
    proj = jnp.concatenate([proj_ref[0], proj_ref[1]], axis=1)
    stream = residual_ref[...].astype(f32) + proj.astype(f32)
    scale = lax.rsqrt(jnp.mean(stream * stream, axis=1, keepdims=True) + NORM_EPS)
    ffn_in = (stream * scale * gain_ref[...]).astype(bf16)
    for q in range(QUARTERS):
        stack_ref[q * rows : (q + 1) * rows] = ffn_in[:, q * part : (q + 1) * part]
    targets = [
        jnp.broadcast_to(t, (rows, rows)).T[:1] for t in route_columns(index_ref, experts, capacity)
    ]
    block = QUARTERS * capacity
    many = BLOCK * block
    line = iota((many, 1), 0)
    device = lax.div(line, block)
    quarter = lax.div(lax.rem(line, block), capacity)
    slot = (device * capacity + lax.rem(line, capacity)).astype(f32)
    for g in range(experts // BLOCK):
        wanted = slot + float(g * BLOCK * capacity)
        hit = jnp.where((wanted == targets[0]) | (wanted == targets[1]), 1.0, 0.0)
        place = jnp.concatenate(
            [jnp.where(quarter == q, hit, 0.0) for q in range(QUARTERS)], axis=1
        ).astype(bf16)
        lines = dot(place, stack_ref[...]).astype(bf16)
        for k in range(BLOCK):
            out_ref[g * BLOCK + k] = lines[k * block : (k + 1) * block]


def build(residual, proj, gain, index, experts, capacity):
    rows, width = residual.shape
    return pl.pallas_call(
        functools.partial(build_kernel, experts, capacity),
        name="build",
        out_shape=jax.ShapeDtypeStruct((experts, QUARTERS * capacity, width // QUARTERS), bf16),
        in_specs=[VMEM_SPEC] * 4,
        out_specs=VMEM_SPEC,
        scratch_shapes=[pltpu.VMEM((QUARTERS * rows, width // QUARTERS), bf16)],
        cost_estimate=pl.CostEstimate(flops=10**9, bytes_accessed=8 << 20, transcendentals=0),
    )(residual, proj, gain, index)


def exchange_kernel(n, src_ref, out_ref, own_sem, sent, came):
    me = lax.axis_index("sp")
    barrier = pltpu.get_barrier_semaphore()

    def greet(k, _):
        pl.semaphore_signal(
            barrier, inc=1, device_id={"sp": lax.rem(me + k, n)}, device_id_type=MESH
        )
        return 0

    lax.fori_loop(1, n, greet, 0)
    own = pltpu.make_async_copy(src_ref.at[me], out_ref.at[me], own_sem)
    own.start()
    pl.semaphore_wait(barrier, n - 1)

    def copy(k):
        to = lax.rem(me + k, n)
        return pltpu.make_async_remote_copy(
            src_ref=src_ref.at[to], dst_ref=out_ref.at[me], send_sem=sent.at[k], recv_sem=came.at[k],
            device_id={"sp": to}, device_id_type=MESH,
        )

    def start(k, _):
        away = n // 2 - lax.div(k, 2)
        copy(jnp.where(lax.rem(k, 2) == 0, away, n - away)).start()
        return 0

    def arrived(k):
        frm = lax.rem(me + n - k, n)
        return pltpu.make_async_remote_copy(
            src_ref=src_ref.at[frm], dst_ref=out_ref.at[frm], send_sem=sent.at[k], recv_sem=came.at[k],
            device_id={"sp": frm}, device_id_type=MESH,
        )

    copy(n // 2).start()
    lax.fori_loop(2, n, start, 0)
    own.wait()

    def finish(k, _):
        arrived(k).wait_recv()
        copy(k).wait_send()
        return 0

    lax.fori_loop(1, n, finish, 0)


def other_core(me):
    return me + 1 - 2 * lax.rem(me, 2)


def spread_kernel(m, src_ref, out_ref, own_sem, sent, came, pass_sent, pass_came):
    me, col = lax.axis_index("sp"), lax.axis_index("tp")
    core, partner = lax.rem(me, 2), other_core(me)
    barrier = pltpu.get_barrier_semaphore()
    pl.semaphore_signal(barrier, inc=1, device_id={"sp": partner}, device_id_type=MESH)
    for k in range(1, m):
        pl.semaphore_signal(
            barrier, inc=1, device_id={"tp": lax.rem(col + k, m)}, device_id_type=MESH
        )
    own = pltpu.make_async_copy(src_ref.at[col], out_ref.at[core, col], own_sem)
    own.start()
    pl.semaphore_wait(barrier, m)

    def send(k):
        to = lax.rem(col + k, m)
        return pltpu.make_async_remote_copy(
            src_ref=src_ref.at[to], dst_ref=out_ref.at[core, col], send_sem=sent.at[k],
            recv_sem=came.at[k], device_id={"tp": to}, device_id_type=MESH,
        )

    def arrival(k):
        frm = lax.rem(col + m - k, m)
        return pltpu.make_async_remote_copy(
            src_ref=src_ref.at[frm], dst_ref=out_ref.at[core, frm], send_sem=sent.at[k],
            recv_sem=came.at[k], device_id={"tp": frm}, device_id_type=MESH,
        )

    def onward(k, source):
        frm = lax.rem(col + m - k, m)
        return pltpu.make_async_remote_copy(
            src_ref=source, dst_ref=out_ref.at[core, frm], send_sem=pass_sent.at[k],
            recv_sem=pass_came.at[k], device_id={"sp": partner}, device_id_type=MESH,
        )

    def from_partner(k):
        frm = lax.rem(col + m - k, m)
        return pltpu.make_async_remote_copy(
            src_ref=src_ref.at[frm], dst_ref=out_ref.at[1 - core, frm], send_sem=pass_sent.at[k],
            recv_sem=pass_came.at[k], device_id={"sp": partner}, device_id_type=MESH,
        )

    order = [m // 2] + [k for k in range(1, m) if k != m // 2]
    for k in order:
        send(k).start()
    onward(0, src_ref.at[col]).start()
    passed = [k for k in range(1, m) if k != m // 2] + [m // 2]
    for k in passed:
        arrival(k).wait_recv()
        onward(k, out_ref.at[core, lax.rem(col + m - k, m)]).start()
    own.wait()
    for k in range(m):
        from_partner(k).wait_recv()
        onward(k, src_ref.at[col]).wait_send()
    for k in range(1, m):
        send(k).wait_send()


def spread(blocks, m, number):
    return pl.pallas_call(
        functools.partial(spread_kernel, m),
        name="spread",
        out_shape=jax.ShapeDtypeStruct((2,) + blocks.shape, blocks.dtype),
        in_specs=[VMEM_SPEC],
        out_specs=VMEM_SPEC,
        scratch_shapes=[pltpu.SemaphoreType.DMA] + [pltpu.SemaphoreType.DMA((m,))] * 4,
        compiler_params=pltpu.CompilerParams(collective_id=number, has_side_effects=True),
        cost_estimate=pl.CostEstimate(flops=10**6, bytes_accessed=40 << 20, transcendentals=0),
    )(blocks)


def swap_kernel(src_ref, out_ref, own_sem, sent, came):
    me = lax.axis_index("sp")
    core, partner = lax.rem(me, 2), other_core(me)
    barrier = pltpu.get_barrier_semaphore()
    pl.semaphore_signal(barrier, inc=1, device_id={"sp": partner}, device_id_type=MESH)
    own = pltpu.make_async_copy(src_ref.at[core], out_ref.at[core], own_sem)
    own.start()
    pl.semaphore_wait(barrier, 1)
    away = pltpu.make_async_remote_copy(
        src_ref=src_ref.at[1 - core], dst_ref=out_ref.at[core], send_sem=sent, recv_sem=came,
        device_id={"sp": partner}, device_id_type=MESH,
    )
    away.start()
    own.wait()
    pltpu.make_async_remote_copy(
        src_ref=src_ref.at[1 - core], dst_ref=out_ref.at[1 - core], send_sem=sent, recv_sem=came,
        device_id={"sp": partner}, device_id_type=MESH,
    ).wait_recv()
    away.wait_send()


def swap(blocks, number):
    return pl.pallas_call(
        swap_kernel,
        name="swap",
        out_shape=jax.ShapeDtypeStruct(blocks.shape, blocks.dtype),
        in_specs=[VMEM_SPEC],
        out_specs=VMEM_SPEC,
        scratch_shapes=[pltpu.SemaphoreType.DMA] * 3,
        compiler_params=pltpu.CompilerParams(collective_id=number, has_side_effects=True),
        cost_estimate=pl.CostEstimate(flops=10**6, bytes_accessed=4 << 20, transcendentals=0),
    )(blocks)


def exchange_gather_kernel(n, m, src_ref, first_ref, second_ref, out_ref, first_all, second_all,
                           stage, own_sem, sent, came, in_sem, out_sem, ring_sent, ring_came, pass_sent, pass_came):
    me, col = lax.axis_index("sp"), lax.axis_index("tp")
    right, left = lax.rem(col + 1, m), lax.rem(col + m - 1, m)
    shards, wholes = (first_ref, second_ref), (first_all, second_all)
    barrier = pltpu.get_barrier_semaphore()

    def greet(k, _):
        pl.semaphore_signal(
            barrier, inc=1, device_id={"sp": lax.rem(me + k, n)}, device_id_type=MESH
        )
        return 0

    for side in (left, right):
        pl.semaphore_signal(barrier, inc=1, device_id={"tp": side}, device_id_type=MESH)
    lax.fori_loop(1, n, greet, 0)
    own = pltpu.make_async_copy(src_ref.at[me], out_ref.at[me], own_sem)
    own.start()
    loads = [pltpu.make_async_copy(shards[a], stage.at[a], in_sem.at[a]) for a in range(2)]
    stores = [pltpu.make_async_copy(stage.at[a], wholes[a].at[col], out_sem.at[a]) for a in range(2)]
    for load in loads:
        load.start()
    for load in loads:
        load.wait()
    pl.semaphore_wait(barrier, n + 1)

    def copy(k):
        to = lax.rem(me + k, n)
        return pltpu.make_async_remote_copy(
            src_ref=src_ref.at[to], dst_ref=out_ref.at[me], send_sem=sent.at[k], recv_sem=came.at[k],
            device_id={"sp": to}, device_id_type=MESH,
        )

    def start(k, _):
        away = n // 2 - lax.div(k, 2)
        copy(jnp.where(lax.rem(k, 2) == 0, away, n - away)).start()
        return 0

    def arrived(k):
        frm = lax.rem(me + n - k, n)
        return pltpu.make_async_remote_copy(
            src_ref=src_ref.at[frm], dst_ref=out_ref.at[frm], send_sem=sent.at[k], recv_sem=came.at[k],
            device_id={"sp": frm}, device_id_type=MESH,
        )

    half = first_ref.shape[0] // 2

    def rows(h):
        return pl.ds(h * half, half)

    def hop(a, d, h):
        return pltpu.make_async_remote_copy(
            src_ref=stage.at[a, rows(h)], dst_ref=wholes[a].at[col, rows(h)],
            send_sem=ring_sent.at[a, d, h], recv_sem=ring_came.at[a, d, h],
            device_id={"tp": (right, left)[d]}, device_id_type=MESH,
        )

    def hop_in(a, d, h):
        frm = (left, right)[d]
        return pltpu.make_async_remote_copy(
            src_ref=stage.at[a, rows(h)], dst_ref=wholes[a].at[frm, rows(h)],
            send_sem=ring_sent.at[a, d, h], recv_sem=ring_came.at[a, d, h],
            device_id={"tp": frm}, device_id_type=MESH,
        )

    def onward(a, d):
        frm = (left, right)[d]
        return pltpu.make_async_remote_copy(
            src_ref=wholes[a].at[frm, rows(d)], dst_ref=wholes[a].at[frm, rows(d)],
            send_sem=pass_sent.at[a, d], recv_sem=pass_came.at[a, d],
            device_id={"tp": (right, left)[d]}, device_id_type=MESH,
        )

    def onward_in(a, d):
        frm = lax.rem(col + 2, m)
        return pltpu.make_async_remote_copy(
            src_ref=wholes[a].at[frm, rows(d)], dst_ref=wholes[a].at[frm, rows(d)],
            send_sem=pass_sent.at[a, d], recv_sem=pass_came.at[a, d],
            device_id={"tp": (left, right)[d]}, device_id_type=MESH,
        )

    copy(n // 2).start()
    lax.fori_loop(2, n, start, 0)
    for a in range(2):
        for d, h in ((0, 0), (1, 1), (0, 1), (1, 0)):
            hop(a, d, h).start()
    for store in stores:
        store.start()
    for a in range(2):
        for d in range(2):
            hop_in(a, d, d).wait_recv()
            onward(a, d).start()
    own.wait()
    for store in stores:
        store.wait()

    def finish(k, _):
        arrived(k).wait_recv()
        copy(k).wait_send()
        return 0

    lax.fori_loop(1, n, finish, 0)
    for a in range(2):
        for d in range(2):
            hop_in(a, d, 1 - d).wait_recv()
            onward_in(a, d).wait_recv()
            onward(a, d).wait_send()
            for h in range(2):
                hop(a, d, h).wait_send()


def exchange_and_gather(blocks, first, second, n, m, number):
    any_spec = pl.BlockSpec(memory_space=pl.ANY)
    whole = jax.ShapeDtypeStruct((m,) + first.shape, first.dtype)
    return pl.pallas_call(
        functools.partial(exchange_gather_kernel, n, m),
        name=f"exchange_{number}",
        out_shape=(jax.ShapeDtypeStruct(blocks.shape, blocks.dtype), whole, whole),
        in_specs=[VMEM_SPEC, any_spec, any_spec],
        out_specs=(VMEM_SPEC, any_spec, any_spec),
        scratch_shapes=[
            pltpu.VMEM((2,) + first.shape, first.dtype),
            pltpu.SemaphoreType.DMA,
            pltpu.SemaphoreType.DMA((n,)),
            pltpu.SemaphoreType.DMA((n,)),
            pltpu.SemaphoreType.DMA((2,)),
            pltpu.SemaphoreType.DMA((2,)),
            pltpu.SemaphoreType.DMA((2, 2, 2)),
            pltpu.SemaphoreType.DMA((2, 2, 2)),
            pltpu.SemaphoreType.DMA((2, 2)),
            pltpu.SemaphoreType.DMA((2, 2)),
        ],
        compiler_params=pltpu.CompilerParams(collective_id=number, has_side_effects=True),
        cost_estimate=pl.CostEstimate(flops=10**6, bytes_accessed=200 << 20, transcendentals=0),
    )(blocks, first, second)


def exchange(blocks, n, number):
    return pl.pallas_call(
        functools.partial(exchange_kernel, n),
        name=f"exchange_{number}",
        out_shape=jax.ShapeDtypeStruct(blocks.shape, blocks.dtype),
        in_specs=[VMEM_SPEC],
        out_specs=VMEM_SPEC,
        scratch_shapes=[
            pltpu.SemaphoreType.DMA,
            pltpu.SemaphoreType.DMA((n,)),
            pltpu.SemaphoreType.DMA((n,)),
        ],
        compiler_params=pltpu.CompilerParams(collective_id=number, has_side_effects=True),
        cost_estimate=pl.CostEstimate(flops=10**6, bytes_accessed=200 << 20, transcendentals=0),
    )(blocks)


def reorder(capacity, to_rows):
    many = BLOCK * QUARTERS * capacity
    square = (many, many)
    out, line = (iota(square, 0), iota(square, 1)) if to_rows else (iota(square, 1), iota(square, 0))
    device, quarter = lax.div(line, QUARTERS * capacity), lax.rem(lax.div(line, capacity), QUARTERS)
    place = (quarter * BLOCK + device) * capacity + lax.rem(line, capacity)
    return jnp.where(out == place, 1.0, 0.0).astype(bf16)


def expert_kernel(n, capacity, came_ref, gate_ref, up_ref, down_ref, out_ref, rows_ref, total_ref):
    j = pl.program_id(0)
    block = QUARTERS * capacity
    height = BLOCK * capacity
    part = rows_ref.shape[1] // QUARTERS

    @pl.when(j == 0)
    def _():
        order = reorder(capacity, True)
        for g in range(n // BLOCK):
            lines = jnp.concatenate([came_ref[g * BLOCK + k] for k in range(BLOCK)], axis=0)
            moved = dot(order, lines).astype(bf16)
            for q in range(QUARTERS):
                rows_ref[g * height : (g + 1) * height, q * part : (q + 1) * part] = moved[
                    q * height : (q + 1) * height
                ]
        total_ref[...] = jnp.zeros_like(total_ref)

    gated = dot(rows_ref[...], gate_ref[0])
    upward = dot(rows_ref[...], up_ref[0])
    hidden = (gated * sigmoid(gated) * upward).astype(bf16)
    total_ref[...] += dot(hidden, down_ref[0])

    @pl.when(j == pl.num_programs(0) - 1)
    def _():
        order = reorder(capacity, False)
        for g in range(n // BLOCK):
            rows = slice(g * height, (g + 1) * height)
            lines = jnp.concatenate(
                [total_ref[rows, q * part : (q + 1) * part] for q in range(QUARTERS)], axis=0
            )
            moved = dot(order, lines).astype(bf16)
            for k in range(BLOCK):
                out_ref[g * BLOCK + k] = moved[k * block : (k + 1) * block]


def expert_rows(came, gate, up, down, capacity):
    n, block, part = came.shape
    pieces, width, units = gate.shape
    whole = pl.BlockSpec((n, block, part), lambda j: (0, 0, 0))
    return pl.pallas_call(
        functools.partial(expert_kernel, n, capacity),
        name="expert_rows",
        grid=(pieces,),
        out_shape=jax.ShapeDtypeStruct(came.shape, bf16),
        in_specs=[
            whole,
            pl.BlockSpec((1, width, units), lambda j: (j, 0, 0)),
            pl.BlockSpec((1, width, units), lambda j: (j, 0, 0)),
            pl.BlockSpec((1, units, width), lambda j: (j, 0, 0)),
        ],
        out_specs=whole,
        scratch_shapes=[
            pltpu.VMEM((n * capacity, width), bf16),
            pltpu.VMEM((n * capacity, width), f32),
        ],
        compiler_params=pltpu.CompilerParams(dimension_semantics=("arbitrary",)),
        cost_estimate=pl.CostEstimate(flops=5 * 10**9, bytes_accessed=16 << 20, transcendentals=0),
    )(came, gate, up, down)


def combine_kernel(n, capacity, residual_ref, proj_ref, index_ref, weight_ref, back_ref, out_ref, rows_ref):
    rows, width = residual_ref.shape
    part = width // QUARTERS
    height = BLOCK * capacity
    order = reorder(capacity, True)
    for g in range(n // BLOCK):
        lines = jnp.concatenate([back_ref[g * BLOCK + k] for k in range(BLOCK)], axis=0)
        moved = dot(order, lines).astype(bf16)
        for q in range(QUARTERS):
            rows_ref[g * height : (g + 1) * height, q * part : (q + 1) * part] = moved[
                q * height : (q + 1) * height
            ]
    targets = route_columns(index_ref, n, capacity)
    slot = iota((rows, n * capacity), 1).astype(f32)
    mix = jnp.where(slot == targets[0], weight_ref[:, 0:1], 0.0) + jnp.where(
        slot == targets[1], weight_ref[:, 1:2], 0.0
    )
    high, low = halves(mix)
    for q in range(QUARTERS):
        cols = slice(q * part, (q + 1) * part)
        routed = dot(high, rows_ref[:, cols]) + dot(low, rows_ref[:, cols])
        half, within = divmod(q, QUARTERS // 2)
        proj = proj_ref[half, :, within * part : (within + 1) * part]
        stream = residual_ref[:, cols].astype(f32) + proj.astype(f32)
        out_ref[:, cols] = (stream + routed).astype(bf16)


def combine(residual, proj, index, weight, back, capacity):
    n = back.shape[0]
    return pl.pallas_call(
        functools.partial(combine_kernel, n, capacity),
        name="combine",
        out_shape=jax.ShapeDtypeStruct(residual.shape, bf16),
        in_specs=[VMEM_SPEC] * 5,
        out_specs=VMEM_SPEC,
        scratch_shapes=[pltpu.VMEM((n * capacity, residual.shape[1]), bf16)],
        cost_estimate=pl.CostEstimate(flops=10**9, bytes_accessed=8 << 20, transcendentals=0),
    )(residual, proj, index, weight, back)


def local(
    recept, key_input, value_input, output_gate_input, decay_input_part, correction_rate_input,
    head_decay_offset, decay_fixed_bias, correction_rate_bias, head_norm_gain, self_term_weight,
    output_weight_matrix, residual, feedforward_norm_gain, routed_expert_index, routed_expert_weight,
    gate_weight_experts, up_weight_experts, down_weight_experts,
):
    n = lax.axis_size("sp")
    cores = 2
    share = output_weight_matrix.shape[1] // cores
    columns = lax.dynamic_slice_in_dim(
        output_weight_matrix, lax.rem(lax.axis_index("sp"), cores) * share, share, axis=1
    )
    columns = lax.all_gather(columns, "tp")

    summary, maps, own = mixer_local(
        recept, key_input, value_input, decay_input_part, correction_rate_input, head_decay_offset,
        decay_fixed_bias[None], correction_rate_bias[None],
    )
    enter = prefix_states(summary, n)
    down, enter = lax.optimization_barrier((down_weight_experts[0], enter))
    down = lax.all_gather(down, "tp")
    mixed = readout(
        recept, key_input, value_input, output_gate_input, head_norm_gain[None], self_term_weight[None],
        maps, own, enter,
    )
    m = lax.axis_size("tp")
    shares = spread(mixed.reshape(m, -1, mixed.shape[1]), m, 3)
    halves_of_proj = jnp.einsum("hjrc,jcd->hrd", shares, columns, preferred_element_type=f32)
    proj = swap(halves_of_proj.astype(bf16), 4)

    rows = residual.shape[0]
    experts = gate_weight_experts.shape[0] * n
    capacity = 3 * rows // experts
    outgoing = build(residual, proj, feedforward_norm_gain[None], routed_expert_index, experts, capacity)
    came, gate, up = exchange_and_gather(
        outgoing, gate_weight_experts[0], up_weight_experts[0], n, lax.axis_size("tp"), 1
    )
    results = expert_rows(came, gate, up, down, capacity)
    back = exchange(results, n, 2)
    return combine(residual, proj, routed_expert_index, routed_expert_weight, back, capacity)


def solution(mesh):
    shared = P(("grp", "sp", "tp"), None)
    split = P(("grp", "sp"), "tp")
    return jax.shard_map(
        local,
        mesh=mesh,
        in_specs=(split,) * 7 + (P("tp"),) * 4 + (P("tp", None), shared, P(), shared, shared)
        + (P("sp", None, "tp"), P("sp", None, "tp"), P("sp", "tp", None)),
        out_specs=shared,
        check_vma=False,
    )
```

```python
import functools

import jax
import jax.numpy as jnp
from jax import lax
from jax.experimental import pallas as pl
from jax.experimental.pallas import tpu as pltpu
from jax.sharding import PartitionSpec as P

f32, bf16 = jnp.float32, jnp.bfloat16
MESH = pl.DeviceIdType.MESH
NN = (((1,), (0,)), ((), ()))
NT = (((1,), (1,)), ((), ()))
GROUP_EPS = 0.00064
NORM_EPS = 1e-06
SPAN = 64
LANES = 128
HEAD = 64
DECAY_SCALE = 0.6065306597126334
QUARTERS = 4
BLOCK = 4
VMEM_SPEC = pl.BlockSpec(memory_space=pltpu.VMEM)


def dot(a, b, dims=NN):
    return lax.dot_general(a.astype(bf16), b.astype(bf16), dims, preferred_element_type=f32)


def halves(x):
    high = x.astype(bf16)
    return high, (x - high.astype(f32)).astype(bf16)


def dot_split_left(a, b):
    high, low = halves(a)
    return dot(high, b) + dot(low, b)


def dot_split_right(a, b):
    high, low = halves(b)
    return dot(a, high) + dot(a, low)


def iota(shape, dim):
    return lax.broadcasted_iota(jnp.int32, shape, dim)


def sigmoid(x):
    return 1.0 / (1.0 + jnp.exp(-x))


def head_ones():
    shape = (LANES, LANES)
    return jnp.where((iota(shape, 0) >> 6) == (iota(shape, 1) >> 6), 1.0, 0.0).astype(bf16)


def stacked(x):
    first = iota(x.shape, 1) < HEAD
    zero = jnp.zeros_like(x)
    return jnp.concatenate([jnp.where(first, x, zero), jnp.where(first, zero, x)], axis=0)


def chunk_maps(units):
    row = iota((SPAN, LANES), 0)
    col = iota((SPAN, LANES), 1) & (HEAD - 1)
    square = (SPAN, SPAN)
    lower = jnp.where(iota(square, 0) >= iota(square, 1), 1.0, 0.0).astype(bf16)
    ones = head_ones()

    def each(work, *lists):
        return [work(*parts) for parts in zip(*lists)]

    def elementwise(recept, key, value, decay_pre, rate_pre, offset, decay_bias, rate_bias):
        decay_log = offset - DECAY_SCALE * sigmoid(decay_bias + decay_pre.astype(f32))
        key = key.astype(f32)
        return decay_log, dot_split_right(lower, decay_log), dot_split_left(key * key, ones)

    def scaled(unit, first):
        recept, key, value, decay_pre, rate_pre, offset, decay_bias, rate_bias = unit
        decay_log, cumul, norm = first
        key = key.astype(f32)
        rate = sigmoid(rate_bias + rate_pre.astype(f32))
        unit_key = key * lax.rsqrt(norm + NORM_EPS)
        middle = cumul[SPAN // 2 - 1 : SPAN // 2, :]
        rel = cumul - middle
        rise, fall = jnp.exp(rel), jnp.exp(-rel)
        to_middle = jnp.exp(middle)
        to_end = jnp.exp(cumul[SPAN - 1 : SPAN, :] - middle)
        remove = -unit_key * jnp.exp(rel - decay_log)
        read = recept.astype(f32) * rise
        write = unit_key * rate * fall
        keys = key * fall
        left = jnp.concatenate([remove.astype(bf16), read.astype(bf16)], axis=0)
        right = jnp.concatenate([stacked(write.astype(bf16)), stacked(keys.astype(bf16))], axis=0)
        from_start = [(remove * to_middle).astype(bf16), (read * to_middle).astype(bf16)]
        write_end = jnp.concatenate([write * to_end, keys * to_end], axis=0).T.astype(bf16)
        ending = jnp.broadcast_to(to_end * to_middle, (LANES, LANES)).T
        return dot(left, right, NT), from_start, write_end, ending

    first = [elementwise(*unit) for unit in units]
    second = each(scaled, units, first)
    scores = [item[0] for item in second]
    strict, within = row > col, row >= col

    def merging(level):
        size = 1 << level
        same = (row >> (level + 1)) == (col >> (level + 1))
        return same & ((row & size) != 0) & ((col & size) == 0)

    lower_part = [jnp.where(strict, s[:SPAN, :LANES], 0.0).astype(bf16) for s in scores]
    remove_key = [jnp.where(strict, s[:SPAN, LANES:], 0.0).astype(bf16) for s in scores]
    within_maps = [
        jnp.where(
            jnp.concatenate([within, within], axis=1), s[SPAN:], 0.0
        ).astype(bf16)
        for s in scores
    ]
    removed_value = [dot(m, stacked(unit[2])).astype(bf16) for m, unit in zip(remove_key, units)]
    inverse = [jnp.where(row == col, 1.0, jnp.where(merging(0), m.astype(f32), 0.0)) for m in lower_part]
    for level in range(1, SPAN.bit_length() - 1):
        chosen = merging(level)
        inner = [
            dot(jnp.where(chosen, m, jnp.zeros_like(m)), stacked(x.astype(bf16)))
            for m, x in zip(lower_part, inverse)
        ]
        inverse = [x + dot(x, stacked(y.astype(bf16))) for x, y in zip(inverse, inner)]
    solved = [
        dot(x, jnp.concatenate([stacked(item[1][0]), stacked(v)], axis=1))
        for x, item, v in zip(inverse, second, removed_value)
    ]
    return [
        (jnp.concatenate([q[:, :LANES].astype(bf16), item[1][1]], axis=0), q[:, LANES:], maps) + item[2:]
        for q, item, maps in zip(solved, second, within_maps)
    ]


def mixer_kernel(
    pairs, chunks,
    recept_ref, key_ref, value_ref, decay_ref, rate_ref, offset_ref, decay_bias_ref, rate_bias_ref,
    summary_ref, map_ref, own_ref,
    left_ref, solved_ref, within_ref, write_ref, ending_ref, state_ref, removed_ref, partial_ref,
):
    first_head = iota((SPAN, LANES), 1) < HEAD

    def rows_of(c):
        return pl.ds(pl.multiple_of(c * SPAN, SPAN), SPAN)

    unroll = 2 if chunks % 2 == 0 else 1

    def prepare(i, _):
        places = [(i * unroll + k, p) for k in range(unroll) for p in range(pairs)]
        units = []
        for c, p in places:
            rows, cols = rows_of(c), slice(p * LANES, (p + 1) * LANES)
            offset = jnp.where(
                first_head, offset_ref[rows, 2 * p : 2 * p + 1], offset_ref[rows, 2 * p + 1 : 2 * p + 2]
            )
            units.append(
                (
                    recept_ref[rows, cols], key_ref[rows, cols], value_ref[rows, cols],
                    decay_ref[rows, cols], rate_ref[rows, cols], offset,
                    decay_bias_ref[:, cols], rate_bias_ref[:, cols],
                )
            )
        for (c, p), (left, solved, within, write, ending) in zip(places, chunk_maps(units)):
            left_ref[c, p] = left
            solved_ref[c, p] = solved
            within_ref[c, p] = within
            write_ref[c, p] = write
            ending_ref[c, p] = ending
        return 0

    lax.fori_loop(0, chunks // unroll, prepare, 0)

    square = (LANES, LANES)
    eye = jnp.where(iota(square, 0) == iota(square, 1), 1.0, 0.0)
    for p in range(pairs):
        state_ref[p, :, :LANES] = eye
        state_ref[p, :, LANES:] = jnp.zeros(square, f32)
    own_block = (iota((LANES, 2 * LANES), 0) >> 6) == ((iota((LANES, 2 * LANES), 1) >> 6) & 1)

    def advance(c, _):
        rows = rows_of(c)
        states = [state_ref[p] for p in range(pairs)]
        crossed = [dot(left_ref[c, p], states[p]) for p in range(pairs)]
        removed = [
            jnp.concatenate(
                [x[:SPAN, :LANES], x[:SPAN, LANES:] + solved_ref[c, p]], axis=1
            ).astype(bf16)
            for p, x in enumerate(crossed)
        ]
        updates = []
        for p in range(pairs):
            value = value_ref[rows, p * LANES : (p + 1) * LANES]
            right = jnp.concatenate(
                [removed[p], jnp.concatenate([jnp.zeros_like(value), value], axis=1)], axis=0
            )
            updates.append(dot(write_ref[c, p], right))
        for p in range(pairs):
            removed_ref[c, p] = removed[p]
            partial_ref[c, p] = crossed[p][SPAN:]
            ending = ending_ref[c, p]
            state_ref[p] = states[p] * jnp.concatenate([ending, ending], axis=1) + jnp.where(
                own_block, updates[p], 0.0
            )
        return 0

    lax.fori_loop(0, chunks, advance, 0)

    for p in range(pairs):
        transit = state_ref[p, :, :LANES] - eye
        added = state_ref[p, :, LANES:]
        summary_ref[p, 0] = (transit[:HEAD] + transit[HEAD:]).astype(bf16)
        summary_ref[p, 1] = (added[:HEAD] + added[HEAD:]).astype(bf16)

    def emit(c, _):
        rows = rows_of(c)
        for p in range(pairs):
            cols = slice(p * LANES, (p + 1) * LANES)
            removed = removed_ref[c, p]
            value = stacked(value_ref[rows, cols])
            right = jnp.concatenate(
                [
                    jnp.concatenate([stacked(removed[:, :LANES]), stacked(removed[:, LANES:])], axis=1),
                    jnp.concatenate([jnp.zeros_like(value), value], axis=1),
                ],
                axis=0,
            )
            both = partial_ref[c, p] + dot(within_ref[c, p], right)
            map_ref[rows, cols] = both[:, :LANES].astype(bf16)
            own_ref[rows, cols] = both[:, LANES:]
        return 0

    lax.fori_loop(0, chunks, emit, 0)


def mixer_local(recept, key, value, decay, rate, offset, decay_bias, rate_bias):
    length, width = recept.shape
    pairs, chunks = width // LANES, length // SPAN
    per = (chunks, pairs)
    return pl.pallas_call(
        functools.partial(mixer_kernel, pairs, chunks),
        name="mixer_local",
        out_shape=(
            jax.ShapeDtypeStruct((pairs, 2, HEAD, LANES), bf16),
            jax.ShapeDtypeStruct((length, width), bf16),
            jax.ShapeDtypeStruct((length, width), f32),
        ),
        in_specs=[VMEM_SPEC] * 8,
        out_specs=(VMEM_SPEC,) * 3,
        scratch_shapes=[
            pltpu.VMEM(per + (2 * SPAN, LANES), bf16),
            pltpu.VMEM(per + (SPAN, LANES), f32),
            pltpu.VMEM(per + (SPAN, 2 * LANES), bf16),
            pltpu.VMEM(per + (LANES, 2 * SPAN), bf16),
            pltpu.VMEM(per + (LANES, LANES), f32),
            pltpu.VMEM((pairs, LANES, 2 * LANES), f32),
            pltpu.VMEM(per + (SPAN, 2 * LANES), bf16),
            pltpu.VMEM(per + (SPAN, 2 * LANES), f32),
        ],
        cost_estimate=pl.CostEstimate(
            flops=80 * 2 * LANES * length * width, bytes_accessed=12 * length * width, transcendentals=0
        ),
    )(recept, key, value, decay, rate, offset, decay_bias, rate_bias)


def prefix_kernel(n, pairs, summary_ref, enter_ref, got, states, entry, sent1, came1, sent2, came2):
    me = lax.axis_index("sp")
    stride = n // pairs
    works = lax.rem(me, stride) == 0
    mine = lax.div(me, stride)
    barrier = pltpu.get_barrier_semaphore()

    def greet(device):
        pl.semaphore_signal(barrier, inc=1, device_id={"sp": device}, device_id_type=MESH)

    @pl.when(works)
    def _():
        def body(j, _):
            greet(lax.rem(me + j, n))
            return 0

        lax.fori_loop(1, n, body, 0)
        pl.semaphore_wait(barrier, n - 1)

    @pl.when(jnp.logical_not(works))
    def _():
        for p in range(pairs):
            greet(p * stride)
        pl.semaphore_wait(barrier, pairs)

    def outward(p):
        return pltpu.make_async_remote_copy(
            src_ref=summary_ref.at[p], dst_ref=got.at[me], send_sem=sent1.at[p], recv_sem=came1.at[me],
            device_id={"sp": p * stride}, device_id_type=MESH,
        )

    def inward(i):
        return pltpu.make_async_remote_copy(
            src_ref=summary_ref.at[0], dst_ref=got.at[i], send_sem=sent1.at[0], recv_sem=came1.at[i],
            device_id={"sp": i}, device_id_type=MESH,
        )

    def back(i, p):
        return pltpu.make_async_remote_copy(
            src_ref=states.at[i], dst_ref=entry.at[p], send_sem=sent2.at[i], recv_sem=came2.at[p],
            device_id={"sp": i}, device_id_type=MESH,
        )

    for p in range(pairs):
        @pl.when(me != p * stride)
        def _():
            outward(p).start()

        @pl.when(me == p * stride)
        def _():
            got[me] = summary_ref[p]

    @pl.when(works)
    def _():
        def step(i, state):
            states[i] = state.astype(bf16)

            @pl.when(i != me)
            def _():
                back(i, mine).start()
                inward(i).wait_recv()

            @pl.when(i == me)
            def _():
                entry[mine] = states[i]

            high, low = halves(state)
            transit, added = got[i, 0], got[i, 1].astype(f32)
            moved = dot(transit, stacked(high)) + dot(transit, stacked(low))
            return state + (moved + added)

        lax.fori_loop(0, n, step, jnp.zeros((HEAD, LANES), f32))

    for p in range(pairs):
        @pl.when(me != p * stride)
        def _():
            back(0, p).wait_recv()

        enter_ref[p] = entry[p]

    for p in range(pairs):
        @pl.when(me != p * stride)
        def _():
            outward(p).wait_send()

    @pl.when(works)
    def _():
        def body(i, _):
            @pl.when(i != me)
            def _():
                back(i, mine).wait_send()

            return 0

        lax.fori_loop(0, n, body, 0)


def prefix_states(summary, n):
    pairs = summary.shape[0]
    return pl.pallas_call(
        functools.partial(prefix_kernel, n, pairs),
        name="prefix_states",
        out_shape=jax.ShapeDtypeStruct((pairs, HEAD, LANES), bf16),
        in_specs=[VMEM_SPEC],
        out_specs=VMEM_SPEC,
        scratch_shapes=[
            pltpu.VMEM((n, 2, HEAD, LANES), bf16),
            pltpu.VMEM((n, HEAD, LANES), bf16),
            pltpu.VMEM((pairs, HEAD, LANES), bf16),
            pltpu.SemaphoreType.DMA((pairs,)),
            pltpu.SemaphoreType.DMA((n,)),
            pltpu.SemaphoreType.DMA((n,)),
            pltpu.SemaphoreType.DMA((pairs,)),
        ],
        compiler_params=pltpu.CompilerParams(collective_id=0, has_side_effects=True),
        cost_estimate=pl.CostEstimate(flops=10**9, bytes_accessed=60 << 20, transcendentals=0),
    )(summary)


def readout_kernel(
    pairs, length, recept_ref, key_ref, value_ref, gate_ref, gain_ref, self_ref, map_ref, own_ref,
    enter_ref, out_ref,
):
    ones = head_ones()
    step = 128

    def some(i, _):
        rows = pl.ds(pl.multiple_of(i * step, step), step)
        every = [slice(p * LANES, (p + 1) * LANES) for p in range(pairs)]
        own = [
            recept_ref[rows, c].astype(f32) * key_ref[rows, c].astype(f32) * self_ref[:, c] for c in every
        ]
        read = [
            dot(map_ref[rows, c], stacked(enter_ref[p])) + own_ref[rows, c] for p, c in enumerate(every)
        ]
        own = [dot_split_left(x, ones) for x in own]
        mean = [dot_split_left(x, ones) * (1.0 / HEAD) for x in read]
        center = [x - y for x, y in zip(read, mean)]
        spread = [dot_split_left(x * x, ones) * (1.0 / HEAD) for x in center]
        for p, c in enumerate(every):
            normed = center[p] * lax.rsqrt(spread[p] + GROUP_EPS) * gain_ref[:, c]
            value = value_ref[rows, c].astype(f32)
            out_ref[rows, c] = (
                (normed + own[p] * value) * gate_ref[rows, c].astype(f32)
            ).astype(bf16)
        return 0

    lax.fori_loop(0, length // step, some, 0)


def readout(recept, key, value, gate, gain, self_weight, maps, own, enter):
    length, width = recept.shape
    return pl.pallas_call(
        functools.partial(readout_kernel, width // LANES, length),
        name="readout",
        out_shape=jax.ShapeDtypeStruct((length, width), bf16),
        in_specs=[VMEM_SPEC] * 9,
        out_specs=VMEM_SPEC,
        cost_estimate=pl.CostEstimate(flops=10**9, bytes_accessed=16 << 20, transcendentals=0),
    )(recept, key, value, gate, gain, self_weight, maps, own, enter)


def route_columns(index_ref, experts, capacity):
    rows = index_ref.shape[0]
    lane = iota((rows, LANES), 1)
    first = lane == index_ref[:, 0:1]
    second = lane == index_ref[:, 1:2]
    square = (rows, rows)
    before = jnp.where(iota(square, 0) > iota(square, 1), 1.0, 0.0)
    both = jnp.where(first, 1.0, 0.0) + jnp.where(second, 1.0, 0.0)
    counts = dot(before, both) + (lane * capacity).astype(f32)
    return [jnp.sum(jnp.where(hit, counts, 0.0), axis=1, keepdims=True) for hit in (first, second)]


def build_kernel(experts, capacity, residual_ref, proj_ref, gain_ref, index_ref, out_ref, stack_ref):
    rows, width = residual_ref.shape
    part = width // QUARTERS
    proj = jnp.concatenate([proj_ref[0], proj_ref[1]], axis=1)
    stream = residual_ref[...].astype(f32) + proj.astype(f32)
    scale = lax.rsqrt(jnp.mean(stream * stream, axis=1, keepdims=True) + NORM_EPS)
    ffn_in = (stream * scale * gain_ref[...]).astype(bf16)
    for q in range(QUARTERS):
        stack_ref[q * rows : (q + 1) * rows] = ffn_in[:, q * part : (q + 1) * part]
    targets = [
        jnp.broadcast_to(t, (rows, rows)).T[:1] for t in route_columns(index_ref, experts, capacity)
    ]
    block = QUARTERS * capacity
    many = BLOCK * block
    line = iota((many, 1), 0)
    device = lax.div(line, block)
    quarter = lax.div(lax.rem(line, block), capacity)
    slot = (device * capacity + lax.rem(line, capacity)).astype(f32)
    for g in range(experts // BLOCK):
        wanted = slot + float(g * BLOCK * capacity)
        hit = jnp.where((wanted == targets[0]) | (wanted == targets[1]), 1.0, 0.0)
        place = jnp.concatenate(
            [jnp.where(quarter == q, hit, 0.0) for q in range(QUARTERS)], axis=1
        ).astype(bf16)
        lines = dot(place, stack_ref[...]).astype(bf16)
        for k in range(BLOCK):
            out_ref[g * BLOCK + k] = lines[k * block : (k + 1) * block]


def build(residual, proj, gain, index, experts, capacity):
    rows, width = residual.shape
    return pl.pallas_call(
        functools.partial(build_kernel, experts, capacity),
        name="build",
        out_shape=jax.ShapeDtypeStruct((experts, QUARTERS * capacity, width // QUARTERS), bf16),
        in_specs=[VMEM_SPEC] * 4,
        out_specs=VMEM_SPEC,
        scratch_shapes=[pltpu.VMEM((QUARTERS * rows, width // QUARTERS), bf16)],
        cost_estimate=pl.CostEstimate(flops=10**9, bytes_accessed=8 << 20, transcendentals=0),
    )(residual, proj, gain, index)


def other_core(me):
    return me + 1 - 2 * lax.rem(me, 2)


def spread_kernel(m, src_ref, out_ref, own_sem, sent, came, pass_sent, pass_came):
    me, col = lax.axis_index("sp"), lax.axis_index("tp")
    core, partner = lax.rem(me, 2), other_core(me)
    barrier = pltpu.get_barrier_semaphore()
    pl.semaphore_signal(barrier, inc=1, device_id={"sp": partner}, device_id_type=MESH)
    for k in range(1, m):
        pl.semaphore_signal(
            barrier, inc=1, device_id={"tp": lax.rem(col + k, m)}, device_id_type=MESH
        )
    own = pltpu.make_async_copy(src_ref.at[col], out_ref.at[core, col], own_sem)
    own.start()
    pl.semaphore_wait(barrier, m)

    def send(k):
        to = lax.rem(col + k, m)
        return pltpu.make_async_remote_copy(
            src_ref=src_ref.at[to], dst_ref=out_ref.at[core, col], send_sem=sent.at[k],
            recv_sem=came.at[k], device_id={"tp": to}, device_id_type=MESH,
        )

    def arrival(k):
        frm = lax.rem(col + m - k, m)
        return pltpu.make_async_remote_copy(
            src_ref=src_ref.at[frm], dst_ref=out_ref.at[core, frm], send_sem=sent.at[k],
            recv_sem=came.at[k], device_id={"tp": frm}, device_id_type=MESH,
        )

    def onward(k, source):
        frm = lax.rem(col + m - k, m)
        return pltpu.make_async_remote_copy(
            src_ref=source, dst_ref=out_ref.at[core, frm], send_sem=pass_sent.at[k],
            recv_sem=pass_came.at[k], device_id={"sp": partner}, device_id_type=MESH,
        )

    def from_partner(k):
        frm = lax.rem(col + m - k, m)
        return pltpu.make_async_remote_copy(
            src_ref=src_ref.at[frm], dst_ref=out_ref.at[1 - core, frm], send_sem=pass_sent.at[k],
            recv_sem=pass_came.at[k], device_id={"sp": partner}, device_id_type=MESH,
        )

    order = [m // 2] + [k for k in range(1, m) if k != m // 2]
    for k in order:
        send(k).start()
    onward(0, src_ref.at[col]).start()
    passed = [k for k in range(1, m) if k != m // 2] + [m // 2]
    for k in passed:
        arrival(k).wait_recv()
        onward(k, out_ref.at[core, lax.rem(col + m - k, m)]).start()
    own.wait()
    for k in range(m):
        from_partner(k).wait_recv()
        onward(k, src_ref.at[col]).wait_send()
    for k in range(1, m):
        send(k).wait_send()


def spread(blocks, m, number):
    return pl.pallas_call(
        functools.partial(spread_kernel, m),
        name="spread",
        out_shape=jax.ShapeDtypeStruct((2,) + blocks.shape, blocks.dtype),
        in_specs=[VMEM_SPEC],
        out_specs=VMEM_SPEC,
        scratch_shapes=[pltpu.SemaphoreType.DMA] + [pltpu.SemaphoreType.DMA((m,))] * 4,
        compiler_params=pltpu.CompilerParams(collective_id=number, has_side_effects=True),
        cost_estimate=pl.CostEstimate(flops=10**6, bytes_accessed=40 << 20, transcendentals=0),
    )(blocks)


def swap_kernel(src_ref, out_ref, own_sem, sent, came):
    me = lax.axis_index("sp")
    core, partner = lax.rem(me, 2), other_core(me)
    barrier = pltpu.get_barrier_semaphore()
    pl.semaphore_signal(barrier, inc=1, device_id={"sp": partner}, device_id_type=MESH)
    own = pltpu.make_async_copy(src_ref.at[core], out_ref.at[core], own_sem)
    own.start()
    pl.semaphore_wait(barrier, 1)
    away = pltpu.make_async_remote_copy(
        src_ref=src_ref.at[1 - core], dst_ref=out_ref.at[core], send_sem=sent, recv_sem=came,
        device_id={"sp": partner}, device_id_type=MESH,
    )
    away.start()
    own.wait()
    pltpu.make_async_remote_copy(
        src_ref=src_ref.at[1 - core], dst_ref=out_ref.at[1 - core], send_sem=sent, recv_sem=came,
        device_id={"sp": partner}, device_id_type=MESH,
    ).wait_recv()
    away.wait_send()


def swap(blocks, number):
    return pl.pallas_call(
        swap_kernel,
        name="swap",
        out_shape=jax.ShapeDtypeStruct(blocks.shape, blocks.dtype),
        in_specs=[VMEM_SPEC],
        out_specs=VMEM_SPEC,
        scratch_shapes=[pltpu.SemaphoreType.DMA] * 3,
        compiler_params=pltpu.CompilerParams(collective_id=number, has_side_effects=True),
        cost_estimate=pl.CostEstimate(flops=10**6, bytes_accessed=4 << 20, transcendentals=0),
    )(blocks)


def exchange_gather_kernel(n, m, src_ref, first_ref, second_ref, out_ref, first_all, second_all,
                           stage, own_sem, sent, came, in_sem, out_sem, ring_sent, ring_came, pass_sent, pass_came):
    me, col = lax.axis_index("sp"), lax.axis_index("tp")
    right, left = lax.rem(col + 1, m), lax.rem(col + m - 1, m)
    shards, wholes = (first_ref, second_ref), (first_all, second_all)
    barrier = pltpu.get_barrier_semaphore()

    def greet(k, _):
        pl.semaphore_signal(
            barrier, inc=1, device_id={"sp": lax.rem(me + k, n)}, device_id_type=MESH
        )
        return 0

    for side in (left, right):
        pl.semaphore_signal(barrier, inc=1, device_id={"tp": side}, device_id_type=MESH)
    lax.fori_loop(1, n, greet, 0)
    own = pltpu.make_async_copy(src_ref.at[me], out_ref.at[me], own_sem)
    own.start()
    loads = [pltpu.make_async_copy(shards[a], stage.at[a], in_sem.at[a]) for a in range(2)]
    stores = [pltpu.make_async_copy(stage.at[a], wholes[a].at[col], out_sem.at[a]) for a in range(2)]
    for load in loads:
        load.start()
    for load in loads:
        load.wait()
    pl.semaphore_wait(barrier, n + 1)

    def copy(k):
        to = lax.rem(me + k, n)
        return pltpu.make_async_remote_copy(
            src_ref=src_ref.at[to], dst_ref=out_ref.at[me], send_sem=sent.at[k], recv_sem=came.at[k],
            device_id={"sp": to}, device_id_type=MESH,
        )

    def start(k, _):
        away = n // 2 - lax.div(k, 2)
        copy(jnp.where(lax.rem(k, 2) == 0, away, n - away)).start()
        return 0

    def arrived(k):
        frm = lax.rem(me + n - k, n)
        return pltpu.make_async_remote_copy(
            src_ref=src_ref.at[frm], dst_ref=out_ref.at[frm], send_sem=sent.at[k], recv_sem=came.at[k],
            device_id={"sp": frm}, device_id_type=MESH,
        )

    half = first_ref.shape[0] // 2

    def rows(h):
        return pl.ds(h * half, half)

    def hop(a, d, h):
        return pltpu.make_async_remote_copy(
            src_ref=stage.at[a, rows(h)], dst_ref=wholes[a].at[col, rows(h)],
            send_sem=ring_sent.at[a, d, h], recv_sem=ring_came.at[a, d, h],
            device_id={"tp": (right, left)[d]}, device_id_type=MESH,
        )

    def hop_in(a, d, h):
        frm = (left, right)[d]
        return pltpu.make_async_remote_copy(
            src_ref=stage.at[a, rows(h)], dst_ref=wholes[a].at[frm, rows(h)],
            send_sem=ring_sent.at[a, d, h], recv_sem=ring_came.at[a, d, h],
            device_id={"tp": frm}, device_id_type=MESH,
        )

    def onward(a, d):
        frm = (left, right)[d]
        return pltpu.make_async_remote_copy(
            src_ref=wholes[a].at[frm, rows(d)], dst_ref=wholes[a].at[frm, rows(d)],
            send_sem=pass_sent.at[a, d], recv_sem=pass_came.at[a, d],
            device_id={"tp": (right, left)[d]}, device_id_type=MESH,
        )

    def onward_in(a, d):
        frm = lax.rem(col + 2, m)
        return pltpu.make_async_remote_copy(
            src_ref=wholes[a].at[frm, rows(d)], dst_ref=wholes[a].at[frm, rows(d)],
            send_sem=pass_sent.at[a, d], recv_sem=pass_came.at[a, d],
            device_id={"tp": (left, right)[d]}, device_id_type=MESH,
        )

    copy(n // 2).start()
    lax.fori_loop(2, n, start, 0)
    for a in range(2):
        for d, h in ((0, 0), (1, 1), (0, 1), (1, 0)):
            hop(a, d, h).start()
    for store in stores:
        store.start()
    for a in range(2):
        for d in range(2):
            hop_in(a, d, d).wait_recv()
            onward(a, d).start()
    own.wait()
    for store in stores:
        store.wait()

    def finish(k, _):
        arrived(k).wait_recv()
        copy(k).wait_send()
        return 0

    lax.fori_loop(1, n, finish, 0)
    for a in range(2):
        for d in range(2):
            hop_in(a, d, 1 - d).wait_recv()
            onward_in(a, d).wait_recv()
            onward(a, d).wait_send()
            for h in range(2):
                hop(a, d, h).wait_send()


def exchange_and_gather(blocks, first, second, n, m, number):
    any_spec = pl.BlockSpec(memory_space=pl.ANY)
    whole = jax.ShapeDtypeStruct((m,) + first.shape, first.dtype)
    return pl.pallas_call(
        functools.partial(exchange_gather_kernel, n, m),
        name=f"exchange_{number}",
        out_shape=(jax.ShapeDtypeStruct(blocks.shape, blocks.dtype), whole, whole),
        in_specs=[VMEM_SPEC, any_spec, any_spec],
        out_specs=(VMEM_SPEC, any_spec, any_spec),
        scratch_shapes=[
            pltpu.VMEM((2,) + first.shape, first.dtype),
            pltpu.SemaphoreType.DMA,
            pltpu.SemaphoreType.DMA((n,)),
            pltpu.SemaphoreType.DMA((n,)),
            pltpu.SemaphoreType.DMA((2,)),
            pltpu.SemaphoreType.DMA((2,)),
            pltpu.SemaphoreType.DMA((2, 2, 2)),
            pltpu.SemaphoreType.DMA((2, 2, 2)),
            pltpu.SemaphoreType.DMA((2, 2)),
            pltpu.SemaphoreType.DMA((2, 2)),
        ],
        compiler_params=pltpu.CompilerParams(collective_id=number, has_side_effects=True),
        cost_estimate=pl.CostEstimate(flops=10**6, bytes_accessed=200 << 20, transcendentals=0),
    )(blocks, first, second)


def reorder(capacity, to_rows):
    many = BLOCK * QUARTERS * capacity
    square = (many, many)
    out, line = (iota(square, 0), iota(square, 1)) if to_rows else (iota(square, 1), iota(square, 0))
    device, quarter = lax.div(line, QUARTERS * capacity), lax.rem(lax.div(line, capacity), QUARTERS)
    place = (quarter * BLOCK + device) * capacity + lax.rem(line, capacity)
    return jnp.where(out == place, 1.0, 0.0).astype(bf16)


def expert_kernel(
    n, capacity, came_ref, gate_ref, up_ref, down_ref, out_ref,
    gates, ups, downs, rows_ref, back_ref, load_sem, sent, came,
):
    me = lax.axis_index("sp")
    block = QUARTERS * capacity
    height = BLOCK * capacity
    part = out_ref.shape[2]
    pieces = gates.shape[0]
    groups = n // BLOCK
    loads = []
    for j in range(pieces):
        for w, (source, target) in enumerate(((gate_ref, gates), (up_ref, ups), (down_ref, downs))):
            loads.append(pltpu.make_async_copy(source.at[j], target.at[j], load_sem.at[j, w]))
    for load in loads:
        load.start()
    barrier = pltpu.get_barrier_semaphore()

    def greet(k, _):
        pl.semaphore_signal(
            barrier, inc=1, device_id={"sp": lax.rem(me + k, n)}, device_id_type=MESH
        )
        return 0

    lax.fori_loop(1, n, greet, 0)
    gather_order, spread_order = reorder(capacity, True), reorder(capacity, False)
    for load in loads:
        load.wait()
    pl.semaphore_wait(barrier, n - 1)

    def home(device):
        return pltpu.make_async_remote_copy(
            src_ref=back_ref.at[device], dst_ref=out_ref.at[me], send_sem=sent.at[device],
            recv_sem=came.at[me], device_id={"sp": device}, device_id_type=MESH,
        )

    def work(c, _):
        own_group = lax.div(me, BLOCK)
        both = (
            lax.rem(own_group + groups // 2 + c, groups),
            lax.rem(own_group + groups // 2 - 1 - c + groups, groups),
        )
        for i, g in enumerate(both):
            lines = jnp.concatenate([came_ref[g * BLOCK + k] for k in range(BLOCK)], axis=0)
            moved = dot(gather_order, lines).astype(bf16)
            for q in range(QUARTERS):
                rows_ref[i * height : (i + 1) * height, q * part : (q + 1) * part] = moved[
                    q * height : (q + 1) * height
                ]
        rows = rows_ref[...]
        hidden = []
        for j in range(pieces):
            gated = dot(rows, gates[j])
            hidden.append((gated * sigmoid(gated) * dot(rows, ups[j])).astype(bf16))
        total = dot(hidden[0], downs[0])
        for j in range(1, pieces):
            total = total + dot(hidden[j], downs[j])
        total = total.astype(bf16)
        for i, g in enumerate(both):
            lines = jnp.concatenate(
                [total[i * height : (i + 1) * height, q * part : (q + 1) * part] for q in range(QUARTERS)],
                axis=0,
            )
            moved = dot(spread_order, lines).astype(bf16)
            for k in range(BLOCK):
                device = g * BLOCK + k
                result = moved[k * block : (k + 1) * block]
                back_ref[device] = result

                @pl.when(device == me)
                def _():
                    out_ref[me] = result

        for g in both:
            for k in range(BLOCK):
                device = g * BLOCK + k

                @pl.when(device != me)
                def _():
                    home(device).start()

        return 0

    lax.fori_loop(0, groups // 2, work, 0)

    def finish(k, _):
        frm = lax.rem(me + k, n)
        pltpu.make_async_remote_copy(
            src_ref=back_ref.at[frm], dst_ref=out_ref.at[frm], send_sem=sent.at[frm],
            recv_sem=came.at[frm], device_id={"sp": frm}, device_id_type=MESH,
        ).wait_recv()
        home(frm).wait_send()
        return 0

    lax.fori_loop(1, n, finish, 0)


def expert_rows(came, gate, up, down, capacity, number):
    n, block, part = came.shape
    pieces, width, units = gate.shape
    any_spec = pl.BlockSpec(memory_space=pl.ANY)
    return pl.pallas_call(
        functools.partial(expert_kernel, n, capacity),
        name="expert_rows",
        out_shape=jax.ShapeDtypeStruct(came.shape, bf16),
        in_specs=[VMEM_SPEC, any_spec, any_spec, any_spec],
        out_specs=VMEM_SPEC,
        scratch_shapes=[
            pltpu.VMEM(gate.shape, bf16),
            pltpu.VMEM(up.shape, bf16),
            pltpu.VMEM(down.shape, bf16),
            pltpu.VMEM((2 * BLOCK * capacity, width), bf16),
            pltpu.VMEM(came.shape, bf16),
            pltpu.SemaphoreType.DMA((pieces, 3)),
            pltpu.SemaphoreType.DMA((n,)),
            pltpu.SemaphoreType.DMA((n,)),
        ],
        compiler_params=pltpu.CompilerParams(collective_id=number, has_side_effects=True),
        cost_estimate=pl.CostEstimate(flops=5 * 10**9, bytes_accessed=200 << 20, transcendentals=0),
    )(came, gate, up, down)


def combine_kernel(n, capacity, residual_ref, proj_ref, index_ref, weight_ref, back_ref, out_ref, rows_ref):
    rows, width = residual_ref.shape
    part = width // QUARTERS
    height = BLOCK * capacity
    order = reorder(capacity, True)
    for g in range(n // BLOCK):
        lines = jnp.concatenate([back_ref[g * BLOCK + k] for k in range(BLOCK)], axis=0)
        moved = dot(order, lines).astype(bf16)
        for q in range(QUARTERS):
            rows_ref[g * height : (g + 1) * height, q * part : (q + 1) * part] = moved[
                q * height : (q + 1) * height
            ]
    targets = route_columns(index_ref, n, capacity)
    slot = iota((rows, n * capacity), 1).astype(f32)
    mix = jnp.where(slot == targets[0], weight_ref[:, 0:1], 0.0) + jnp.where(
        slot == targets[1], weight_ref[:, 1:2], 0.0
    )
    high, low = halves(mix)
    for q in range(QUARTERS):
        cols = slice(q * part, (q + 1) * part)
        routed = dot(high, rows_ref[:, cols]) + dot(low, rows_ref[:, cols])
        half, within = divmod(q, QUARTERS // 2)
        proj = proj_ref[half, :, within * part : (within + 1) * part]
        stream = residual_ref[:, cols].astype(f32) + proj.astype(f32)
        out_ref[:, cols] = (stream + routed).astype(bf16)


def combine(residual, proj, index, weight, back, capacity):
    n = back.shape[0]
    return pl.pallas_call(
        functools.partial(combine_kernel, n, capacity),
        name="combine",
        out_shape=jax.ShapeDtypeStruct(residual.shape, bf16),
        in_specs=[VMEM_SPEC] * 5,
        out_specs=VMEM_SPEC,
        scratch_shapes=[pltpu.VMEM((n * capacity, residual.shape[1]), bf16)],
        cost_estimate=pl.CostEstimate(flops=10**9, bytes_accessed=8 << 20, transcendentals=0),
    )(residual, proj, index, weight, back)


def local(
    recept, key_input, value_input, output_gate_input, decay_input_part, correction_rate_input,
    head_decay_offset, decay_fixed_bias, correction_rate_bias, head_norm_gain, self_term_weight,
    output_weight_matrix, residual, feedforward_norm_gain, routed_expert_index, routed_expert_weight,
    gate_weight_experts, up_weight_experts, down_weight_experts,
):
    n = lax.axis_size("sp")
    cores = 2
    share = output_weight_matrix.shape[1] // cores
    columns = lax.dynamic_slice_in_dim(
        output_weight_matrix, lax.rem(lax.axis_index("sp"), cores) * share, share, axis=1
    )
    columns = lax.all_gather(columns, "tp")

    summary, maps, own = mixer_local(
        recept, key_input, value_input, decay_input_part, correction_rate_input, head_decay_offset,
        decay_fixed_bias[None], correction_rate_bias[None],
    )
    enter = prefix_states(summary, n)
    down, enter = lax.optimization_barrier((down_weight_experts[0], enter))
    down = lax.all_gather(down, "tp")
    mixed = readout(
        recept, key_input, value_input, output_gate_input, head_norm_gain[None], self_term_weight[None],
        maps, own, enter,
    )
    m = lax.axis_size("tp")
    shares = spread(mixed.reshape(m, -1, mixed.shape[1]), m, 3)
    halves_of_proj = jnp.einsum("hjrc,jcd->hrd", shares, columns, preferred_element_type=f32)
    proj = swap(halves_of_proj.astype(bf16), 4)

    rows = residual.shape[0]
    experts = gate_weight_experts.shape[0] * n
    capacity = 3 * rows // experts
    outgoing = build(residual, proj, feedforward_norm_gain[None], routed_expert_index, experts, capacity)
    came, gate, up = exchange_and_gather(
        outgoing, gate_weight_experts[0], up_weight_experts[0], n, lax.axis_size("tp"), 1
    )
    back = expert_rows(came, gate, up, down, capacity, 2)
    return combine(residual, proj, routed_expert_index, routed_expert_weight, back, capacity)


def solution(mesh):
    shared = P(("grp", "sp", "tp"), None)
    split = P(("grp", "sp"), "tp")
    return jax.shard_map(
        local,
        mesh=mesh,
        in_specs=(split,) * 7 + (P("tp"),) * 4 + (P("tp", None), shared, P(), shared, shared)
        + (P("sp", None, "tp"), P("sp", None, "tp"), P("sp", "tp", None)),
        out_specs=shared,
        check_vma=False,
    )
```

```python
import functools

import jax
import jax.numpy as jnp
from jax import lax
from jax.experimental import pallas as pl
from jax.experimental.pallas import tpu as pltpu
from jax.sharding import PartitionSpec as P

f32, bf16 = jnp.float32, jnp.bfloat16
MESH = pl.DeviceIdType.MESH
NN = (((1,), (0,)), ((), ()))
NT = (((1,), (1,)), ((), ()))
GROUP_EPS = 0.00064
NORM_EPS = 1e-06
SPAN = 64
LANES = 128
HEAD = 64
DECAY_SCALE = 0.6065306597126334
QUARTERS = 4
BLOCK = 4
VMEM_SPEC = pl.BlockSpec(memory_space=pltpu.VMEM)


def dot(a, b, dims=NN):
    return lax.dot_general(a.astype(bf16), b.astype(bf16), dims, preferred_element_type=f32)


def halves(x):
    high = x.astype(bf16)
    return high, (x - high.astype(f32)).astype(bf16)


def dot_split_left(a, b):
    high, low = halves(a)
    return dot(high, b) + dot(low, b)


def dot_split_right(a, b):
    high, low = halves(b)
    return dot(a, high) + dot(a, low)


def iota(shape, dim):
    return lax.broadcasted_iota(jnp.int32, shape, dim)


def sigmoid(x):
    return 1.0 / (1.0 + jnp.exp(-x))


def head_ones():
    shape = (LANES, LANES)
    return jnp.where((iota(shape, 0) >> 6) == (iota(shape, 1) >> 6), 1.0, 0.0).astype(bf16)


def stacked(x):
    first = iota(x.shape, 1) < HEAD
    zero = jnp.zeros_like(x)
    return jnp.concatenate([jnp.where(first, x, zero), jnp.where(first, zero, x)], axis=0)


def chunk_maps(units):
    row = iota((SPAN, LANES), 0)
    col = iota((SPAN, LANES), 1) & (HEAD - 1)
    square = (SPAN, SPAN)
    lower = jnp.where(iota(square, 0) >= iota(square, 1), 1.0, 0.0).astype(bf16)
    ones = head_ones()

    def each(work, *lists):
        return [work(*parts) for parts in zip(*lists)]

    def elementwise(recept, key, value, decay_pre, rate_pre, offset, decay_bias, rate_bias):
        decay_log = offset - DECAY_SCALE * sigmoid(decay_bias + decay_pre.astype(f32))
        key = key.astype(f32)
        return decay_log, dot_split_right(lower, decay_log), dot_split_left(key * key, ones)

    def scaled(unit, first):
        recept, key, value, decay_pre, rate_pre, offset, decay_bias, rate_bias = unit
        decay_log, cumul, norm = first
        key = key.astype(f32)
        rate = sigmoid(rate_bias + rate_pre.astype(f32))
        unit_key = key * lax.rsqrt(norm + NORM_EPS)
        middle = cumul[SPAN // 2 - 1 : SPAN // 2, :]
        rel = cumul - middle
        rise, fall = jnp.exp(rel), jnp.exp(-rel)
        to_middle = jnp.exp(middle)
        to_end = jnp.exp(cumul[SPAN - 1 : SPAN, :] - middle)
        remove = -unit_key * jnp.exp(rel - decay_log)
        read = recept.astype(f32) * rise
        write = unit_key * rate * fall
        keys = key * fall
        left = jnp.concatenate([remove.astype(bf16), read.astype(bf16)], axis=0)
        right = jnp.concatenate([stacked(write.astype(bf16)), stacked(keys.astype(bf16))], axis=0)
        from_start = [(remove * to_middle).astype(bf16), (read * to_middle).astype(bf16)]
        write_end = jnp.concatenate([write * to_end, keys * to_end], axis=0).T.astype(bf16)
        ending = jnp.broadcast_to(to_end * to_middle, (LANES, LANES)).T
        return dot(left, right, NT), from_start, write_end, ending

    first = [elementwise(*unit) for unit in units]
    second = each(scaled, units, first)
    scores = [item[0] for item in second]
    strict, within = row > col, row >= col

    def merging(level):
        size = 1 << level
        same = (row >> (level + 1)) == (col >> (level + 1))
        return same & ((row & size) != 0) & ((col & size) == 0)

    lower_part = [jnp.where(strict, s[:SPAN, :LANES], 0.0).astype(bf16) for s in scores]
    remove_key = [jnp.where(strict, s[:SPAN, LANES:], 0.0).astype(bf16) for s in scores]
    within_maps = [
        jnp.where(
            jnp.concatenate([within, within], axis=1), s[SPAN:], 0.0
        ).astype(bf16)
        for s in scores
    ]
    removed_value = [dot(m, stacked(unit[2])).astype(bf16) for m, unit in zip(remove_key, units)]
    inverse = [jnp.where(row == col, 1.0, jnp.where(merging(0), m.astype(f32), 0.0)) for m in lower_part]
    for level in range(1, SPAN.bit_length() - 1):
        chosen = merging(level)
        inner = [
            dot(jnp.where(chosen, m, jnp.zeros_like(m)), stacked(x.astype(bf16)))
            for m, x in zip(lower_part, inverse)
        ]
        inverse = [x + dot(x, stacked(y.astype(bf16))) for x, y in zip(inverse, inner)]
    solved = [
        dot(x, jnp.concatenate([stacked(item[1][0]), stacked(v)], axis=1))
        for x, item, v in zip(inverse, second, removed_value)
    ]
    return [
        (jnp.concatenate([q[:, :LANES].astype(bf16), item[1][1]], axis=0), q[:, LANES:], maps) + item[2:]
        for q, item, maps in zip(solved, second, within_maps)
    ]


def mixer_kernel(
    pairs, chunks,
    recept_ref, key_ref, value_ref, decay_ref, rate_ref, offset_ref, decay_bias_ref, rate_bias_ref,
    summary_ref, map_ref, own_ref,
    left_ref, solved_ref, within_ref, write_ref, ending_ref, state_ref, removed_ref, partial_ref,
):
    first_head = iota((SPAN, LANES), 1) < HEAD

    def rows_of(c):
        return pl.ds(pl.multiple_of(c * SPAN, SPAN), SPAN)

    unroll = 2 if chunks % 2 == 0 else 1

    def prepare(i, _):
        places = [(i * unroll + k, p) for k in range(unroll) for p in range(pairs)]
        units = []
        for c, p in places:
            rows, cols = rows_of(c), slice(p * LANES, (p + 1) * LANES)
            offset = jnp.where(
                first_head, offset_ref[rows, 2 * p : 2 * p + 1], offset_ref[rows, 2 * p + 1 : 2 * p + 2]
            )
            units.append(
                (
                    recept_ref[rows, cols], key_ref[rows, cols], value_ref[rows, cols],
                    decay_ref[rows, cols], rate_ref[rows, cols], offset,
                    decay_bias_ref[:, cols], rate_bias_ref[:, cols],
                )
            )
        for (c, p), (left, solved, within, write, ending) in zip(places, chunk_maps(units)):
            left_ref[c, p] = left
            solved_ref[c, p] = solved
            within_ref[c, p] = within
            write_ref[c, p] = write
            ending_ref[c, p] = ending
        return 0

    lax.fori_loop(0, chunks // unroll, prepare, 0)

    square = (LANES, LANES)
    eye = jnp.where(iota(square, 0) == iota(square, 1), 1.0, 0.0)
    for p in range(pairs):
        state_ref[p, :, :LANES] = eye
        state_ref[p, :, LANES:] = jnp.zeros(square, f32)
    own_block = (iota((LANES, 2 * LANES), 0) >> 6) == ((iota((LANES, 2 * LANES), 1) >> 6) & 1)

    def advance(c, _):
        rows = rows_of(c)
        states = [state_ref[p] for p in range(pairs)]
        crossed = [dot(left_ref[c, p], states[p]) for p in range(pairs)]
        removed = [
            jnp.concatenate(
                [x[:SPAN, :LANES], x[:SPAN, LANES:] + solved_ref[c, p]], axis=1
            ).astype(bf16)
            for p, x in enumerate(crossed)
        ]
        updates = []
        for p in range(pairs):
            value = value_ref[rows, p * LANES : (p + 1) * LANES]
            right = jnp.concatenate(
                [removed[p], jnp.concatenate([jnp.zeros_like(value), value], axis=1)], axis=0
            )
            updates.append(dot(write_ref[c, p], right))
        for p in range(pairs):
            removed_ref[c, p] = removed[p]
            partial_ref[c, p] = crossed[p][SPAN:]
            ending = ending_ref[c, p]
            state_ref[p] = states[p] * jnp.concatenate([ending, ending], axis=1) + jnp.where(
                own_block, updates[p], 0.0
            )
        return 0

    lax.fori_loop(0, chunks, advance, 0)

    for p in range(pairs):
        transit = state_ref[p, :, :LANES] - eye
        added = state_ref[p, :, LANES:]
        summary_ref[p, 0] = (transit[:HEAD] + transit[HEAD:]).astype(bf16)
        summary_ref[p, 1] = (added[:HEAD] + added[HEAD:]).astype(bf16)

    def emit(c, _):
        rows = rows_of(c)
        for p in range(pairs):
            cols = slice(p * LANES, (p + 1) * LANES)
            removed = removed_ref[c, p]
            value = stacked(value_ref[rows, cols])
            right = jnp.concatenate(
                [
                    jnp.concatenate([stacked(removed[:, :LANES]), stacked(removed[:, LANES:])], axis=1),
                    jnp.concatenate([jnp.zeros_like(value), value], axis=1),
                ],
                axis=0,
            )
            both = partial_ref[c, p] + dot(within_ref[c, p], right)
            map_ref[rows, cols] = both[:, :LANES].astype(bf16)
            own_ref[rows, cols] = both[:, LANES:]
        return 0

    lax.fori_loop(0, chunks, emit, 0)


def mixer_local(recept, key, value, decay, rate, offset, decay_bias, rate_bias):
    length, width = recept.shape
    pairs, chunks = width // LANES, length // SPAN
    per = (chunks, pairs)
    return pl.pallas_call(
        functools.partial(mixer_kernel, pairs, chunks),
        name="mixer_local",
        out_shape=(
            jax.ShapeDtypeStruct((pairs, 2, HEAD, LANES), bf16),
            jax.ShapeDtypeStruct((length, width), bf16),
            jax.ShapeDtypeStruct((length, width), f32),
        ),
        in_specs=[VMEM_SPEC] * 8,
        out_specs=(VMEM_SPEC,) * 3,
        scratch_shapes=[
            pltpu.VMEM(per + (2 * SPAN, LANES), bf16),
            pltpu.VMEM(per + (SPAN, LANES), f32),
            pltpu.VMEM(per + (SPAN, 2 * LANES), bf16),
            pltpu.VMEM(per + (LANES, 2 * SPAN), bf16),
            pltpu.VMEM(per + (LANES, LANES), f32),
            pltpu.VMEM((pairs, LANES, 2 * LANES), f32),
            pltpu.VMEM(per + (SPAN, 2 * LANES), bf16),
            pltpu.VMEM(per + (SPAN, 2 * LANES), f32),
        ],
        cost_estimate=pl.CostEstimate(
            flops=80 * 2 * LANES * length * width, bytes_accessed=12 * length * width, transcendentals=0
        ),
    )(recept, key, value, decay, rate, offset, decay_bias, rate_bias)


def prefix_kernel(
    n, m, pairs, summary_ref, shard_ref, enter_ref, whole_ref,
    got, states, entry, stage, sent1, came1, sent2, came2,
    in_sem, out_sem, ring_sent, ring_came, pass_sent, pass_came,
):
    me, col = lax.axis_index("sp"), lax.axis_index("tp")
    right, left = lax.rem(col + 1, m), lax.rem(col + m - 1, m)
    half = stage.shape[0] // 2
    load = pltpu.make_async_copy(shard_ref.at[pl.ds(0, 2 * half)], stage, in_sem)
    store = pltpu.make_async_copy(stage, whole_ref.at[col], out_sem)
    load.start()

    def part(h):
        return pl.ds(h * half, half)

    def hop(d, h):
        return pltpu.make_async_remote_copy(
            src_ref=stage.at[part(h)], dst_ref=whole_ref.at[col, part(h)],
            send_sem=ring_sent.at[d, h], recv_sem=ring_came.at[d, h],
            device_id={"tp": (right, left)[d]}, device_id_type=MESH,
        )

    def hop_in(d, h):
        frm = (left, right)[d]
        return pltpu.make_async_remote_copy(
            src_ref=stage.at[part(h)], dst_ref=whole_ref.at[frm, part(h)],
            send_sem=ring_sent.at[d, h], recv_sem=ring_came.at[d, h],
            device_id={"tp": frm}, device_id_type=MESH,
        )

    def onward(d):
        frm = (left, right)[d]
        return pltpu.make_async_remote_copy(
            src_ref=whole_ref.at[frm, part(d)], dst_ref=whole_ref.at[frm, part(d)],
            send_sem=pass_sent.at[d], recv_sem=pass_came.at[d],
            device_id={"tp": (right, left)[d]}, device_id_type=MESH,
        )

    def onward_in(d):
        frm = lax.rem(col + 2, m)
        return pltpu.make_async_remote_copy(
            src_ref=whole_ref.at[frm, part(d)], dst_ref=whole_ref.at[frm, part(d)],
            send_sem=pass_sent.at[d], recv_sem=pass_came.at[d],
            device_id={"tp": (left, right)[d]}, device_id_type=MESH,
        )

    stride = n // pairs
    works = lax.rem(me, stride) == 0
    mine = lax.div(me, stride)
    barrier = pltpu.get_barrier_semaphore()

    def greet(device):
        pl.semaphore_signal(barrier, inc=1, device_id={"sp": device}, device_id_type=MESH)

    for side in (left, right):
        pl.semaphore_signal(barrier, inc=1, device_id={"tp": side}, device_id_type=MESH)

    @pl.when(works)
    def _():
        def body(j, _):
            greet(lax.rem(me + j, n))
            return 0

        lax.fori_loop(1, n, body, 0)
        pl.semaphore_wait(barrier, n + 1)

    @pl.when(jnp.logical_not(works))
    def _():
        for p in range(pairs):
            greet(p * stride)
        pl.semaphore_wait(barrier, pairs + 2)

    def outward(p):
        return pltpu.make_async_remote_copy(
            src_ref=summary_ref.at[p], dst_ref=got.at[me], send_sem=sent1.at[p], recv_sem=came1.at[me],
            device_id={"sp": p * stride}, device_id_type=MESH,
        )

    def inward(i):
        return pltpu.make_async_remote_copy(
            src_ref=summary_ref.at[0], dst_ref=got.at[i], send_sem=sent1.at[0], recv_sem=came1.at[i],
            device_id={"sp": i}, device_id_type=MESH,
        )

    def back(i, p):
        return pltpu.make_async_remote_copy(
            src_ref=states.at[i], dst_ref=entry.at[p], send_sem=sent2.at[i], recv_sem=came2.at[p],
            device_id={"sp": i}, device_id_type=MESH,
        )

    for p in range(pairs):
        @pl.when(me != p * stride)
        def _():
            outward(p).start()

        @pl.when(me == p * stride)
        def _():
            got[me] = summary_ref[p]

    load.wait()
    for d, h in ((0, 0), (1, 1), (0, 1), (1, 0)):
        hop(d, h).start()
    store.start()

    @pl.when(works)
    def _():
        def step(i, state):
            states[i] = state.astype(bf16)

            @pl.when(i != me)
            def _():
                back(i, mine).start()
                inward(i).wait_recv()

            @pl.when(i == me)
            def _():
                entry[mine] = states[i]

            high, low = halves(state)
            transit, added = got[i, 0], got[i, 1].astype(f32)
            moved = dot(transit, stacked(high)) + dot(transit, stacked(low))
            return state + (moved + added)

        lax.fori_loop(0, n, step, jnp.zeros((HEAD, LANES), f32))

    for d in range(2):
        hop_in(d, d).wait_recv()
        onward(d).start()

    for p in range(pairs):
        @pl.when(me != p * stride)
        def _():
            back(0, p).wait_recv()

        enter_ref[p] = entry[p]

    for p in range(pairs):
        @pl.when(me != p * stride)
        def _():
            outward(p).wait_send()

    @pl.when(works)
    def _():
        def body(i, _):
            @pl.when(i != me)
            def _():
                back(i, mine).wait_send()

            return 0

        lax.fori_loop(0, n, body, 0)

    store.wait()
    for d in range(2):
        hop_in(d, 1 - d).wait_recv()
        onward_in(d).wait_recv()
        onward(d).wait_send()
        for h in range(2):
            hop(d, h).wait_send()


def prefix_states(summary, shard, early, n, m):
    pairs = summary.shape[0]
    any_spec = pl.BlockSpec(memory_space=pl.ANY)
    return pl.pallas_call(
        functools.partial(prefix_kernel, n, m, pairs),
        name="prefix_states",
        out_shape=(
            jax.ShapeDtypeStruct((pairs, HEAD, LANES), bf16),
            jax.ShapeDtypeStruct((m, early, shard.shape[1]), shard.dtype),
        ),
        in_specs=[VMEM_SPEC, any_spec],
        out_specs=(VMEM_SPEC, any_spec),
        scratch_shapes=[
            pltpu.VMEM((n, 2, HEAD, LANES), bf16),
            pltpu.VMEM((n, HEAD, LANES), bf16),
            pltpu.VMEM((pairs, HEAD, LANES), bf16),
            pltpu.VMEM((early, shard.shape[1]), shard.dtype),
            pltpu.SemaphoreType.DMA((pairs,)),
            pltpu.SemaphoreType.DMA((n,)),
            pltpu.SemaphoreType.DMA((n,)),
            pltpu.SemaphoreType.DMA((pairs,)),
            pltpu.SemaphoreType.DMA,
            pltpu.SemaphoreType.DMA,
            pltpu.SemaphoreType.DMA((2, 2)),
            pltpu.SemaphoreType.DMA((2, 2)),
            pltpu.SemaphoreType.DMA((2,)),
            pltpu.SemaphoreType.DMA((2,)),
        ],
        compiler_params=pltpu.CompilerParams(collective_id=0, has_side_effects=True),
        cost_estimate=pl.CostEstimate(flops=10**9, bytes_accessed=60 << 20, transcendentals=0),
    )(summary, shard)


def readout_kernel(
    pairs, length, recept_ref, key_ref, value_ref, gate_ref, gain_ref, self_ref, map_ref, own_ref,
    enter_ref, out_ref,
):
    ones = head_ones()
    step = 128

    def some(i, _):
        rows = pl.ds(pl.multiple_of(i * step, step), step)
        every = [slice(p * LANES, (p + 1) * LANES) for p in range(pairs)]
        own = [
            recept_ref[rows, c].astype(f32) * key_ref[rows, c].astype(f32) * self_ref[:, c] for c in every
        ]
        read = [
            dot(map_ref[rows, c], stacked(enter_ref[p])) + own_ref[rows, c] for p, c in enumerate(every)
        ]
        own = [dot_split_left(x, ones) for x in own]
        mean = [dot_split_left(x, ones) * (1.0 / HEAD) for x in read]
        center = [x - y for x, y in zip(read, mean)]
        spread = [dot_split_left(x * x, ones) * (1.0 / HEAD) for x in center]
        for p, c in enumerate(every):
            normed = center[p] * lax.rsqrt(spread[p] + GROUP_EPS) * gain_ref[:, c]
            value = value_ref[rows, c].astype(f32)
            out_ref[rows, c] = (
                (normed + own[p] * value) * gate_ref[rows, c].astype(f32)
            ).astype(bf16)
        return 0

    lax.fori_loop(0, length // step, some, 0)


def readout(recept, key, value, gate, gain, self_weight, maps, own, enter):
    length, width = recept.shape
    return pl.pallas_call(
        functools.partial(readout_kernel, width // LANES, length),
        name="readout",
        out_shape=jax.ShapeDtypeStruct((length, width), bf16),
        in_specs=[VMEM_SPEC] * 9,
        out_specs=VMEM_SPEC,
        cost_estimate=pl.CostEstimate(flops=10**9, bytes_accessed=16 << 20, transcendentals=0),
    )(recept, key, value, gate, gain, self_weight, maps, own, enter)


def route_columns(index_ref, experts, capacity):
    rows = index_ref.shape[0]
    lane = iota((rows, LANES), 1)
    first = lane == index_ref[:, 0:1]
    second = lane == index_ref[:, 1:2]
    square = (rows, rows)
    before = jnp.where(iota(square, 0) > iota(square, 1), 1.0, 0.0)
    both = jnp.where(first, 1.0, 0.0) + jnp.where(second, 1.0, 0.0)
    counts = dot(before, both) + (lane * capacity).astype(f32)
    return [jnp.sum(jnp.where(hit, counts, 0.0), axis=1, keepdims=True) for hit in (first, second)]


def build_kernel(experts, capacity, residual_ref, proj_ref, gain_ref, index_ref, out_ref, stack_ref):
    rows, width = residual_ref.shape
    part = width // QUARTERS
    proj = jnp.concatenate([proj_ref[0], proj_ref[1]], axis=1)
    stream = residual_ref[...].astype(f32) + proj.astype(f32)
    scale = lax.rsqrt(jnp.mean(stream * stream, axis=1, keepdims=True) + NORM_EPS)
    ffn_in = (stream * scale * gain_ref[...]).astype(bf16)
    for q in range(QUARTERS):
        stack_ref[q * rows : (q + 1) * rows] = ffn_in[:, q * part : (q + 1) * part]
    targets = [
        jnp.broadcast_to(t, (rows, rows)).T[:1] for t in route_columns(index_ref, experts, capacity)
    ]
    block = QUARTERS * capacity
    many = BLOCK * block
    line = iota((many, 1), 0)
    device = lax.div(line, block)
    quarter = lax.div(lax.rem(line, block), capacity)
    slot = (device * capacity + lax.rem(line, capacity)).astype(f32)
    for g in range(experts // BLOCK):
        wanted = slot + float(g * BLOCK * capacity)
        hit = jnp.where((wanted == targets[0]) | (wanted == targets[1]), 1.0, 0.0)
        place = jnp.concatenate(
            [jnp.where(quarter == q, hit, 0.0) for q in range(QUARTERS)], axis=1
        ).astype(bf16)
        lines = dot(place, stack_ref[...]).astype(bf16)
        for k in range(BLOCK):
            out_ref[g * BLOCK + k] = lines[k * block : (k + 1) * block]


def build(residual, proj, gain, index, experts, capacity):
    rows, width = residual.shape
    return pl.pallas_call(
        functools.partial(build_kernel, experts, capacity),
        name="build",
        out_shape=jax.ShapeDtypeStruct((experts, QUARTERS * capacity, width // QUARTERS), bf16),
        in_specs=[VMEM_SPEC] * 4,
        out_specs=VMEM_SPEC,
        scratch_shapes=[pltpu.VMEM((QUARTERS * rows, width // QUARTERS), bf16)],
        cost_estimate=pl.CostEstimate(flops=10**9, bytes_accessed=8 << 20, transcendentals=0),
    )(residual, proj, gain, index)


def other_core(me):
    return me + 1 - 2 * lax.rem(me, 2)


def spread_kernel(m, src_ref, out_ref, own_sem, sent, came, pass_sent, pass_came):
    me, col = lax.axis_index("sp"), lax.axis_index("tp")
    core, partner = lax.rem(me, 2), other_core(me)
    barrier = pltpu.get_barrier_semaphore()
    pl.semaphore_signal(barrier, inc=1, device_id={"sp": partner}, device_id_type=MESH)
    for k in range(1, m):
        pl.semaphore_signal(
            barrier, inc=1, device_id={"tp": lax.rem(col + k, m)}, device_id_type=MESH
        )
    own = pltpu.make_async_copy(src_ref.at[col], out_ref.at[core, col], own_sem)
    own.start()
    pl.semaphore_wait(barrier, m)

    def send(k):
        to = lax.rem(col + k, m)
        return pltpu.make_async_remote_copy(
            src_ref=src_ref.at[to], dst_ref=out_ref.at[core, col], send_sem=sent.at[k],
            recv_sem=came.at[k], device_id={"tp": to}, device_id_type=MESH,
        )

    def arrival(k):
        frm = lax.rem(col + m - k, m)
        return pltpu.make_async_remote_copy(
            src_ref=src_ref.at[frm], dst_ref=out_ref.at[core, frm], send_sem=sent.at[k],
            recv_sem=came.at[k], device_id={"tp": frm}, device_id_type=MESH,
        )

    def onward(k, source):
        frm = lax.rem(col + m - k, m)
        return pltpu.make_async_remote_copy(
            src_ref=source, dst_ref=out_ref.at[core, frm], send_sem=pass_sent.at[k],
            recv_sem=pass_came.at[k], device_id={"sp": partner}, device_id_type=MESH,
        )

    def from_partner(k):
        frm = lax.rem(col + m - k, m)
        return pltpu.make_async_remote_copy(
            src_ref=src_ref.at[frm], dst_ref=out_ref.at[1 - core, frm], send_sem=pass_sent.at[k],
            recv_sem=pass_came.at[k], device_id={"sp": partner}, device_id_type=MESH,
        )

    order = [m // 2] + [k for k in range(1, m) if k != m // 2]
    for k in order:
        send(k).start()
    onward(0, src_ref.at[col]).start()
    passed = [k for k in range(1, m) if k != m // 2] + [m // 2]
    for k in passed:
        arrival(k).wait_recv()
        onward(k, out_ref.at[core, lax.rem(col + m - k, m)]).start()
    own.wait()
    for k in range(m):
        from_partner(k).wait_recv()
        onward(k, src_ref.at[col]).wait_send()
    for k in range(1, m):
        send(k).wait_send()


def spread(blocks, m, number):
    return pl.pallas_call(
        functools.partial(spread_kernel, m),
        name="spread",
        out_shape=jax.ShapeDtypeStruct((2,) + blocks.shape, blocks.dtype),
        in_specs=[VMEM_SPEC],
        out_specs=VMEM_SPEC,
        scratch_shapes=[pltpu.SemaphoreType.DMA] + [pltpu.SemaphoreType.DMA((m,))] * 4,
        compiler_params=pltpu.CompilerParams(collective_id=number, has_side_effects=True),
        cost_estimate=pl.CostEstimate(flops=10**6, bytes_accessed=40 << 20, transcendentals=0),
    )(blocks)


def swap_kernel(src_ref, out_ref, own_sem, sent, came):
    me = lax.axis_index("sp")
    core, partner = lax.rem(me, 2), other_core(me)
    barrier = pltpu.get_barrier_semaphore()
    pl.semaphore_signal(barrier, inc=1, device_id={"sp": partner}, device_id_type=MESH)
    own = pltpu.make_async_copy(src_ref.at[core], out_ref.at[core], own_sem)
    own.start()
    pl.semaphore_wait(barrier, 1)
    away = pltpu.make_async_remote_copy(
        src_ref=src_ref.at[1 - core], dst_ref=out_ref.at[core], send_sem=sent, recv_sem=came,
        device_id={"sp": partner}, device_id_type=MESH,
    )
    away.start()
    own.wait()
    pltpu.make_async_remote_copy(
        src_ref=src_ref.at[1 - core], dst_ref=out_ref.at[1 - core], send_sem=sent, recv_sem=came,
        device_id={"sp": partner}, device_id_type=MESH,
    ).wait_recv()
    away.wait_send()


def swap(blocks, number):
    return pl.pallas_call(
        swap_kernel,
        name="swap",
        out_shape=jax.ShapeDtypeStruct(blocks.shape, blocks.dtype),
        in_specs=[VMEM_SPEC],
        out_specs=VMEM_SPEC,
        scratch_shapes=[pltpu.SemaphoreType.DMA] * 3,
        compiler_params=pltpu.CompilerParams(collective_id=number, has_side_effects=True),
        cost_estimate=pl.CostEstimate(flops=10**6, bytes_accessed=4 << 20, transcendentals=0),
    )(blocks)


def exchange_gather_kernel(n, m, skip, src_ref, first_ref, second_ref, out_ref, first_all, second_all,
                           first_stage, second_stage, own_sem, sent, came, in_sem, out_sem, ring_sent, ring_came, pass_sent, pass_came):
    me, col = lax.axis_index("sp"), lax.axis_index("tp")
    right, left = lax.rem(col + 1, m), lax.rem(col + m - 1, m)
    counts = (first_ref.shape[0] - skip, second_ref.shape[0])
    shards = (first_ref.at[pl.ds(skip, counts[0])], second_ref)
    wholes, stage = (first_all, second_all), (first_stage, second_stage)
    barrier = pltpu.get_barrier_semaphore()

    def greet(k, _):
        pl.semaphore_signal(
            barrier, inc=1, device_id={"sp": lax.rem(me + k, n)}, device_id_type=MESH
        )
        return 0

    for side in (left, right):
        pl.semaphore_signal(barrier, inc=1, device_id={"tp": side}, device_id_type=MESH)
    lax.fori_loop(1, n, greet, 0)
    own = pltpu.make_async_copy(src_ref.at[me], out_ref.at[me], own_sem)
    own.start()
    loads = [pltpu.make_async_copy(shards[a], stage[a], in_sem.at[a]) for a in range(2)]
    stores = [pltpu.make_async_copy(stage[a], wholes[a].at[col], out_sem.at[a]) for a in range(2)]
    for load in loads:
        load.start()
    for load in loads:
        load.wait()
    pl.semaphore_wait(barrier, n + 1)

    def copy(k):
        to = lax.rem(me + k, n)
        return pltpu.make_async_remote_copy(
            src_ref=src_ref.at[to], dst_ref=out_ref.at[me], send_sem=sent.at[k], recv_sem=came.at[k],
            device_id={"sp": to}, device_id_type=MESH,
        )

    def start(k, _):
        away = n // 2 - lax.div(k, 2)
        copy(jnp.where(lax.rem(k, 2) == 0, away, n - away)).start()
        return 0

    def arrived(k):
        frm = lax.rem(me + n - k, n)
        return pltpu.make_async_remote_copy(
            src_ref=src_ref.at[frm], dst_ref=out_ref.at[frm], send_sem=sent.at[k], recv_sem=came.at[k],
            device_id={"sp": frm}, device_id_type=MESH,
        )

    def rows(a, h):
        return pl.ds(h * (counts[a] // 2), counts[a] // 2)

    def hop(a, d, h):
        return pltpu.make_async_remote_copy(
            src_ref=stage[a].at[rows(a, h)], dst_ref=wholes[a].at[col, rows(a, h)],
            send_sem=ring_sent.at[a, d, h], recv_sem=ring_came.at[a, d, h],
            device_id={"tp": (right, left)[d]}, device_id_type=MESH,
        )

    def hop_in(a, d, h):
        frm = (left, right)[d]
        return pltpu.make_async_remote_copy(
            src_ref=stage[a].at[rows(a, h)], dst_ref=wholes[a].at[frm, rows(a, h)],
            send_sem=ring_sent.at[a, d, h], recv_sem=ring_came.at[a, d, h],
            device_id={"tp": frm}, device_id_type=MESH,
        )

    def onward(a, d):
        frm = (left, right)[d]
        return pltpu.make_async_remote_copy(
            src_ref=wholes[a].at[frm, rows(a, d)], dst_ref=wholes[a].at[frm, rows(a, d)],
            send_sem=pass_sent.at[a, d], recv_sem=pass_came.at[a, d],
            device_id={"tp": (right, left)[d]}, device_id_type=MESH,
        )

    def onward_in(a, d):
        frm = lax.rem(col + 2, m)
        return pltpu.make_async_remote_copy(
            src_ref=wholes[a].at[frm, rows(a, d)], dst_ref=wholes[a].at[frm, rows(a, d)],
            send_sem=pass_sent.at[a, d], recv_sem=pass_came.at[a, d],
            device_id={"tp": (left, right)[d]}, device_id_type=MESH,
        )

    copy(n // 2).start()
    lax.fori_loop(2, n, start, 0)
    for a in range(2):
        for d, h in ((0, 0), (1, 1), (0, 1), (1, 0)):
            hop(a, d, h).start()
    for store in stores:
        store.start()
    for a in range(2):
        for d in range(2):
            hop_in(a, d, d).wait_recv()
            onward(a, d).start()
    own.wait()
    for store in stores:
        store.wait()

    def finish(k, _):
        arrived(k).wait_recv()
        copy(k).wait_send()
        return 0

    lax.fori_loop(1, n, finish, 0)
    for a in range(2):
        for d in range(2):
            hop_in(a, d, 1 - d).wait_recv()
            onward_in(a, d).wait_recv()
            onward(a, d).wait_send()
            for h in range(2):
                hop(a, d, h).wait_send()


def exchange_and_gather(blocks, first, second, skip, n, m, number):
    any_spec = pl.BlockSpec(memory_space=pl.ANY)
    tail = (first.shape[0] - skip, first.shape[1])
    return pl.pallas_call(
        functools.partial(exchange_gather_kernel, n, m, skip),
        name=f"exchange_{number}",
        out_shape=(
            jax.ShapeDtypeStruct(blocks.shape, blocks.dtype),
            jax.ShapeDtypeStruct((m,) + tail, first.dtype),
            jax.ShapeDtypeStruct((m,) + second.shape, second.dtype),
        ),
        in_specs=[VMEM_SPEC, any_spec, any_spec],
        out_specs=(VMEM_SPEC, any_spec, any_spec),
        scratch_shapes=[
            pltpu.VMEM(tail, first.dtype),
            pltpu.VMEM(second.shape, second.dtype),
            pltpu.SemaphoreType.DMA,
            pltpu.SemaphoreType.DMA((n,)),
            pltpu.SemaphoreType.DMA((n,)),
            pltpu.SemaphoreType.DMA((2,)),
            pltpu.SemaphoreType.DMA((2,)),
            pltpu.SemaphoreType.DMA((2, 2, 2)),
            pltpu.SemaphoreType.DMA((2, 2, 2)),
            pltpu.SemaphoreType.DMA((2, 2)),
            pltpu.SemaphoreType.DMA((2, 2)),
        ],
        compiler_params=pltpu.CompilerParams(collective_id=number, has_side_effects=True),
        cost_estimate=pl.CostEstimate(flops=10**6, bytes_accessed=200 << 20, transcendentals=0),
    )(blocks, first, second)


def reorder(capacity, to_rows):
    many = BLOCK * QUARTERS * capacity
    square = (many, many)
    out, line = (iota(square, 0), iota(square, 1)) if to_rows else (iota(square, 1), iota(square, 0))
    device, quarter = lax.div(line, QUARTERS * capacity), lax.rem(lax.div(line, capacity), QUARTERS)
    place = (quarter * BLOCK + device) * capacity + lax.rem(line, capacity)
    return jnp.where(out == place, 1.0, 0.0).astype(bf16)


def expert_kernel(
    n, capacity, came_ref, early_ref, gate_ref, up_ref, down_ref, out_ref,
    gates, ups, downs, rows_ref, back_ref, load_sem, sent, came,
):
    me = lax.axis_index("sp")
    block = QUARTERS * capacity
    height = BLOCK * capacity
    part = out_ref.shape[2]
    pieces = gates.shape[0]
    groups = n // BLOCK
    loads = []
    for j in range(pieces):
        early = early_ref.shape[1]
        moves = (
            (early_ref.at[j], gates.at[j, pl.ds(0, early)]),
            (gate_ref.at[j], gates.at[j, pl.ds(early, gate_ref.shape[1])]),
            (up_ref.at[j], ups.at[j]),
            (down_ref.at[j], downs.at[j]),
        )
        for w, (source, target) in enumerate(moves):
            loads.append(pltpu.make_async_copy(source, target, load_sem.at[j, w]))
    for load in loads:
        load.start()
    barrier = pltpu.get_barrier_semaphore()

    def greet(k, _):
        pl.semaphore_signal(
            barrier, inc=1, device_id={"sp": lax.rem(me + k, n)}, device_id_type=MESH
        )
        return 0

    lax.fori_loop(1, n, greet, 0)
    gather_order, spread_order = reorder(capacity, True), reorder(capacity, False)
    for load in loads:
        load.wait()
    pl.semaphore_wait(barrier, n - 1)

    def home(device):
        return pltpu.make_async_remote_copy(
            src_ref=back_ref.at[device], dst_ref=out_ref.at[me], send_sem=sent.at[device],
            recv_sem=came.at[me], device_id={"sp": device}, device_id_type=MESH,
        )

    def work(c, _):
        own_group = lax.div(me, BLOCK)
        both = (
            lax.rem(own_group + groups // 2 + c, groups),
            lax.rem(own_group + groups // 2 - 1 - c + groups, groups),
        )
        for i, g in enumerate(both):
            lines = jnp.concatenate([came_ref[g * BLOCK + k] for k in range(BLOCK)], axis=0)
            moved = dot(gather_order, lines).astype(bf16)
            for q in range(QUARTERS):
                rows_ref[i * height : (i + 1) * height, q * part : (q + 1) * part] = moved[
                    q * height : (q + 1) * height
                ]
        rows = rows_ref[...]
        hidden = []
        for j in range(pieces):
            gated = dot(rows, gates[j])
            hidden.append((gated * sigmoid(gated) * dot(rows, ups[j])).astype(bf16))
        total = dot(hidden[0], downs[0])
        for j in range(1, pieces):
            total = total + dot(hidden[j], downs[j])
        total = total.astype(bf16)
        for i, g in enumerate(both):
            lines = jnp.concatenate(
                [total[i * height : (i + 1) * height, q * part : (q + 1) * part] for q in range(QUARTERS)],
                axis=0,
            )
            moved = dot(spread_order, lines).astype(bf16)
            for k in range(BLOCK):
                device = g * BLOCK + k
                result = moved[k * block : (k + 1) * block]
                back_ref[device] = result

                @pl.when(device == me)
                def _():
                    out_ref[me] = result

        for g in both:
            for k in range(BLOCK):
                device = g * BLOCK + k

                @pl.when(device != me)
                def _():
                    home(device).start()

        return 0

    lax.fori_loop(0, groups // 2, work, 0)

    def finish(k, _):
        frm = lax.rem(me + k, n)
        pltpu.make_async_remote_copy(
            src_ref=back_ref.at[frm], dst_ref=out_ref.at[frm], send_sem=sent.at[frm],
            recv_sem=came.at[frm], device_id={"sp": frm}, device_id_type=MESH,
        ).wait_recv()
        home(frm).wait_send()
        return 0

    lax.fori_loop(1, n, finish, 0)


def expert_rows(came, early, gate, up, down, capacity, number):
    n, block, part = came.shape
    pieces, width, units = up.shape
    any_spec = pl.BlockSpec(memory_space=pl.ANY)
    return pl.pallas_call(
        functools.partial(expert_kernel, n, capacity),
        name="expert_rows",
        out_shape=jax.ShapeDtypeStruct(came.shape, bf16),
        in_specs=[VMEM_SPEC, any_spec, any_spec, any_spec, any_spec],
        out_specs=VMEM_SPEC,
        scratch_shapes=[
            pltpu.VMEM(up.shape, bf16),
            pltpu.VMEM(up.shape, bf16),
            pltpu.VMEM(down.shape, bf16),
            pltpu.VMEM((2 * BLOCK * capacity, width), bf16),
            pltpu.VMEM(came.shape, bf16),
            pltpu.SemaphoreType.DMA((pieces, 4)),
            pltpu.SemaphoreType.DMA((n,)),
            pltpu.SemaphoreType.DMA((n,)),
        ],
        compiler_params=pltpu.CompilerParams(collective_id=number, has_side_effects=True),
        cost_estimate=pl.CostEstimate(flops=5 * 10**9, bytes_accessed=200 << 20, transcendentals=0),
    )(came, early, gate, up, down)


def combine_kernel(n, capacity, residual_ref, proj_ref, index_ref, weight_ref, back_ref, out_ref, rows_ref):
    rows, width = residual_ref.shape
    part = width // QUARTERS
    height = BLOCK * capacity
    order = reorder(capacity, True)
    for g in range(n // BLOCK):
        lines = jnp.concatenate([back_ref[g * BLOCK + k] for k in range(BLOCK)], axis=0)
        moved = dot(order, lines).astype(bf16)
        for q in range(QUARTERS):
            rows_ref[g * height : (g + 1) * height, q * part : (q + 1) * part] = moved[
                q * height : (q + 1) * height
            ]
    targets = route_columns(index_ref, n, capacity)
    slot = iota((rows, n * capacity), 1).astype(f32)
    mix = jnp.where(slot == targets[0], weight_ref[:, 0:1], 0.0) + jnp.where(
        slot == targets[1], weight_ref[:, 1:2], 0.0
    )
    high, low = halves(mix)
    for q in range(QUARTERS):
        cols = slice(q * part, (q + 1) * part)
        routed = dot(high, rows_ref[:, cols]) + dot(low, rows_ref[:, cols])
        half, within = divmod(q, QUARTERS // 2)
        proj = proj_ref[half, :, within * part : (within + 1) * part]
        stream = residual_ref[:, cols].astype(f32) + proj.astype(f32)
        out_ref[:, cols] = (stream + routed).astype(bf16)


def combine(residual, proj, index, weight, back, capacity):
    n = back.shape[0]
    return pl.pallas_call(
        functools.partial(combine_kernel, n, capacity),
        name="combine",
        out_shape=jax.ShapeDtypeStruct(residual.shape, bf16),
        in_specs=[VMEM_SPEC] * 5,
        out_specs=VMEM_SPEC,
        scratch_shapes=[pltpu.VMEM((n * capacity, residual.shape[1]), bf16)],
        cost_estimate=pl.CostEstimate(flops=10**9, bytes_accessed=8 << 20, transcendentals=0),
    )(residual, proj, index, weight, back)


def local(
    recept, key_input, value_input, output_gate_input, decay_input_part, correction_rate_input,
    head_decay_offset, decay_fixed_bias, correction_rate_bias, head_norm_gain, self_term_weight,
    output_weight_matrix, residual, feedforward_norm_gain, routed_expert_index, routed_expert_weight,
    gate_weight_experts, up_weight_experts, down_weight_experts,
):
    n = lax.axis_size("sp")
    cores = 2
    share = output_weight_matrix.shape[1] // cores
    columns = lax.dynamic_slice_in_dim(
        output_weight_matrix, lax.rem(lax.axis_index("sp"), cores) * share, share, axis=1
    )
    columns = lax.all_gather(columns, "tp")

    summary, maps, own = mixer_local(
        recept, key_input, value_input, decay_input_part, correction_rate_input, head_decay_offset,
        decay_fixed_bias[None], correction_rate_bias[None],
    )
    gate_shard = gate_weight_experts[0]
    early_rows = gate_shard.shape[0] // 4
    enter, early = prefix_states(summary, gate_shard, early_rows, n, lax.axis_size("tp"))
    down, enter = lax.optimization_barrier((down_weight_experts[0], enter))
    down = lax.all_gather(down, "tp")
    mixed = readout(
        recept, key_input, value_input, output_gate_input, head_norm_gain[None], self_term_weight[None],
        maps, own, enter,
    )
    m = lax.axis_size("tp")
    shares = spread(mixed.reshape(m, -1, mixed.shape[1]), m, 3)
    halves_of_proj = jnp.einsum("hjrc,jcd->hrd", shares, columns, preferred_element_type=f32)
    proj = swap(halves_of_proj.astype(bf16), 4)

    rows = residual.shape[0]
    experts = gate_weight_experts.shape[0] * n
    capacity = 3 * rows // experts
    outgoing = build(residual, proj, feedforward_norm_gain[None], routed_expert_index, experts, capacity)
    came, gate, up = exchange_and_gather(
        outgoing, gate_shard, up_weight_experts[0], early_rows, n, m, 1
    )
    back = expert_rows(came, early, gate, up, down, capacity, 2)
    return combine(residual, proj, routed_expert_index, routed_expert_weight, back, capacity)


def solution(mesh):
    shared = P(("grp", "sp", "tp"), None)
    split = P(("grp", "sp"), "tp")
    return jax.shard_map(
        local,
        mesh=mesh,
        in_specs=(split,) * 7 + (P("tp"),) * 4 + (P("tp", None), shared, P(), shared, shared)
        + (P("sp", None, "tp"), P("sp", None, "tp"), P("sp", "tp", None)),
        out_specs=shared,
        check_vma=False,
    )
```

```python
import functools

import jax
import jax.numpy as jnp
from jax import lax
from jax.experimental import pallas as pl
from jax.experimental.pallas import tpu as pltpu
from jax.sharding import PartitionSpec as P

f32, bf16 = jnp.float32, jnp.bfloat16
MESH = pl.DeviceIdType.MESH
NN = (((1,), (0,)), ((), ()))
NT = (((1,), (1,)), ((), ()))
GROUP_EPS = 0.00064
NORM_EPS = 1e-06
SPAN = 64
LANES = 128
HEAD = 64
DECAY_SCALE = 0.6065306597126334
QUARTERS = 4
BLOCK = 4
VMEM_SPEC = pl.BlockSpec(memory_space=pltpu.VMEM)


def dot(a, b, dims=NN):
    return lax.dot_general(a.astype(bf16), b.astype(bf16), dims, preferred_element_type=f32)


def halves(x):
    high = x.astype(bf16)
    return high, (x - high.astype(f32)).astype(bf16)


def dot_split_left(a, b):
    high, low = halves(a)
    return dot(high, b) + dot(low, b)


def dot_split_right(a, b):
    high, low = halves(b)
    return dot(a, high) + dot(a, low)


def iota(shape, dim):
    return lax.broadcasted_iota(jnp.int32, shape, dim)


def sigmoid(x):
    return 1.0 / (1.0 + jnp.exp(-x))


def head_ones():
    shape = (LANES, LANES)
    return jnp.where((iota(shape, 0) >> 6) == (iota(shape, 1) >> 6), 1.0, 0.0).astype(bf16)


def stacked(x):
    first = iota(x.shape, 1) < HEAD
    zero = jnp.zeros_like(x)
    return jnp.concatenate([jnp.where(first, x, zero), jnp.where(first, zero, x)], axis=0)


def chunk_maps(units):
    row = iota((SPAN, LANES), 0)
    col = iota((SPAN, LANES), 1) & (HEAD - 1)
    square = (SPAN, SPAN)
    lower = jnp.where(iota(square, 0) >= iota(square, 1), 1.0, 0.0).astype(bf16)
    ones = head_ones()

    def each(work, *lists):
        return [work(*parts) for parts in zip(*lists)]

    def elementwise(recept, key, value, decay_pre, rate_pre, offset, decay_bias, rate_bias):
        decay_log = offset - DECAY_SCALE * sigmoid(decay_bias + decay_pre.astype(f32))
        key = key.astype(f32)
        return decay_log, dot_split_right(lower, decay_log), dot_split_left(key * key, ones)

    def scaled(unit, first):
        recept, key, value, decay_pre, rate_pre, offset, decay_bias, rate_bias = unit
        decay_log, cumul, norm = first
        key = key.astype(f32)
        rate = sigmoid(rate_bias + rate_pre.astype(f32))
        unit_key = key * lax.rsqrt(norm + NORM_EPS)
        middle = cumul[SPAN // 2 - 1 : SPAN // 2, :]
        rel = cumul - middle
        rise, fall = jnp.exp(rel), jnp.exp(-rel)
        to_middle = jnp.exp(middle)
        to_end = jnp.exp(cumul[SPAN - 1 : SPAN, :] - middle)
        remove = -unit_key * jnp.exp(rel - decay_log)
        read = recept.astype(f32) * rise
        write = unit_key * rate * fall
        keys = key * fall
        left = jnp.concatenate([remove.astype(bf16), read.astype(bf16)], axis=0)
        right = jnp.concatenate([stacked(write.astype(bf16)), stacked(keys.astype(bf16))], axis=0)
        from_start = [(remove * to_middle).astype(bf16), (read * to_middle).astype(bf16)]
        write_end = jnp.concatenate([write * to_end, keys * to_end], axis=0).T.astype(bf16)
        ending = jnp.broadcast_to(to_end * to_middle, (LANES, LANES)).T
        return dot(left, right, NT), from_start, write_end, ending

    first = [elementwise(*unit) for unit in units]
    second = each(scaled, units, first)
    scores = [item[0] for item in second]
    strict, within = row > col, row >= col

    def merging(level):
        size = 1 << level
        same = (row >> (level + 1)) == (col >> (level + 1))
        return same & ((row & size) != 0) & ((col & size) == 0)

    lower_part = [jnp.where(strict, s[:SPAN, :LANES], 0.0).astype(bf16) for s in scores]
    remove_key = [jnp.where(strict, s[:SPAN, LANES:], 0.0).astype(bf16) for s in scores]
    within_maps = [
        jnp.where(
            jnp.concatenate([within, within], axis=1), s[SPAN:], 0.0
        ).astype(bf16)
        for s in scores
    ]
    removed_value = [dot(m, stacked(unit[2])).astype(bf16) for m, unit in zip(remove_key, units)]
    inverse = [jnp.where(row == col, 1.0, jnp.where(merging(0), m.astype(f32), 0.0)) for m in lower_part]
    for level in range(1, SPAN.bit_length() - 1):
        chosen = merging(level)
        inner = [
            dot(jnp.where(chosen, m, jnp.zeros_like(m)), stacked(x.astype(bf16)))
            for m, x in zip(lower_part, inverse)
        ]
        inverse = [x + dot(x, stacked(y.astype(bf16))) for x, y in zip(inverse, inner)]
    solved = [
        dot(x, jnp.concatenate([stacked(item[1][0]), stacked(v)], axis=1))
        for x, item, v in zip(inverse, second, removed_value)
    ]
    return [
        (jnp.concatenate([q[:, :LANES].astype(bf16), item[1][1]], axis=0), q[:, LANES:], maps) + item[2:]
        for q, item, maps in zip(solved, second, within_maps)
    ]


def mixer_kernel(
    pairs, chunks,
    recept_ref, key_ref, value_ref, decay_ref, rate_ref, offset_ref, decay_bias_ref, rate_bias_ref,
    summary_ref, map_ref, own_ref,
    left_ref, solved_ref, within_ref, write_ref, ending_ref, state_ref, removed_ref, partial_ref,
):
    first_head = iota((SPAN, LANES), 1) < HEAD

    def rows_of(c):
        return pl.ds(pl.multiple_of(c * SPAN, SPAN), SPAN)

    unroll = 2 if chunks % 2 == 0 else 1

    def prepare(i, _):
        places = [(i * unroll + k, p) for k in range(unroll) for p in range(pairs)]
        units = []
        for c, p in places:
            rows, cols = rows_of(c), slice(p * LANES, (p + 1) * LANES)
            offset = jnp.where(
                first_head, offset_ref[rows, 2 * p : 2 * p + 1], offset_ref[rows, 2 * p + 1 : 2 * p + 2]
            )
            units.append(
                (
                    recept_ref[rows, cols], key_ref[rows, cols], value_ref[rows, cols],
                    decay_ref[rows, cols], rate_ref[rows, cols], offset,
                    decay_bias_ref[:, cols], rate_bias_ref[:, cols],
                )
            )
        for (c, p), (left, solved, within, write, ending) in zip(places, chunk_maps(units)):
            left_ref[c, p] = left
            solved_ref[c, p] = solved
            within_ref[c, p] = within
            write_ref[c, p] = write
            ending_ref[c, p] = ending
        return 0

    lax.fori_loop(0, chunks // unroll, prepare, 0)

    square = (LANES, LANES)
    eye = jnp.where(iota(square, 0) == iota(square, 1), 1.0, 0.0)
    for p in range(pairs):
        state_ref[p, :, :LANES] = eye
        state_ref[p, :, LANES:] = jnp.zeros(square, f32)
    own_block = (iota((LANES, 2 * LANES), 0) >> 6) == ((iota((LANES, 2 * LANES), 1) >> 6) & 1)

    def advance(c, _):
        rows = rows_of(c)
        states = [state_ref[p] for p in range(pairs)]
        crossed = [dot(left_ref[c, p], states[p]) for p in range(pairs)]
        removed = [
            jnp.concatenate(
                [x[:SPAN, :LANES], x[:SPAN, LANES:] + solved_ref[c, p]], axis=1
            ).astype(bf16)
            for p, x in enumerate(crossed)
        ]
        updates = []
        for p in range(pairs):
            value = value_ref[rows, p * LANES : (p + 1) * LANES]
            right = jnp.concatenate(
                [removed[p], jnp.concatenate([jnp.zeros_like(value), value], axis=1)], axis=0
            )
            updates.append(dot(write_ref[c, p], right))
        for p in range(pairs):
            removed_ref[c, p] = removed[p]
            partial_ref[c, p] = crossed[p][SPAN:]
            ending = ending_ref[c, p]
            state_ref[p] = states[p] * jnp.concatenate([ending, ending], axis=1) + jnp.where(
                own_block, updates[p], 0.0
            )
        return 0

    lax.fori_loop(0, chunks, advance, 0)

    for p in range(pairs):
        transit = state_ref[p, :, :LANES] - eye
        added = state_ref[p, :, LANES:]
        summary_ref[p, 0] = (transit[:HEAD] + transit[HEAD:]).astype(bf16)
        summary_ref[p, 1] = (added[:HEAD] + added[HEAD:]).astype(bf16)

    def emit(c, _):
        rows = rows_of(c)
        for p in range(pairs):
            cols = slice(p * LANES, (p + 1) * LANES)
            removed = removed_ref[c, p]
            value = stacked(value_ref[rows, cols])
            right = jnp.concatenate(
                [
                    jnp.concatenate([stacked(removed[:, :LANES]), stacked(removed[:, LANES:])], axis=1),
                    jnp.concatenate([jnp.zeros_like(value), value], axis=1),
                ],
                axis=0,
            )
            both = partial_ref[c, p] + dot(within_ref[c, p], right)
            map_ref[rows, cols] = both[:, :LANES].astype(bf16)
            own_ref[rows, cols] = both[:, LANES:]
        return 0

    lax.fori_loop(0, chunks, emit, 0)


def mixer_local(recept, key, value, decay, rate, offset, decay_bias, rate_bias):
    length, width = recept.shape
    pairs, chunks = width // LANES, length // SPAN
    per = (chunks, pairs)
    return pl.pallas_call(
        functools.partial(mixer_kernel, pairs, chunks),
        name="mixer_local",
        out_shape=(
            jax.ShapeDtypeStruct((pairs, 2, HEAD, LANES), bf16),
            jax.ShapeDtypeStruct((length, width), bf16),
            jax.ShapeDtypeStruct((length, width), f32),
        ),
        in_specs=[VMEM_SPEC] * 8,
        out_specs=(VMEM_SPEC,) * 3,
        scratch_shapes=[
            pltpu.VMEM(per + (2 * SPAN, LANES), bf16),
            pltpu.VMEM(per + (SPAN, LANES), f32),
            pltpu.VMEM(per + (SPAN, 2 * LANES), bf16),
            pltpu.VMEM(per + (LANES, 2 * SPAN), bf16),
            pltpu.VMEM(per + (LANES, LANES), f32),
            pltpu.VMEM((pairs, LANES, 2 * LANES), f32),
            pltpu.VMEM(per + (SPAN, 2 * LANES), bf16),
            pltpu.VMEM(per + (SPAN, 2 * LANES), f32),
        ],
        cost_estimate=pl.CostEstimate(
            flops=80 * 2 * LANES * length * width, bytes_accessed=12 * length * width, transcendentals=0
        ),
    )(recept, key, value, decay, rate, offset, decay_bias, rate_bias)


def prefix_kernel(n, pairs, summary_ref, enter_ref, got, states, entry, sent1, came1, sent2, came2):
    me = lax.axis_index("sp")
    stride = n // pairs
    works = lax.rem(me, stride) == 0
    mine = lax.div(me, stride)
    barrier = pltpu.get_barrier_semaphore()

    def greet(device):
        pl.semaphore_signal(barrier, inc=1, device_id={"sp": device}, device_id_type=MESH)

    @pl.when(works)
    def _():
        def body(j, _):
            greet(lax.rem(me + j, n))
            return 0

        lax.fori_loop(1, n, body, 0)
        pl.semaphore_wait(barrier, n - 1)

    @pl.when(jnp.logical_not(works))
    def _():
        for p in range(pairs):
            greet(p * stride)
        pl.semaphore_wait(barrier, pairs)

    def outward(p):
        return pltpu.make_async_remote_copy(
            src_ref=summary_ref.at[p], dst_ref=got.at[me], send_sem=sent1.at[p], recv_sem=came1.at[me],
            device_id={"sp": p * stride}, device_id_type=MESH,
        )

    def inward(i):
        return pltpu.make_async_remote_copy(
            src_ref=summary_ref.at[0], dst_ref=got.at[i], send_sem=sent1.at[0], recv_sem=came1.at[i],
            device_id={"sp": i}, device_id_type=MESH,
        )

    def back(i, p):
        return pltpu.make_async_remote_copy(
            src_ref=states.at[i], dst_ref=entry.at[p], send_sem=sent2.at[i], recv_sem=came2.at[p],
            device_id={"sp": i}, device_id_type=MESH,
        )

    for p in range(pairs):
        @pl.when(me != p * stride)
        def _():
            outward(p).start()

        @pl.when(me == p * stride)
        def _():
            got[me] = summary_ref[p]

    @pl.when(works)
    def _():
        def step(i, state):
            states[i] = state.astype(bf16)

            @pl.when(i != me)
            def _():
                back(i, mine).start()
                inward(i).wait_recv()

            @pl.when(i == me)
            def _():
                entry[mine] = states[i]

            high, low = halves(state)
            transit, added = got[i, 0], got[i, 1].astype(f32)
            moved = dot(transit, stacked(high)) + dot(transit, stacked(low))
            return state + (moved + added)

        lax.fori_loop(0, n, step, jnp.zeros((HEAD, LANES), f32))

    for p in range(pairs):
        @pl.when(me != p * stride)
        def _():
            back(0, p).wait_recv()

        enter_ref[p] = entry[p]

    for p in range(pairs):
        @pl.when(me != p * stride)
        def _():
            outward(p).wait_send()

    @pl.when(works)
    def _():
        def body(i, _):
            @pl.when(i != me)
            def _():
                back(i, mine).wait_send()

            return 0

        lax.fori_loop(0, n, body, 0)


def prefix_states(summary, n):
    pairs = summary.shape[0]
    return pl.pallas_call(
        functools.partial(prefix_kernel, n, pairs),
        name="prefix_states",
        out_shape=jax.ShapeDtypeStruct((pairs, HEAD, LANES), bf16),
        in_specs=[VMEM_SPEC],
        out_specs=VMEM_SPEC,
        scratch_shapes=[
            pltpu.VMEM((n, 2, HEAD, LANES), bf16),
            pltpu.VMEM((n, HEAD, LANES), bf16),
            pltpu.VMEM((pairs, HEAD, LANES), bf16),
            pltpu.SemaphoreType.DMA((pairs,)),
            pltpu.SemaphoreType.DMA((n,)),
            pltpu.SemaphoreType.DMA((n,)),
            pltpu.SemaphoreType.DMA((pairs,)),
        ],
        compiler_params=pltpu.CompilerParams(collective_id=0, has_side_effects=True),
        cost_estimate=pl.CostEstimate(flops=10**9, bytes_accessed=60 << 20, transcendentals=0),
    )(summary)


def readout_kernel(
    pairs, length, recept_ref, key_ref, value_ref, gate_ref, gain_ref, self_ref, map_ref, own_ref,
    enter_ref, out_ref,
):
    ones = head_ones()
    step = 128

    def some(i, _):
        rows = pl.ds(pl.multiple_of(i * step, step), step)
        every = [slice(p * LANES, (p + 1) * LANES) for p in range(pairs)]
        own = [
            recept_ref[rows, c].astype(f32) * key_ref[rows, c].astype(f32) * self_ref[:, c] for c in every
        ]
        read = [
            dot(map_ref[rows, c], stacked(enter_ref[p])) + own_ref[rows, c] for p, c in enumerate(every)
        ]
        own = [dot_split_left(x, ones) for x in own]
        mean = [dot_split_left(x, ones) * (1.0 / HEAD) for x in read]
        center = [x - y for x, y in zip(read, mean)]
        spread = [dot_split_left(x * x, ones) * (1.0 / HEAD) for x in center]
        for p, c in enumerate(every):
            normed = center[p] * lax.rsqrt(spread[p] + GROUP_EPS) * gain_ref[:, c]
            value = value_ref[rows, c].astype(f32)
            out_ref[rows, c] = (
                (normed + own[p] * value) * gate_ref[rows, c].astype(f32)
            ).astype(bf16)
        return 0

    lax.fori_loop(0, length // step, some, 0)


def readout(recept, key, value, gate, gain, self_weight, maps, own, enter):
    length, width = recept.shape
    return pl.pallas_call(
        functools.partial(readout_kernel, width // LANES, length),
        name="readout",
        out_shape=jax.ShapeDtypeStruct((length, width), bf16),
        in_specs=[VMEM_SPEC] * 9,
        out_specs=VMEM_SPEC,
        cost_estimate=pl.CostEstimate(flops=10**9, bytes_accessed=16 << 20, transcendentals=0),
    )(recept, key, value, gate, gain, self_weight, maps, own, enter)


def route_columns(index_ref, experts, capacity):
    rows = index_ref.shape[0]
    lane = iota((rows, LANES), 1)
    first = lane == index_ref[:, 0:1]
    second = lane == index_ref[:, 1:2]
    square = (rows, rows)
    before = jnp.where(iota(square, 0) > iota(square, 1), 1.0, 0.0)
    both = jnp.where(first, 1.0, 0.0) + jnp.where(second, 1.0, 0.0)
    counts = dot(before, both) + (lane * capacity).astype(f32)
    return [jnp.sum(jnp.where(hit, counts, 0.0), axis=1, keepdims=True) for hit in (first, second)]


def build_kernel(experts, capacity, residual_ref, proj_ref, gain_ref, index_ref, out_ref, stack_ref):
    rows, width = residual_ref.shape
    part = width // QUARTERS
    proj = jnp.concatenate([proj_ref[0], proj_ref[1]], axis=1)
    stream = residual_ref[...].astype(f32) + proj.astype(f32)
    scale = lax.rsqrt(jnp.mean(stream * stream, axis=1, keepdims=True) + NORM_EPS)
    ffn_in = (stream * scale * gain_ref[...]).astype(bf16)
    for q in range(QUARTERS):
        stack_ref[q * rows : (q + 1) * rows] = ffn_in[:, q * part : (q + 1) * part]
    targets = [
        jnp.broadcast_to(t, (rows, rows)).T[:1] for t in route_columns(index_ref, experts, capacity)
    ]
    block = QUARTERS * capacity
    many = BLOCK * block
    line = iota((many, 1), 0)
    device = lax.div(line, block)
    quarter = lax.div(lax.rem(line, block), capacity)
    slot = (device * capacity + lax.rem(line, capacity)).astype(f32)
    for g in range(experts // BLOCK):
        wanted = slot + float(g * BLOCK * capacity)
        hit = jnp.where((wanted == targets[0]) | (wanted == targets[1]), 1.0, 0.0)
        place = jnp.concatenate(
            [jnp.where(quarter == q, hit, 0.0) for q in range(QUARTERS)], axis=1
        ).astype(bf16)
        lines = dot(place, stack_ref[...]).astype(bf16)
        for k in range(BLOCK):
            out_ref[g * BLOCK + k] = lines[k * block : (k + 1) * block]


def build(residual, proj, gain, index, experts, capacity):
    rows, width = residual.shape
    return pl.pallas_call(
        functools.partial(build_kernel, experts, capacity),
        name="build",
        out_shape=jax.ShapeDtypeStruct((experts, QUARTERS * capacity, width // QUARTERS), bf16),
        in_specs=[VMEM_SPEC] * 4,
        out_specs=VMEM_SPEC,
        scratch_shapes=[pltpu.VMEM((QUARTERS * rows, width // QUARTERS), bf16)],
        cost_estimate=pl.CostEstimate(flops=10**9, bytes_accessed=8 << 20, transcendentals=0),
    )(residual, proj, gain, index)


def other_core(me):
    return me + 1 - 2 * lax.rem(me, 2)


def spread_kernel(m, src_ref, out_ref, own_sem, sent, came, pass_sent, pass_came):
    me, col = lax.axis_index("sp"), lax.axis_index("tp")
    core, partner = lax.rem(me, 2), other_core(me)
    barrier = pltpu.get_barrier_semaphore()
    pl.semaphore_signal(barrier, inc=1, device_id={"sp": partner}, device_id_type=MESH)
    for k in range(1, m):
        pl.semaphore_signal(
            barrier, inc=1, device_id={"tp": lax.rem(col + k, m)}, device_id_type=MESH
        )
    own = pltpu.make_async_copy(src_ref.at[col], out_ref.at[core, col], own_sem)
    own.start()
    pl.semaphore_wait(barrier, m)

    def send(k):
        to = lax.rem(col + k, m)
        return pltpu.make_async_remote_copy(
            src_ref=src_ref.at[to], dst_ref=out_ref.at[core, col], send_sem=sent.at[k],
            recv_sem=came.at[k], device_id={"tp": to}, device_id_type=MESH,
        )

    def arrival(k):
        frm = lax.rem(col + m - k, m)
        return pltpu.make_async_remote_copy(
            src_ref=src_ref.at[frm], dst_ref=out_ref.at[core, frm], send_sem=sent.at[k],
            recv_sem=came.at[k], device_id={"tp": frm}, device_id_type=MESH,
        )

    def onward(k, source):
        frm = lax.rem(col + m - k, m)
        return pltpu.make_async_remote_copy(
            src_ref=source, dst_ref=out_ref.at[core, frm], send_sem=pass_sent.at[k],
            recv_sem=pass_came.at[k], device_id={"sp": partner}, device_id_type=MESH,
        )

    def from_partner(k):
        frm = lax.rem(col + m - k, m)
        return pltpu.make_async_remote_copy(
            src_ref=src_ref.at[frm], dst_ref=out_ref.at[1 - core, frm], send_sem=pass_sent.at[k],
            recv_sem=pass_came.at[k], device_id={"sp": partner}, device_id_type=MESH,
        )

    order = [m // 2] + [k for k in range(1, m) if k != m // 2]
    for k in order:
        send(k).start()
    onward(0, src_ref.at[col]).start()
    passed = [k for k in range(1, m) if k != m // 2] + [m // 2]
    for k in passed:
        arrival(k).wait_recv()
        onward(k, out_ref.at[core, lax.rem(col + m - k, m)]).start()
    own.wait()
    for k in range(m):
        from_partner(k).wait_recv()
        onward(k, src_ref.at[col]).wait_send()
    for k in range(1, m):
        send(k).wait_send()


def spread(blocks, m, number):
    return pl.pallas_call(
        functools.partial(spread_kernel, m),
        name="spread",
        out_shape=jax.ShapeDtypeStruct((2,) + blocks.shape, blocks.dtype),
        in_specs=[VMEM_SPEC],
        out_specs=VMEM_SPEC,
        scratch_shapes=[pltpu.SemaphoreType.DMA] + [pltpu.SemaphoreType.DMA((m,))] * 4,
        compiler_params=pltpu.CompilerParams(collective_id=number, has_side_effects=True),
        cost_estimate=pl.CostEstimate(flops=10**6, bytes_accessed=40 << 20, transcendentals=0),
    )(blocks)


def swap_kernel(src_ref, out_ref, own_sem, sent, came):
    me = lax.axis_index("sp")
    core, partner = lax.rem(me, 2), other_core(me)
    barrier = pltpu.get_barrier_semaphore()
    pl.semaphore_signal(barrier, inc=1, device_id={"sp": partner}, device_id_type=MESH)
    own = pltpu.make_async_copy(src_ref.at[core], out_ref.at[core], own_sem)
    own.start()
    pl.semaphore_wait(barrier, 1)
    away = pltpu.make_async_remote_copy(
        src_ref=src_ref.at[1 - core], dst_ref=out_ref.at[core], send_sem=sent, recv_sem=came,
        device_id={"sp": partner}, device_id_type=MESH,
    )
    away.start()
    own.wait()
    pltpu.make_async_remote_copy(
        src_ref=src_ref.at[1 - core], dst_ref=out_ref.at[1 - core], send_sem=sent, recv_sem=came,
        device_id={"sp": partner}, device_id_type=MESH,
    ).wait_recv()
    away.wait_send()


def swap(blocks, number):
    return pl.pallas_call(
        swap_kernel,
        name="swap",
        out_shape=jax.ShapeDtypeStruct(blocks.shape, blocks.dtype),
        in_specs=[VMEM_SPEC],
        out_specs=VMEM_SPEC,
        scratch_shapes=[pltpu.SemaphoreType.DMA] * 3,
        compiler_params=pltpu.CompilerParams(collective_id=number, has_side_effects=True),
        cost_estimate=pl.CostEstimate(flops=10**6, bytes_accessed=4 << 20, transcendentals=0),
    )(blocks)


def exchange_gather_kernel(n, m, src_ref, first_ref, second_ref, out_ref, first_all, second_all,
                           stage, own_sem, sent, came, in_sem, out_sem, ring_sent, ring_came, pass_sent, pass_came):
    me, col = lax.axis_index("sp"), lax.axis_index("tp")
    right, left = lax.rem(col + 1, m), lax.rem(col + m - 1, m)
    shards, wholes = (first_ref, second_ref), (first_all, second_all)
    barrier = pltpu.get_barrier_semaphore()

    def greet(k, _):
        pl.semaphore_signal(
            barrier, inc=1, device_id={"sp": lax.rem(me + k, n)}, device_id_type=MESH
        )
        return 0

    for side in (left, right):
        pl.semaphore_signal(barrier, inc=1, device_id={"tp": side}, device_id_type=MESH)
    lax.fori_loop(1, n, greet, 0)
    own = pltpu.make_async_copy(src_ref.at[me], out_ref.at[me], own_sem)
    own.start()
    loads = [pltpu.make_async_copy(shards[a], stage.at[a], in_sem.at[a]) for a in range(2)]
    stores = [pltpu.make_async_copy(stage.at[a], wholes[a].at[col], out_sem.at[a]) for a in range(2)]
    for load in loads:
        load.start()
    for load in loads:
        load.wait()
    pl.semaphore_wait(barrier, n + 1)

    def copy(k):
        to = lax.rem(me + k, n)
        return pltpu.make_async_remote_copy(
            src_ref=src_ref.at[to], dst_ref=out_ref.at[me], send_sem=sent.at[k], recv_sem=came.at[k],
            device_id={"sp": to}, device_id_type=MESH,
        )

    def start(k, _):
        away = n // 2 - lax.div(k, 2)
        copy(jnp.where(lax.rem(k, 2) == 0, away, n - away)).start()
        return 0

    def arrived(k):
        frm = lax.rem(me + n - k, n)
        return pltpu.make_async_remote_copy(
            src_ref=src_ref.at[frm], dst_ref=out_ref.at[frm], send_sem=sent.at[k], recv_sem=came.at[k],
            device_id={"sp": frm}, device_id_type=MESH,
        )

    half = first_ref.shape[0] // 2

    def rows(h):
        return pl.ds(h * half, half)

    def hop(a, d, h):
        return pltpu.make_async_remote_copy(
            src_ref=stage.at[a, rows(h)], dst_ref=wholes[a].at[col, rows(h)],
            send_sem=ring_sent.at[a, d, h], recv_sem=ring_came.at[a, d, h],
            device_id={"tp": (right, left)[d]}, device_id_type=MESH,
        )

    def hop_in(a, d, h):
        frm = (left, right)[d]
        return pltpu.make_async_remote_copy(
            src_ref=stage.at[a, rows(h)], dst_ref=wholes[a].at[frm, rows(h)],
            send_sem=ring_sent.at[a, d, h], recv_sem=ring_came.at[a, d, h],
            device_id={"tp": frm}, device_id_type=MESH,
        )

    def onward(a, d):
        frm = (left, right)[d]
        return pltpu.make_async_remote_copy(
            src_ref=wholes[a].at[frm, rows(d)], dst_ref=wholes[a].at[frm, rows(d)],
            send_sem=pass_sent.at[a, d], recv_sem=pass_came.at[a, d],
            device_id={"tp": (right, left)[d]}, device_id_type=MESH,
        )

    def onward_in(a, d):
        frm = lax.rem(col + 2, m)
        return pltpu.make_async_remote_copy(
            src_ref=wholes[a].at[frm, rows(d)], dst_ref=wholes[a].at[frm, rows(d)],
            send_sem=pass_sent.at[a, d], recv_sem=pass_came.at[a, d],
            device_id={"tp": (left, right)[d]}, device_id_type=MESH,
        )

    copy(n // 2).start()
    lax.fori_loop(2, n, start, 0)
    for a in range(2):
        for d, h in ((0, 0), (1, 1), (0, 1), (1, 0)):
            hop(a, d, h).start()
    for store in stores:
        store.start()
    for a in range(2):
        for d in range(2):
            hop_in(a, d, d).wait_recv()
            onward(a, d).start()
    own.wait()
    for store in stores:
        store.wait()

    def finish(k, _):
        arrived(k).wait_recv()
        copy(k).wait_send()
        return 0

    lax.fori_loop(1, n, finish, 0)
    for a in range(2):
        for d in range(2):
            hop_in(a, d, 1 - d).wait_recv()
            onward_in(a, d).wait_recv()
            onward(a, d).wait_send()
            for h in range(2):
                hop(a, d, h).wait_send()


def exchange_and_gather(blocks, first, second, n, m, number):
    any_spec = pl.BlockSpec(memory_space=pl.ANY)
    whole = jax.ShapeDtypeStruct((m,) + first.shape, first.dtype)
    return pl.pallas_call(
        functools.partial(exchange_gather_kernel, n, m),
        name=f"exchange_{number}",
        out_shape=(jax.ShapeDtypeStruct(blocks.shape, blocks.dtype), whole, whole),
        in_specs=[VMEM_SPEC, any_spec, any_spec],
        out_specs=(VMEM_SPEC, any_spec, any_spec),
        scratch_shapes=[
            pltpu.VMEM((2,) + first.shape, first.dtype),
            pltpu.SemaphoreType.DMA,
            pltpu.SemaphoreType.DMA((n,)),
            pltpu.SemaphoreType.DMA((n,)),
            pltpu.SemaphoreType.DMA((2,)),
            pltpu.SemaphoreType.DMA((2,)),
            pltpu.SemaphoreType.DMA((2, 2, 2)),
            pltpu.SemaphoreType.DMA((2, 2, 2)),
            pltpu.SemaphoreType.DMA((2, 2)),
            pltpu.SemaphoreType.DMA((2, 2)),
        ],
        compiler_params=pltpu.CompilerParams(collective_id=number, has_side_effects=True),
        cost_estimate=pl.CostEstimate(flops=10**6, bytes_accessed=200 << 20, transcendentals=0),
    )(blocks, first, second)


def reorder(capacity, to_rows):
    many = BLOCK * QUARTERS * capacity
    square = (many, many)
    out, line = (iota(square, 0), iota(square, 1)) if to_rows else (iota(square, 1), iota(square, 0))
    device, quarter = lax.div(line, QUARTERS * capacity), lax.rem(lax.div(line, capacity), QUARTERS)
    place = (quarter * BLOCK + device) * capacity + lax.rem(line, capacity)
    return jnp.where(out == place, 1.0, 0.0).astype(bf16)


def expert_kernel(
    n, capacity, came_ref, gate_ref, up_ref, down_ref, out_ref,
    gates, ups, downs, rows_ref, back_ref, load_sem, sent, came,
):
    me = lax.axis_index("sp")
    block = QUARTERS * capacity
    height = BLOCK * capacity
    part = out_ref.shape[2]
    pieces = gates.shape[0]
    groups = n // BLOCK
    loads = []
    for j in range(pieces):
        for w, (source, target) in enumerate(((gate_ref, gates), (up_ref, ups), (down_ref, downs))):
            loads.append(pltpu.make_async_copy(source.at[j], target.at[j], load_sem.at[j, w]))
    for load in loads:
        load.start()
    barrier = pltpu.get_barrier_semaphore()

    def greet(k, _):
        pl.semaphore_signal(
            barrier, inc=1, device_id={"sp": lax.rem(me + k, n)}, device_id_type=MESH
        )
        return 0

    lax.fori_loop(1, n, greet, 0)
    gather_order, spread_order = reorder(capacity, True), reorder(capacity, False)
    for load in loads:
        load.wait()

    def home(device):
        return pltpu.make_async_remote_copy(
            src_ref=back_ref.at[device], dst_ref=out_ref.at[me], send_sem=sent.at[device],
            recv_sem=came.at[me], device_id={"sp": device}, device_id_type=MESH,
        )

    def work(c, _):
        own_group = lax.div(me, BLOCK)
        both = (
            lax.rem(own_group + groups // 2 + c, groups),
            lax.rem(own_group + groups // 2 - 1 - c + groups, groups),
        )
        for i, g in enumerate(both):
            lines = jnp.concatenate([came_ref[g * BLOCK + k] for k in range(BLOCK)], axis=0)
            moved = dot(gather_order, lines).astype(bf16)
            for q in range(QUARTERS):
                rows_ref[i * height : (i + 1) * height, q * part : (q + 1) * part] = moved[
                    q * height : (q + 1) * height
                ]
        rows = rows_ref[...]
        hidden = []
        for j in range(pieces):
            gated = dot(rows, gates[j])
            hidden.append((gated * sigmoid(gated) * dot(rows, ups[j])).astype(bf16))
        total = dot(hidden[0], downs[0])
        for j in range(1, pieces):
            total = total + dot(hidden[j], downs[j])
        total = total.astype(bf16)
        for i, g in enumerate(both):
            lines = jnp.concatenate(
                [total[i * height : (i + 1) * height, q * part : (q + 1) * part] for q in range(QUARTERS)],
                axis=0,
            )
            moved = dot(spread_order, lines).astype(bf16)
            for k in range(BLOCK):
                device = g * BLOCK + k
                result = moved[k * block : (k + 1) * block]
                back_ref[device] = result

                @pl.when(device == me)
                def _():
                    out_ref[me] = result

        @pl.when(c == 0)
        def _():
            pl.semaphore_wait(barrier, n - 1)

        for g in both:
            for k in range(BLOCK):
                device = g * BLOCK + k

                @pl.when(device != me)
                def _():
                    home(device).start()

        return 0

    lax.fori_loop(0, groups // 2, work, 0)

    def finish(k, _):
        frm = lax.rem(me + k, n)
        pltpu.make_async_remote_copy(
            src_ref=back_ref.at[frm], dst_ref=out_ref.at[frm], send_sem=sent.at[frm],
            recv_sem=came.at[frm], device_id={"sp": frm}, device_id_type=MESH,
        ).wait_recv()
        home(frm).wait_send()
        return 0

    lax.fori_loop(1, n, finish, 0)


def expert_rows(came, gate, up, down, capacity, number):
    n, block, part = came.shape
    pieces, width, units = gate.shape
    any_spec = pl.BlockSpec(memory_space=pl.ANY)
    return pl.pallas_call(
        functools.partial(expert_kernel, n, capacity),
        name="expert_rows",
        out_shape=jax.ShapeDtypeStruct(came.shape, bf16),
        in_specs=[VMEM_SPEC, any_spec, any_spec, any_spec],
        out_specs=VMEM_SPEC,
        scratch_shapes=[
            pltpu.VMEM(gate.shape, bf16),
            pltpu.VMEM(up.shape, bf16),
            pltpu.VMEM(down.shape, bf16),
            pltpu.VMEM((2 * BLOCK * capacity, width), bf16),
            pltpu.VMEM(came.shape, bf16),
            pltpu.SemaphoreType.DMA((pieces, 3)),
            pltpu.SemaphoreType.DMA((n,)),
            pltpu.SemaphoreType.DMA((n,)),
        ],
        compiler_params=pltpu.CompilerParams(collective_id=number, has_side_effects=True),
        cost_estimate=pl.CostEstimate(flops=5 * 10**9, bytes_accessed=200 << 20, transcendentals=0),
    )(came, gate, up, down)


def combine_kernel(n, capacity, residual_ref, proj_ref, index_ref, weight_ref, back_ref, out_ref, rows_ref):
    rows, width = residual_ref.shape
    part = width // QUARTERS
    height = BLOCK * capacity
    order = reorder(capacity, True)
    for g in range(n // BLOCK):
        lines = jnp.concatenate([back_ref[g * BLOCK + k] for k in range(BLOCK)], axis=0)
        moved = dot(order, lines).astype(bf16)
        for q in range(QUARTERS):
            rows_ref[g * height : (g + 1) * height, q * part : (q + 1) * part] = moved[
                q * height : (q + 1) * height
            ]
    targets = route_columns(index_ref, n, capacity)
    slot = iota((rows, n * capacity), 1).astype(f32)
    mix = jnp.where(slot == targets[0], weight_ref[:, 0:1], 0.0) + jnp.where(
        slot == targets[1], weight_ref[:, 1:2], 0.0
    )
    high, low = halves(mix)
    for q in range(QUARTERS):
        cols = slice(q * part, (q + 1) * part)
        routed = dot(high, rows_ref[:, cols]) + dot(low, rows_ref[:, cols])
        half, within = divmod(q, QUARTERS // 2)
        proj = proj_ref[half, :, within * part : (within + 1) * part]
        stream = residual_ref[:, cols].astype(f32) + proj.astype(f32)
        out_ref[:, cols] = (stream + routed).astype(bf16)


def combine(residual, proj, index, weight, back, capacity):
    n = back.shape[0]
    return pl.pallas_call(
        functools.partial(combine_kernel, n, capacity),
        name="combine",
        out_shape=jax.ShapeDtypeStruct(residual.shape, bf16),
        in_specs=[VMEM_SPEC] * 5,
        out_specs=VMEM_SPEC,
        scratch_shapes=[pltpu.VMEM((n * capacity, residual.shape[1]), bf16)],
        cost_estimate=pl.CostEstimate(flops=10**9, bytes_accessed=8 << 20, transcendentals=0),
    )(residual, proj, index, weight, back)


def local(
    recept, key_input, value_input, output_gate_input, decay_input_part, correction_rate_input,
    head_decay_offset, decay_fixed_bias, correction_rate_bias, head_norm_gain, self_term_weight,
    output_weight_matrix, residual, feedforward_norm_gain, routed_expert_index, routed_expert_weight,
    gate_weight_experts, up_weight_experts, down_weight_experts,
):
    n = lax.axis_size("sp")
    cores = 2
    share = output_weight_matrix.shape[1] // cores
    columns = lax.dynamic_slice_in_dim(
        output_weight_matrix, lax.rem(lax.axis_index("sp"), cores) * share, share, axis=1
    )
    columns = lax.all_gather(columns, "tp")

    summary, maps, own = mixer_local(
        recept, key_input, value_input, decay_input_part, correction_rate_input, head_decay_offset,
        decay_fixed_bias[None], correction_rate_bias[None],
    )
    enter = prefix_states(summary, n)
    down, enter = lax.optimization_barrier((down_weight_experts[0], enter))
    down = lax.all_gather(down, "tp")
    mixed = readout(
        recept, key_input, value_input, output_gate_input, head_norm_gain[None], self_term_weight[None],
        maps, own, enter,
    )
    m = lax.axis_size("tp")
    shares = spread(mixed.reshape(m, -1, mixed.shape[1]), m, 3)
    halves_of_proj = jnp.einsum("hjrc,jcd->hrd", shares, columns, preferred_element_type=f32)
    proj = swap(halves_of_proj.astype(bf16), 4)

    rows = residual.shape[0]
    experts = gate_weight_experts.shape[0] * n
    capacity = 3 * rows // experts
    outgoing = build(residual, proj, feedforward_norm_gain[None], routed_expert_index, experts, capacity)
    came, gate, up = exchange_and_gather(
        outgoing, gate_weight_experts[0], up_weight_experts[0], n, lax.axis_size("tp"), 1
    )
    back = expert_rows(came, gate, up, down, capacity, 2)
    return combine(residual, proj, routed_expert_index, routed_expert_weight, back, capacity)


def solution(mesh):
    shared = P(("grp", "sp", "tp"), None)
    split = P(("grp", "sp"), "tp")
    return jax.shard_map(
        local,
        mesh=mesh,
        in_specs=(split,) * 7 + (P("tp"),) * 4 + (P("tp", None), shared, P(), shared, shared)
        + (P("sp", None, "tp"), P("sp", None, "tp"), P("sp", "tp", None)),
        out_specs=shared,
        check_vma=False,
    )
```
